32 devices in a mesh: grp: 2 (over y), sp: 4 (over z), fs: 2 (over x), tp: 2 (over core).
Axes of the slice: x: 2, y: 2, z: 4, core: 2. Of those that a mesh axis runs over, the one named last changes fastest.
Arguments:
- tokens: bfloat16 [8, 256, 2048], P(('grp', 'fs'), 'sp'), parts along dimension 0, may hold values from -6 to 6
- pre_gain: float32 [2048], replicated, may hold values from 0.1 to 1.9
- query_weight: bfloat16 [2048, 1024], P(('sp', 'fs'), 'tp'), may hold values from -0.125 to 0.125
- key_weight: bfloat16 [2048, 1024], P(('sp', 'fs'), 'tp'), may hold values from -0.125 to 0.125
- value_weight: bfloat16 [2048, 1024], P(('sp', 'fs'), 'tp'), may hold values from -0.125 to 0.125
- beta_weight: bfloat16 [2048, 8], replicated, may hold values from -0.125 to 0.125
- decay_weight: bfloat16 [2048, 8], replicated, may hold values from -0.125 to 0.125
- decay_rate: float32 [8], replicated, may hold values from 0 to 1
- delta_gain: float32 [128], replicated, may hold values from 0.1 to 1.9
- query_down: bfloat16 [2048, 512], P(('sp', 'fs')), may hold values from -0.125 to 0.125
- latent_down: bfloat16 [2048, 256], P(('sp', 'fs')), may hold values from -0.125 to 0.125
- rope_weight: bfloat16 [2048, 32], replicated, may hold values from -0.125 to 0.125
- query_gain: float32 [512], replicated, may hold values from 0.1 to 1.9
- latent_gain: float32 [256], replicated, may hold values from 0.1 to 1.9
- query_up: bfloat16 [512, 1536], P(None, 'tp'), may hold values from -4 to 4
- latent_up: bfloat16 [256, 2048], P(None, 'tp'), may hold values from -4 to 4
- delta_out: bfloat16 [1024, 2048], P('tp', ('sp', 'fs')), may hold values from -8 to 8
- latent_out: bfloat16 [1024, 2048], P('tp', ('sp', 'fs')), may hold values from -8 to 8
- post_gain: float32 [2048], P('tp'), may hold values from 0.1 to 1.9
Outputs:
- mixed_out: bfloat16 [8, 256, 2048], P(('grp', 'fs'), 'sp', 'tp'), parts along dimension 0
The draws below stay inside these ranges and needn't reach their ends.
There are 2 independent parts, one for each index of `grp`. The reference program is written for one: setup_inputs(seed, part) draws one part's arguments, and reference() takes and returns one part's arrays. A program takes and returns all parts, laid end to end along the dimension named above; an argument that names none is the same for every part. Nothing has to cross between parts.
All inputs are finite; a program needn't handle non-finite values.
Results may differ from the reference program's by a relative error of at most 0.018.
The reference program's roundings to bfloat16 on the way count: a program that leaves them out, or rounds other values in their place, can miss the bound.
Values may be sent and summed in bfloat16 or wider, within the bound.
No kernel may reach another device: no remote copies, remote signals or barrier semaphores. Data moves between devices by JAX's collectives and lax.ppermute only.
A program may use at most 128 MiB of HBM per device.

```python
import math
import jax
import jax.numpy as jnp
from jax import lax

D = 2048
DELTA_HEADS = 8
HEAD = 128
LATENT_HEADS = 16
NOPE = 64
ROPE = 32
VDIM = 64
QRANK = 512
KVRANK = 256
BLOCK = 64
SEQS = 4
LENGTH = 256


def draw_decay_rate(key, part):
    slow_key, fast_key, order_key = jax.random.split(key, 3)
    slow_rate = jnp.exp(jax.random.uniform(slow_key, (DELTA_HEADS,), jnp.float32, math.log(0.3), math.log(1.5))) / LENGTH
    fast_rate = jnp.exp(jax.random.uniform(fast_key, (DELTA_HEADS,), jnp.float32, math.log(0.025), math.log(0.06)))
    head_order = jax.random.permutation(order_key, DELTA_HEADS)
    return jnp.where(head_order < DELTA_HEADS // 2, fast_rate, slow_rate)


def column_scaled(key, row_count):
    entry_key, jitter_key = jax.random.split(key)
    entries = jnp.clip(jax.random.normal(entry_key, (row_count, D), jnp.float32), -6.0, 6.0)
    jitter = jax.random.uniform(jitter_key, (D,), jnp.float32, -0.5, 0.5)
    column_tilt = 2.2 * (jnp.arange(D, dtype=jnp.float32) / D - 0.5)
    fan_scale = (DELTA_HEADS * HEAD + LATENT_HEADS * VDIM) ** (-0.5)
    return entries * jnp.exp(column_tilt + jitter)[None, :] * fan_scale


def draw_delta_out(key, part):
    return column_scaled(jax.random.fold_in(key, 11), DELTA_HEADS * HEAD).astype(jnp.bfloat16)


def draw_latent_out(key, part):
    return column_scaled(jax.random.fold_in(key, 23), LATENT_HEADS * VDIM).astype(jnp.bfloat16)


def expansion_base(key, rank, head_width):
    entries = jnp.clip(jax.random.normal(key, (rank, LATENT_HEADS, head_width), jnp.float32), -6.0, 6.0)
    return entries / math.sqrt(rank)


def draw_query_up(key, part):
    entries = expansion_base(jax.random.fold_in(key, 31), QRANK, NOPE + ROPE)
    return entries.reshape(QRANK, LATENT_HEADS * (NOPE + ROPE)).astype(jnp.bfloat16)


def draw_latent_up(key, part):
    entries = expansion_base(jax.random.fold_in(key, 53), KVRANK, NOPE + VDIM)
    return entries.reshape(KVRANK, LATENT_HEADS * (NOPE + VDIM)).astype(jnp.bfloat16)


def shard_levels(stream_key, extent, cuts, low, largest):
    def one(axis_at, parts):
        heights = jax.random.uniform(jax.random.fold_in(jax.random.fold_in(stream_key, 6), axis_at), (parts,), jnp.float32, low / len(cuts), largest / len(cuts))
        return jnp.repeat(jnp.exp(heights), extent[axis_at] // parts).reshape((-1,) + (1,) * (len(extent) - axis_at - 1))

    factor_of = one(*cuts[0])
    for cut in cuts[1:]:
        factor_of = factor_of * one(*cut)
    return factor_of


def gaussian(stream_key, dims, scale, limit, cuts=(), held_as=jnp.bfloat16):
    result = scale * jax.random.normal(stream_key, dims, jnp.float32)
    if cuts:
        result = result * shard_levels(stream_key, dims, cuts, -0.22, 0.18)
    return jnp.clip(result, -limit, limit).astype(held_as)


def setup_inputs(seed: int = 0, part: int = 0) -> dict:
    key_of = jax.random.split(jax.random.key(seed), 20)
    own_keys = jax.random.split(jax.random.fold_in(key_of[19], part), 20)
    tokens = gaussian(own_keys[0], (SEQS, LENGTH, D), 1.0, 6.0, ((0, 2), (1, 4)))
    pre_gain = jnp.clip(1.0 + 0.18 * jax.random.normal(key_of[1], (D,), jnp.float32), 0.1, 1.9)
    query_weight = gaussian(key_of[2], (D, DELTA_HEADS * HEAD), D ** -0.5, 0.125, ((0, 8), (1, 2)))
    key_weight = gaussian(key_of[3], (D, DELTA_HEADS * HEAD), D ** -0.5, 0.125, ((0, 8), (1, 2)))
    value_weight = gaussian(key_of[4], (D, DELTA_HEADS * HEAD), D ** -0.5, 0.125, ((0, 8), (1, 2)))
    beta_weight = gaussian(key_of[5], (D, DELTA_HEADS), D ** -0.5, 0.125)
    decay_weight = gaussian(key_of[6], (D, DELTA_HEADS), D ** -0.5, 0.125)
    decay_rate = draw_decay_rate(jax.random.fold_in(key_of[19], 71), part)
    delta_gain = jnp.clip(1.0 + 0.18 * jax.random.normal(key_of[8], (HEAD,), jnp.float32), 0.1, 1.9)
    query_down = gaussian(key_of[9], (D, QRANK), D ** -0.5, 0.125, ((0, 8),))
    latent_down = gaussian(key_of[10], (D, KVRANK), D ** -0.5, 0.125, ((0, 8),))
    rope_weight = gaussian(key_of[11], (D, ROPE), D ** -0.5, 0.125)
    query_gain = jnp.clip(1.0 + 0.18 * jax.random.normal(key_of[12], (QRANK,), jnp.float32), 0.1, 1.9)
    latent_gain = jnp.clip(1.0 + 0.18 * jax.random.normal(key_of[13], (KVRANK,), jnp.float32), 0.1, 1.9)
    query_up = draw_query_up(jax.random.fold_in(key_of[19], 71), part)
    latent_up = draw_latent_up(jax.random.fold_in(key_of[19], 71), part)
    delta_out = draw_delta_out(jax.random.fold_in(key_of[19], 71), part)
    latent_out = draw_latent_out(jax.random.fold_in(key_of[19], 71), part)
    post_gain = jnp.clip(1.0 + 0.18 * jax.random.normal(key_of[18], (D,), jnp.float32), 0.1, 1.9)
    return dict(tokens=tokens, pre_gain=pre_gain, query_weight=query_weight, key_weight=key_weight, value_weight=value_weight, beta_weight=beta_weight, decay_weight=decay_weight, decay_rate=decay_rate, delta_gain=delta_gain, query_down=query_down, latent_down=latent_down, rope_weight=rope_weight, query_gain=query_gain, latent_gain=latent_gain, query_up=query_up, latent_up=latent_up, delta_out=delta_out, latent_out=latent_out, post_gain=post_gain)


NORM_EPS = 1e-06
ROPE_THETA = 10000.0
HIGHEST = lax.Precision.HIGHEST

def stored(values):
    return lax.optimization_barrier(values.astype(jnp.bfloat16))

def rms_scale(values):
    return lax.rsqrt(lax.optimization_barrier(jnp.mean(values * values, axis=-1, keepdims=True)) + NORM_EPS)

def unit_rows(values):
    return values * lax.rsqrt(lax.optimization_barrier(jnp.sum(values * values, axis=-1, keepdims=True)) + NORM_EPS)

def rope_tables(positions, rope_width):
    frequency = ROPE_THETA ** (-jnp.arange(0, rope_width, 2, dtype=jnp.float32) / rope_width)
    angles = positions.astype(jnp.float32)[:, None] * frequency[None, :]
    return (jnp.cos(angles), jnp.sin(angles))

def rotate(values, cosine_table, sine_table):
    lower_half, upper_half = jnp.split(values, 2, axis=-1)
    return jnp.concatenate([lower_half * cosine_table - upper_half * sine_table, upper_half * cosine_table + lower_half * sine_table], axis=-1)

def delta_terms(query_vectors, key_vectors, value_vectors, beta_gate, log_decay):
    length, head_count, head_width = query_vectors.shape
    nblocks = length // BLOCK

    def split_blocks(tensor):
        return jnp.moveaxis(tensor.reshape((nblocks, BLOCK, head_count) + tensor.shape[2:]), 2, 0)
    query_vectors = split_blocks(query_vectors)
    key_vectors = split_blocks(key_vectors)
    value_vectors = split_blocks(value_vectors)
    beta_gate = split_blocks(beta_gate)
    gate_sum = jnp.cumsum(split_blocks(log_decay), axis=-1)
    position = jnp.arange(BLOCK)
    strict = position[:, None] > position[None, :]
    causal = position[:, None] >= position[None, :]
    gate_gap = gate_sum[..., :, None] - gate_sum[..., None, :]
    strict_decay = jnp.where(strict, jnp.exp(jnp.where(strict, gate_gap, 0.0)), 0.0)
    causal_decay = jnp.where(causal, jnp.exp(jnp.where(causal, gate_gap, 0.0)), 0.0)
    keys_scaled = key_vectors * beta_gate[..., None]
    lower_mat = jnp.einsum('hnid,hnjd->hnij', keys_scaled, key_vectors, precision=HIGHEST) * strict_decay
    identity = jnp.eye(BLOCK, dtype=jnp.float32)
    inverse = jax.scipy.linalg.solve_triangular(identity + lower_mat, jnp.broadcast_to(identity, lower_mat.shape), lower=True)
    new_values = jnp.einsum('hnij,hnjd->hnid', inverse, value_vectors * beta_gate[..., None], precision=HIGHEST)
    key_weights = jnp.einsum('hnij,hnjd->hnid', inverse, keys_scaled * jnp.exp(gate_sum)[..., None], precision=HIGHEST)
    scores = jnp.einsum('hnid,hnjd->hnij', query_vectors, key_vectors, precision=HIGHEST) * causal_decay
    last_gate = gate_sum[..., -1]
    query_decay = query_vectors * jnp.exp(gate_sum)[..., None]
    key_decay = key_vectors * jnp.exp(last_gate[..., None] - gate_sum)[..., None]
    return (query_decay, key_decay, new_values, key_weights, scores, last_gate)

def delta_rule(query_vectors, key_vectors, value_vectors, beta_gate, log_decay):
    head_count, head_width = (query_vectors.shape[1], query_vectors.shape[2])
    block_terms = delta_terms(query_vectors, key_vectors, value_vectors, beta_gate, log_decay)
    inputs = tuple((jnp.moveaxis(tensor, 1, 0) for tensor in block_terms))

    def advance(carried, block_in):
        query_decay, key_decay, new_values, key_weights, scores, last_gate = block_in
        corrected = new_values - jnp.einsum('hcd,hde->hce', key_weights, carried, precision=HIGHEST)
        output = jnp.einsum('hcd,hde->hce', query_decay, carried, precision=HIGHEST) + jnp.einsum('hij,hje->hie', scores, corrected, precision=HIGHEST)
        carried = carried * jnp.exp(last_gate)[:, None, None] + jnp.einsum('hcd,hce->hde', key_decay, corrected, precision=HIGHEST)
        return (carried, output)
    zero_state = jnp.zeros((head_count, head_width, head_width), jnp.float32)
    _, outputs = lax.scan(advance, zero_state, inputs)
    return jnp.transpose(outputs, (0, 2, 1, 3)).reshape(-1, head_count, head_width)

def reference(tokens, pre_gain, query_weight, key_weight, value_weight, beta_weight, decay_weight, decay_rate, delta_gain, query_down, latent_down, rope_weight, query_gain, latent_gain, query_up, latent_up, delta_out, latent_out, post_gain):
    f32 = jnp.float32

    def one_sequence(sequence):
        length = sequence.shape[0]
        positions = jnp.arange(length)
        seq_float = sequence.astype(f32)
        normed = stored(seq_float * rms_scale(seq_float) * pre_gain)
        raw_query = stored(jnp.dot(normed, query_weight, preferred_element_type=f32))
        raw_key = stored(jnp.dot(normed, key_weight, preferred_element_type=f32))
        raw_value = stored(jnp.dot(normed, value_weight, preferred_element_type=f32))
        q_latent = stored(jnp.dot(normed, query_down, preferred_element_type=f32))
        kv_latent = stored(jnp.dot(normed, latent_down, preferred_element_type=f32))
        rope_raw = stored(jnp.dot(normed, rope_weight, preferred_element_type=f32))
        beta_gate = jax.nn.sigmoid(jnp.dot(normed, beta_weight, preferred_element_type=f32))
        log_decay = -decay_rate[None, :] * jax.nn.softplus(jnp.dot(normed, decay_weight, preferred_element_type=f32))
        query_vectors = unit_rows(jax.nn.silu(raw_query.astype(f32)).reshape(length, DELTA_HEADS, HEAD)) * HEAD ** (-0.5)
        key_vectors = unit_rows(jax.nn.silu(raw_key.astype(f32)).reshape(length, DELTA_HEADS, HEAD))
        value_vectors = jax.nn.silu(raw_value.astype(f32)).reshape(length, DELTA_HEADS, HEAD)
        delta_raw = delta_rule(query_vectors, key_vectors, value_vectors, beta_gate, log_decay)
        delta_heads = stored(delta_raw * rms_scale(delta_raw) * delta_gain).reshape(length, DELTA_HEADS * HEAD)
        q_lat32 = q_latent.astype(f32)
        kv_lat32 = kv_latent.astype(f32)
        q_normed = stored(q_lat32 * rms_scale(q_lat32) * query_gain)
        kv_normed = stored(kv_lat32 * rms_scale(kv_lat32) * latent_gain)
        cosine_table, sine_table = rope_tables(positions, ROPE)
        rope_keys = stored(rotate(rope_raw.astype(f32), cosine_table, sine_table)).astype(f32)
        query_all = stored(jnp.dot(q_normed, query_up, preferred_element_type=f32)).reshape(length, LATENT_HEADS, NOPE + ROPE)
        kv_all = stored(jnp.dot(kv_normed, latent_up, preferred_element_type=f32)).reshape(length, LATENT_HEADS, NOPE + VDIM)
        query_plain = query_all[..., :NOPE].astype(f32)
        query_turned = stored(rotate(query_all[..., NOPE:].astype(f32), cosine_table[:, None, :], sine_table[:, None, :])).astype(f32)
        key_plain = kv_all[..., :NOPE].astype(f32)
        value_rows = kv_all[..., NOPE:].astype(f32)
        score_scale = (NOPE + ROPE) ** (-0.5)
        query_span = math.gcd(length, 512)
        key_block = positions // BLOCK

        def attend(block_index):
            row_start = block_index * query_span
            plain_rows = lax.dynamic_slice_in_dim(query_plain, row_start, query_span, 0)
            turned_rows = lax.dynamic_slice_in_dim(query_turned, row_start, query_span, 0)
            logits = (jnp.einsum('qhd,khd->hqk', plain_rows, key_plain) + jnp.einsum('qhd,kd->hqk', turned_rows, rope_keys)) * score_scale
            query_block = (row_start + jnp.arange(query_span)) // BLOCK
            allowed = key_block[None, :] <= query_block[:, None]
            logits = jnp.where(allowed[None], logits, -jnp.inf)
            peak = lax.optimization_barrier(jnp.max(logits, axis=-1, keepdims=True))
            weights = jnp.where(allowed[None], jnp.exp(logits - peak), 0.0)
            row_sum = lax.optimization_barrier(jnp.sum(weights, axis=-1))
            weights_b = stored(weights).astype(f32)
            weighted = jnp.einsum('hqk,khd->qhd', weights_b, value_rows)
            return stored(weighted / jnp.transpose(row_sum)[:, :, None]).reshape(query_span, LATENT_HEADS * VDIM)
        latent_heads = lax.map(attend, jnp.arange(length // query_span)).reshape(length, LATENT_HEADS * VDIM)
        half_delta = DELTA_HEADS * HEAD // 2
        half_latent = LATENT_HEADS * VDIM // 2
        mixed = jnp.zeros((length, D), f32)
        for group_index in range(2):
            group_heads = jnp.concatenate([delta_heads[:, group_index * half_delta:(group_index + 1) * half_delta], latent_heads[:, group_index * half_latent:(group_index + 1) * half_latent]], axis=1)
            group_rows = jnp.concatenate([delta_out[group_index * half_delta:(group_index + 1) * half_delta], latent_out[group_index * half_latent:(group_index + 1) * half_latent]], axis=0)
            group_term = jnp.dot(group_heads, group_rows, preferred_element_type=f32)
            mixed = mixed + stored(group_term).astype(f32)
        return (mixed * rms_scale(mixed) * post_gain).astype(jnp.bfloat16)
    return lax.map(one_sequence, tokens)
```

```python
import math

import jax
import jax.numpy as jnp
from jax import lax
from jax.experimental import pallas as pl
from jax.experimental.pallas import tpu as pltpu
from jax.sharding import PartitionSpec as P

D = 2048
HEAD = 128
NOPE = 64
ROPE = 32
VDIM = 64
BLOCK = 64


NORM_EPS = 1e-06
ROPE_THETA = 10000.0
HIGHEST = lax.Precision.HIGHEST


def prefix(array, axis, join, neutral):
    place = lax.axis_index(axis)
    gathered = jax.tree.map(
        lambda a, kind: lax.all_gather(a.astype(kind), axis), array, (jnp.bfloat16, jnp.bfloat16)
    )
    state = jax.tree.map(lambda a, e: jnp.zeros_like(a) + jnp.asarray(e, a.dtype), array, neutral)

    def one(step, state):
        return join(
            state,
            jax.tree.map(
                lambda a, own: lax.dynamic_index_in_dim(a, step, 0, False).astype(own.dtype),
                gathered,
                array,
            ),
        )

    return lax.fori_loop(0, place, one, state)


def stored(values):
    return lax.optimization_barrier(values.astype(jnp.bfloat16))


def rms_scale(values):
    return lax.rsqrt(jnp.mean(values * values, axis=-1, keepdims=True) + NORM_EPS)


def unit_rows(values):
    return values * lax.rsqrt(jnp.sum(values * values, axis=-1, keepdims=True) + NORM_EPS)


def rope_tables(positions, rope_width):
    frequency = ROPE_THETA ** (-jnp.arange(0, rope_width, 2, dtype=jnp.float32) / rope_width)
    angles = positions.astype(jnp.float32)[:, None] * frequency[None, :]
    return (jnp.cos(angles), jnp.sin(angles))


def rotate(values, cosine_table, sine_table):
    lower_half, upper_half = jnp.split(values, 2, axis=-1)
    return jnp.concatenate(
        [
            lower_half * cosine_table - upper_half * sine_table,
            upper_half * cosine_table + lower_half * sine_table,
        ],
        axis=-1,
    )


def delta_terms(query_vectors, key_vectors, value_vectors, beta_gate, log_decay):
    length, head_count, head_width = query_vectors.shape
    nblocks = length // BLOCK

    def split_blocks(tensor):
        return jnp.moveaxis(tensor.reshape((nblocks, BLOCK, head_count) + tensor.shape[2:]), 2, 0)

    query_vectors = split_blocks(query_vectors)
    key_vectors = split_blocks(key_vectors)
    value_vectors = split_blocks(value_vectors)
    beta_gate = split_blocks(beta_gate)
    gate_sum = jnp.cumsum(split_blocks(log_decay), axis=-1)
    position = jnp.arange(BLOCK)
    strict = position[:, None] > position[None, :]
    causal = position[:, None] >= position[None, :]
    gate_gap = gate_sum[..., :, None] - gate_sum[..., None, :]
    strict_decay = jnp.where(strict, jnp.exp(jnp.where(strict, gate_gap, 0.0)), 0.0)
    causal_decay = jnp.where(causal, jnp.exp(jnp.where(causal, gate_gap, 0.0)), 0.0)
    keys_scaled = key_vectors * beta_gate[..., None]
    lower_mat = (
        jnp.einsum("hnid,hnjd->hnij", keys_scaled, key_vectors, precision=HIGHEST) * strict_decay
    )
    identity = jnp.eye(BLOCK, dtype=jnp.float32)
    inverse = jax.scipy.linalg.solve_triangular(
        identity + lower_mat, jnp.broadcast_to(identity, lower_mat.shape), lower=True
    )
    new_values = jnp.einsum(
        "hnij,hnjd->hnid", inverse, value_vectors * beta_gate[..., None], precision=HIGHEST
    )
    key_weights = jnp.einsum(
        "hnij,hnjd->hnid", inverse, keys_scaled * jnp.exp(gate_sum)[..., None], precision=HIGHEST
    )
    scores = (
        jnp.einsum("hnid,hnjd->hnij", query_vectors, key_vectors, precision=HIGHEST) * causal_decay
    )
    last_gate = gate_sum[..., -1]
    query_decay = query_vectors * jnp.exp(gate_sum)[..., None]
    key_decay = key_vectors * jnp.exp(last_gate[..., None] - gate_sum)[..., None]
    return (query_decay, key_decay, new_values, key_weights, scores, last_gate)


def compose(earlier, following):
    return (
        jnp.einsum("hij,hjk->hik", following[0], earlier[0], precision=HIGHEST),
        jnp.einsum("hij,hjk->hik", following[0], earlier[1], precision=HIGHEST) + following[1],
    )


def keep_same(current):
    return current


def local(
    tokens,
    pre_gain,
    query_weight,
    key_weight,
    value_weight,
    beta_weight,
    decay_weight,
    decay_rate,
    delta_gain,
    query_down,
    latent_down,
    rope_weight,
    query_gain,
    latent_gain,
    query_up,
    latent_up,
    delta_out,
    latent_out,
    post_gain,
):
    f32 = jnp.float32
    seq_count, token_count = (tokens.shape[0], tokens.shape[1])
    row_total = seq_count * token_count
    sequence = tokens.reshape(row_total, tokens.shape[2]).astype(f32)
    query_start = lax.axis_index("sp") * token_count
    positions = query_start + jnp.arange(token_count)
    normed = (sequence * rms_scale(sequence) * pre_gain).astype(jnp.bfloat16)
    head_group = lax.axis_index("tp")
    q_width = query_down.shape[1] // lax.axis_size("tp")
    kv_width = latent_down.shape[1] // lax.axis_size("tp")
    q_own = lax.dynamic_slice_in_dim(query_down, head_group * q_width, q_width, 1)
    kv_own = lax.dynamic_slice_in_dim(latent_down, head_group * kv_width, kv_width, 1)
    weights = (query_weight, key_weight, value_weight, q_own, kv_own)
    portion = (
        lax.all_gather(query_weight, ("sp", "fs"), axis=0, tiled=True),
        lax.all_gather(key_weight, ("sp", "fs"), axis=0, tiled=True),
        lax.all_gather(value_weight, ("sp", "fs"), axis=0, tiled=True),
        lax.all_gather(q_own, ("sp", "fs"), axis=0, tiled=True),
        lax.all_gather(kv_own, ("sp", "fs"), axis=0, tiled=True),
    )
    row_count = portion[0].shape[0]
    projected = tuple((jnp.dot(normed, weight, preferred_element_type=f32) for weight in portion))
    raw_query, raw_key, raw_value, q_half, kv_half = tuple((stored(member) for member in projected))
    q_latent, kv_latent = (
        lax.all_gather(q_half, "tp", axis=1, tiled=True),
        lax.all_gather(kv_half, "tp", axis=1, tiled=True),
    )
    head_count = query_weight.shape[1] // HEAD
    lane_count = seq_count * head_count
    beta_full = jax.nn.sigmoid(jnp.dot(normed, beta_weight, preferred_element_type=f32))
    beta_gate = lax.dynamic_slice_in_dim(beta_full, head_group * head_count, head_count, 1)
    decay_full = jnp.dot(normed, decay_weight, preferred_element_type=f32)
    decay_pre = lax.dynamic_slice_in_dim(decay_full, head_group * head_count, head_count, 1)
    decay_local = lax.dynamic_slice_in_dim(decay_rate, head_group * head_count, head_count, 0)
    log_decay = -decay_local[None, :] * jax.nn.softplus(decay_pre)

    def by_position(values):
        shaped = values.reshape((seq_count, token_count) + values.shape[1:])
        shaped = jnp.moveaxis(shaped, 0, 1)
        return shaped.reshape((token_count, seq_count * values.shape[1]) + values.shape[2:])

    query_vectors = by_position(
        unit_rows(jax.nn.silu(raw_query.astype(f32)).reshape(row_total, head_count, HEAD))
        * HEAD ** (-0.5)
    )
    key_vectors = by_position(
        unit_rows(jax.nn.silu(raw_key.astype(f32)).reshape(row_total, head_count, HEAD))
    )
    value_vectors = by_position(
        jax.nn.silu(raw_value.astype(f32)).reshape(row_total, head_count, HEAD)
    )
    block_terms = delta_terms(
        query_vectors, key_vectors, value_vectors, by_position(beta_gate), by_position(log_decay)
    )
    inputs = tuple((jnp.moveaxis(tensor, 1, 0) for tensor in block_terms))

    def advance(totals, block_in):
        carried, transfer = totals
        query_decay, key_decay, new_values, key_weights, scores, last_gate = block_in
        corrected = new_values - jnp.einsum("hcd,hde->hce", key_weights, carried, precision=HIGHEST)
        output = jnp.einsum("hcd,hde->hce", query_decay, carried, precision=HIGHEST) + jnp.einsum(
            "hij,hje->hie", scores, corrected, precision=HIGHEST
        )
        reader_rows = query_decay - jnp.einsum(
            "hij,hjd->hid", scores, key_weights, precision=HIGHEST
        )
        reader = jnp.einsum("hcd,hde->hce", reader_rows, transfer, precision=HIGHEST)
        factor = jnp.exp(last_gate)[:, None, None]
        carried = carried * factor + jnp.einsum(
            "hcd,hce->hde", key_decay, corrected, precision=HIGHEST
        )
        moved = jnp.einsum("hcd,hde->hce", key_weights, transfer, precision=HIGHEST)
        transfer = transfer * factor - jnp.einsum(
            "hcd,hce->hde", key_decay, moved, precision=HIGHEST
        )
        return ((carried, transfer), (output, reader))

    eye_stack = jnp.broadcast_to(jnp.eye(HEAD, dtype=f32), (lane_count, HEAD, HEAD))
    zero_state = jnp.zeros((lane_count, HEAD, HEAD), f32)
    (state_end, transfer_end), (outputs, readers) = lax.scan(
        advance, (zero_state, eye_stack), inputs
    )
    _, incoming = prefix((transfer_end, state_end), "sp", compose, (eye_stack, zero_state))
    outputs = outputs + jnp.einsum("nhcd,hde->nhce", readers, incoming, precision=HIGHEST)
    delta_raw = jnp.transpose(outputs, (0, 2, 1, 3)).reshape(
        token_count, seq_count, head_count, HEAD
    )
    delta_raw = jnp.moveaxis(delta_raw, 1, 0).reshape(row_total, head_count, HEAD)
    delta_heads = (
        (delta_raw * rms_scale(delta_raw) * delta_gain)
        .astype(jnp.bfloat16)
        .reshape(row_total, head_count * HEAD)
    )
    q_lat32 = q_latent.astype(f32)
    kv_lat32 = kv_latent.astype(f32)
    q_normed = (q_lat32 * rms_scale(q_lat32) * query_gain).astype(jnp.bfloat16)
    kv_normed = (kv_lat32 * rms_scale(kv_lat32) * latent_gain).astype(jnp.bfloat16)
    rope_raw = stored(jnp.dot(normed, rope_weight, preferred_element_type=f32))
    cosine_table, sine_table = rope_tables(positions, rope_raw.shape[1])
    rope_keys = rotate(
        rope_raw.astype(f32).reshape(seq_count, token_count, rope_raw.shape[1]),
        cosine_table,
        sine_table,
    ).astype(jnp.bfloat16)
    latent_count = query_up.shape[1] // (NOPE + ROPE)
    query_all = stored(jnp.dot(q_normed, query_up, preferred_element_type=f32)).reshape(
        seq_count, token_count, latent_count, NOPE + ROPE
    )
    query_plain = query_all[..., :NOPE]
    query_turned = rotate(
        query_all[..., NOPE:].astype(f32), cosine_table[:, None, :], sine_table[:, None, :]
    ).astype(jnp.bfloat16)
    score_scale = (NOPE + ROPE) ** (-0.5)
    query_block = positions // BLOCK
    kv_seq = kv_normed.reshape(seq_count, token_count, kv_normed.shape[1])

    def attend_block(totals, key_plain, value_rows, rope_rows, key_start):
        row_max, row_sum, weighted = totals
        key_block = (key_start + jnp.arange(key_plain.shape[1])) // BLOCK
        allowed = key_block[None, :] <= query_block[:, None]
        logits = (
            jnp.einsum("sqhd,skhd->shqk", query_plain, key_plain, preferred_element_type=f32)
            + jnp.einsum("sqhd,skd->shqk", query_turned, rope_rows, preferred_element_type=f32)
        ) * score_scale
        logits = jnp.where(allowed[None, None], logits, -jnp.inf)
        new_max = jnp.maximum(row_max, jnp.max(logits, axis=-1))
        shift = jnp.where(jnp.isfinite(new_max), new_max, 0.0)
        weights = jnp.where(allowed[None, None], jnp.exp(logits - shift[..., None]), 0.0)
        rescale = jnp.exp(row_max - shift)
        row_sum = row_sum * rescale + jnp.sum(weights, axis=-1)
        weighted = weighted * rescale[..., None] + jnp.einsum(
            "shqk,skhd->shqd", weights.astype(jnp.bfloat16), value_rows, preferred_element_type=f32
        )
        return (new_max, row_sum, weighted)

    start_stats = (
        jnp.full((seq_count, latent_count, token_count), -jnp.inf, f32),
        jnp.zeros((seq_count, latent_count, token_count), f32),
        jnp.zeros((seq_count, latent_count, token_count, VDIM), f32),
    )

    def expand_latent(portion, row_start, span_rows):
        latent_rows = lax.dynamic_slice_in_dim(portion[0], row_start, span_rows, 1)
        expanded = jnp.dot(
            latent_rows.reshape(seq_count * span_rows, latent_rows.shape[2]),
            latent_up,
            preferred_element_type=f32,
        ).astype(jnp.bfloat16)
        expanded = expanded.reshape(seq_count, span_rows, latent_count, NOPE + VDIM)
        return (
            expanded[..., :NOPE],
            expanded[..., NOPE:],
            lax.dynamic_slice_in_dim(portion[1], row_start, span_rows, 1),
        )

    portion = (
        lax.all_gather(kv_seq, "sp", axis=1, tiled=True),
        lax.all_gather(rope_keys, "sp", axis=1, tiled=True),
    )
    row_count = portion[0].shape[1]
    span_rows = math.gcd(row_count, token_count * max(1, 512 // token_count))

    def visit_rows(current):

        def visit_block(block_index, stats):
            row_start = block_index * span_rows
            key_plain, value_rows, rope_rows = expand_latent(portion, row_start, span_rows)
            return attend_block(stats, key_plain, value_rows, rope_rows, row_start)

        return lax.fori_loop(0, row_count // span_rows, visit_block, current)

    row_max, row_sum, weighted = lax.cond(
        jnp.int32(0) < query_start + token_count, visit_rows, keep_same, start_stats
    )
    latent_heads = (
        jnp.transpose(weighted / row_sum[..., None], (0, 2, 1, 3))
        .reshape(row_total, latent_count * VDIM)
        .astype(jnp.bfloat16)
    )
    heads_joined = jnp.concatenate([delta_heads, latent_heads], axis=1)
    out_rows = jnp.concatenate([delta_out, latent_out], axis=0)
    partial_value = jnp.dot(
        heads_joined,
        lax.all_gather(out_rows, ("sp", "fs"), axis=1, tiled=True),
        preferred_element_type=f32,
    )
    mixed_half = lax.psum_scatter(
        partial_value.astype(jnp.bfloat16), "tp", scatter_dimension=1, tiled=True
    ).astype(jnp.float32)
    squares = lax.psum(jnp.sum(mixed_half * mixed_half, axis=1), "tp")
    row_scale = lax.rsqrt(squares / D + NORM_EPS)
    result = mixed_half * row_scale[:, None] * post_gain
    return result.astype(jnp.bfloat16).reshape(seq_count, token_count, result.shape[1])


def shift(count, step):
    return [(i, (i + step) % count) for i in range(count)]


def pick(array, index):
    return lax.dynamic_index_in_dim(array, index, 0, False)


def dot32(left, right):
    return jnp.dot(left, right, preferred_element_type=jnp.float32)


def dot_t(left, right, precision=None):
    return lax.dot_general(
        left,
        right,
        (((1,), (1,)), ((), ())),
        precision=precision,
        preferred_element_type=jnp.float32,
    )


def exact(left, right):
    return jnp.dot(left, right, precision=HIGHEST, preferred_element_type=jnp.float32)


def kernel_call(body, out_shapes, args, scratch=(), scalars=1, name=None):
    specs = [
        pl.BlockSpec(memory_space=pltpu.SMEM if i < scalars else pltpu.VMEM)
        for i in range(len(args))
    ]
    return pl.pallas_call(
        body,
        out_shape=out_shapes,
        in_specs=specs,
        out_specs=jax.tree.map(lambda _: pl.BlockSpec(memory_space=pltpu.VMEM), out_shapes),
        scratch_shapes=scratch,
        name=name,
        compiler_params=pltpu.CompilerParams(vmem_limit_bytes=56 * 1024 * 1024),
    )(*args)


def project(ids, tokens_own, mine, theirs, weights, extra, sizes):
    sp_size, seq_count, token_count, half, fine, q_cols, kv_cols = sizes
    rows = seq_count * token_count
    span = sp_size * token_count
    width = tokens_own.shape[1]
    part = mine[0].shape[1]
    columns = weights[0].shape[1]
    extra_width = extra.shape[1]
    others = sp_size - 1

    def body(ids_ref, *refs):
        own_ref, refs = refs[0], refs[1:]
        mine_refs, refs = refs[:others], refs[others:]
        their_refs, refs = refs[:others], refs[others:]
        block_refs, refs = refs[:10], refs[10:]
        extra_ref, fine_ref, lat_ref, ext_ref, weight_ref, token_ref = refs
        place, fs_at, grp_at, tp_at = (ids_ref[i] for i in range(4))

        def at_row(offset, fs_flip, grp_flip):
            source = lax.rem(place + offset, sp_size)
            fs_from = 1 - fs_at if fs_flip else fs_at
            grp_from = 1 - grp_at if grp_flip else grp_at
            return pl.multiple_of(((source * 2 + fs_from) * 2 + grp_from) * half, half)

        for group, first, number in ((0, 0, 1), (5, 1, others)):
            for k, (fs_flip, grp_flip) in enumerate(((0, 0), (1, 0), (0, 1))):
                for j in range(number):
                    weight_ref[pl.ds(at_row(first + j, fs_flip, grp_flip), half), :] = block_refs[
                        group + k
                    ][j * half : (j + 1) * half, :]
            step = half // 2
            for j in range(2 * number):
                source = block_refs[group + 3 + j // number]
                begin = pl.multiple_of(at_row(first + j // 2, 1, 1) + (j % 2) * step, step)
                weight_ref[pl.ds(begin, step), :] = source[
                    (j % number) * step : (j % number + 1) * step, :
                ]
        mine_at = pl.multiple_of(tp_at * part, part)
        their_at = pl.multiple_of((1 - tp_at) * part, part)
        for j in range(others):
            token_ref[:, pl.ds(mine_at, part)] = mine_refs[j][...]
            token_ref[:, pl.ds(their_at, part)] = their_refs[j][...]
            lhs = token_ref[...]
            emit(lhs, j + 1, place, weight_ref, extra_ref, fine_ref, lat_ref, ext_ref)
        emit(own_ref[...], 0, place, weight_ref, extra_ref, fine_ref, lat_ref, ext_ref)

    def emit(lhs, offset, place, weight_ref, extra_ref, fine_ref, lat_ref, ext_ref):
        begin = pl.multiple_of(lax.rem(place + offset, sp_size) * token_count, token_count)
        value = dot32(lhs, weight_ref[...]).astype(jnp.bfloat16)
        outer = dot32(lhs, extra_ref[...])
        for n in range(seq_count):
            cut = slice(n * token_count, (n + 1) * token_count)
            fine_ref[n, pl.ds(begin, token_count), :] = value[cut, :fine]
            lat_ref[n, pl.ds(begin, token_count), :] = value[cut, fine:]
            ext_ref[n, pl.ds(begin, token_count), :] = outer[cut]

    return kernel_call(
        body,
        (
            jax.ShapeDtypeStruct((seq_count, span, fine), jnp.bfloat16),
            jax.ShapeDtypeStruct((seq_count, span, q_cols + kv_cols), jnp.bfloat16),
            jax.ShapeDtypeStruct((seq_count, span, extra_width), jnp.float32),
        ),
        (ids, tokens_own, *mine, *theirs, *weights, extra),
        scratch=(
            pltpu.VMEM((width, columns), jnp.bfloat16),
            pltpu.VMEM((rows, width), jnp.bfloat16),
        ),
        name="project",
    )


def lower_inverse(lower, base):
    size = lower.shape[0]
    row = lax.broadcasted_iota(jnp.int32, (size, size), 0)
    col = lax.broadcasted_iota(jnp.int32, (size, size), 1)
    unit = jnp.where(row == col, 1.0, 0.0)
    inner = jnp.where(row // base == col // base, lower, 0.0)
    inverse = unit - inner
    power, reach = inner, 2
    while reach < base:
        power = exact(power, power)
        inverse = inverse + exact(inverse, power)
        reach *= 2
    block = base
    while block < size:
        joint = (row // (2 * block) == col // (2 * block)) & (row // block != col // block)
        inverse = inverse - exact(exact(inverse, jnp.where(joint, lower, 0.0)), inverse)
        block *= 2
    return inverse


def delta_mix(decay_own, fine, ext, gain, first_gate, heads):
    seq_count, span, _ = fine.shape
    tile = math.gcd(span, 128)

    def one(raw_query, raw_key, raw_value, beta_pre, decay_pre, rate, gain_row):
        query = unit_rows(jax.nn.silu(raw_query)) * HEAD ** (-0.5)
        key = unit_rows(jax.nn.silu(raw_key))
        value = jax.nn.silu(raw_value)
        beta = jax.nn.sigmoid(beta_pre)
        log_decay = -rate * jax.nn.softplus(decay_pre)
        row = lax.broadcasted_iota(jnp.int32, (span, span), 0)
        col = lax.broadcasted_iota(jnp.int32, (span, span), 1)
        as_row = jnp.sum(jnp.where(row == col, log_decay, 0.0), axis=0, keepdims=True)
        gate = jnp.sum(jnp.where(row >= col, as_row, 0.0), axis=1, keepdims=True)
        gate_row = jnp.sum(jnp.where(row == col, gate, 0.0), axis=0, keepdims=True)
        decay = jnp.where(row >= col, jnp.exp(jnp.where(row >= col, gate - gate_row, 0.0)), 0.0)
        lower = dot_t(key * beta, key, HIGHEST) * jnp.where(row > col, decay, 0.0)
        scores = dot_t(query, key, HIGHEST) * decay
        wanted = value * beta
        solved = []
        for j in range(span // tile):
            rows = slice(j * tile, (j + 1) * tile)
            rest = wanted[rows]
            if j:
                rest = rest - exact(lower[rows, : j * tile], jnp.concatenate(solved, axis=0))
            solved.append(exact(lower_inverse(lower[rows, rows], 8), rest))
        out = exact(scores, jnp.concatenate(solved, axis=0))
        return (out * rms_scale(out) * gain_row).astype(jnp.bfloat16)

    def body(rate_ref, fine_ref, ext_ref, gain_ref, out_ref):
        for n in range(seq_count):
            for h in range(heads):
                raw = [
                    fine_ref[n, :, (k * heads + h) * HEAD : (k * heads + h + 1) * HEAD].astype(
                        jnp.float32
                    )
                    for k in range(3)
                ]
                beta_pre = ext_ref[n, :, first_gate + h : first_gate + h + 1]
                decay_pre = ext_ref[n, :, first_gate + heads + h : first_gate + heads + h + 1]
                out_ref[n * span : (n + 1) * span, h * HEAD : (h + 1) * HEAD] = one(
                    *raw, beta_pre, decay_pre, rate_ref[h], gain_ref[...]
                )

    return kernel_call(
        body,
        jax.ShapeDtypeStruct((seq_count * span, heads * HEAD), jnp.bfloat16),
        (decay_own, fine, ext, gain),
        name="delta_mix",
    )


def latent_mix(pieces, ext, tables, gains, ups, q_cols, kv_cols, heads):
    seq_count, span, _ = ext.shape
    count = len(pieces)
    scale = (NOPE + ROPE) ** (-0.5)

    def body(*refs):
        piece_refs, refs = refs[:count], refs[count:]
        ext_ref, cos_ref, sin_ref, qg_ref, kg_ref, qup_ref, kup_ref, out_ref = refs
        row = lax.broadcasted_iota(jnp.int32, (span, span), 0) // BLOCK
        col = lax.broadcasted_iota(jnp.int32, (span, span), 1) // BLOCK
        allowed = col <= row
        cosine, sine = cos_ref[...], sin_ref[...]
        for n in range(seq_count):
            q_lat = jnp.concatenate([p[n, :, :q_cols] for p in piece_refs], axis=1)
            kv_lat = jnp.concatenate([p[n, :, q_cols:] for p in piece_refs], axis=1)
            q_lat, kv_lat = q_lat.astype(jnp.float32), kv_lat.astype(jnp.float32)
            q_norm = (q_lat * rms_scale(q_lat) * qg_ref[...]).astype(jnp.bfloat16)
            kv_norm = (kv_lat * rms_scale(kv_lat) * kg_ref[...]).astype(jnp.bfloat16)
            q_all = dot32(q_norm, qup_ref[...]).astype(jnp.bfloat16)
            kv_all = dot32(kv_norm, kup_ref[...]).astype(jnp.bfloat16)
            plain_width, turn_width = heads * NOPE, heads * ROPE
            plain = q_all[:, :plain_width]
            turn = q_all[:, plain_width : plain_width + turn_width].astype(jnp.float32)
            swapped = q_all[:, plain_width + turn_width :].astype(jnp.float32)
            turned = (turn * cosine + swapped * sine).astype(jnp.bfloat16)
            raw = ext_ref[n, :, : 2 * ROPE].astype(jnp.bfloat16).astype(jnp.float32)
            key_turn = (raw[:, :ROPE] * cosine[:, :ROPE] + raw[:, ROPE:] * sine[:, :ROPE]).astype(
                jnp.bfloat16
            )
            results = []
            for h in range(heads):
                key_plain = kv_all[:, h * (NOPE + VDIM) : h * (NOPE + VDIM) + NOPE]
                values = kv_all[:, h * (NOPE + VDIM) + NOPE : (h + 1) * (NOPE + VDIM)]
                logits = (
                    dot_t(plain[:, h * NOPE : (h + 1) * NOPE], key_plain)
                    + dot_t(turned[:, h * ROPE : (h + 1) * ROPE], key_turn)
                ) * scale
                logits = jnp.where(allowed, logits, -jnp.inf)
                peak = jnp.max(logits, axis=-1, keepdims=True)
                weights = jnp.exp(logits - peak)
                total = jnp.sum(weights, axis=-1, keepdims=True)
                results.append(dot32(weights.astype(jnp.bfloat16), values) / total)
            out_ref[n * span : (n + 1) * span, :] = jnp.concatenate(results, axis=1).astype(
                jnp.bfloat16
            )

    return kernel_call(
        body,
        jax.ShapeDtypeStruct((seq_count * span, heads * VDIM), jnp.bfloat16),
        (*pieces, ext, *tables, *gains, *ups),
        scalars=0,
        name="latent_mix",
    )


def output_partial(ids, delta_pieces, latent_pieces, weights, sizes):
    sp_size, seq_count, token_count = sizes
    span = sp_size * token_count
    rows, d_width = delta_pieces[0].shape
    l_width = latent_pieces[0].shape[1]
    d_total, l_total = d_width * sp_size, l_width * sp_size
    columns = weights[0].shape[1]

    def body(ids_ref, *refs):
        d_refs, refs = refs[:sp_size], refs[sp_size:]
        l_refs, refs = refs[:sp_size], refs[sp_size:]
        d_own, d_other, l_own, l_other, out_ref, lhs_ref = refs
        place, fs_at = ids_ref[0], ids_ref[1]
        for j in range(sp_size):
            source = lax.rem(place + j, sp_size)
            lhs_ref[:, pl.ds(pl.multiple_of(source * d_width, d_width), d_width)] = d_refs[j][...]
            lhs_ref[:, pl.ds(pl.multiple_of(d_total + source * l_width, l_width), l_width)] = (
                l_refs[j][...]
            )
        for d_ref, l_ref, at in ((d_own, l_own, fs_at), (d_other, l_other, 1 - fs_at)):
            value = dot32(lhs_ref[:, :d_total], d_ref[...]) + dot32(
                lhs_ref[:, d_total:], l_ref[...]
            )
            value = value.astype(jnp.bfloat16)
            begin = pl.multiple_of(at * columns, columns)
            for n in range(seq_count):
                for j in range(sp_size):
                    first = n * span + j * token_count
                    out_ref[
                        j, n * token_count : (n + 1) * token_count, pl.ds(begin, columns)
                    ] = value[first : first + token_count]

    return kernel_call(
        body,
        jax.ShapeDtypeStruct((sp_size, seq_count * token_count, 2 * columns), jnp.bfloat16),
        (ids, *delta_pieces, *latent_pieces, *weights),
        scratch=(pltpu.VMEM((rows, d_total + l_total), jnp.bfloat16),),
        name="output_partial",
    )


def whole_sequences(
    tokens,
    pre_gain,
    query_weight,
    key_weight,
    value_weight,
    beta_weight,
    decay_weight,
    decay_rate,
    delta_gain,
    query_down,
    latent_down,
    rope_weight,
    query_gain,
    latent_gain,
    query_up,
    latent_up,
    delta_out,
    latent_out,
    post_gain,
):
    f32, bf16 = jnp.float32, jnp.bfloat16
    sp_size, tp_size = lax.axis_size("sp"), lax.axis_size("tp")
    place, fs_at = lax.axis_index("sp"), lax.axis_index("fs")
    grp_at, tp_at = lax.axis_index("grp"), lax.axis_index("tp")
    ids = jnp.stack([place, fs_at, grp_at, tp_at]).astype(jnp.int32)
    seq_count, token_count, width = tokens.shape
    rows = seq_count * token_count
    heads = query_weight.shape[1] // HEAD // sp_size
    own_width = heads * HEAD
    half = query_weight.shape[0] // 2
    shares = sp_size * tp_size
    q_cols, kv_cols = query_down.shape[1] // shares, latent_down.shape[1] // shares

    def from_sp(value_for):
        return [
            lax.ppermute(value_for(step), "sp", shift(sp_size, step))
            for step in range(sp_size - 1, 0, -1)
        ]

    def swap(values, axis):
        return lax.ppermute(values, axis, shift(2, 1))

    def cut(array):
        return lax.dynamic_slice_in_dim(array, grp_at * half, half, 0)

    def by_place(array, per):
        return jnp.moveaxis(cut(array).reshape(half, sp_size, per), 1, 0)

    def lat_columns(array, per):
        shaped = cut(array).reshape(half, sp_size, tp_size, per)
        return jnp.moveaxis(lax.dynamic_index_in_dim(shaped, tp_at, 2, False), 1, 0)

    outgoing = jnp.concatenate(
        [by_place(w, own_width) for w in (query_weight, key_weight, value_weight)]
        + [lat_columns(query_down, q_cols), lat_columns(latent_down, kv_cols)],
        axis=2,
    )
    received = from_sp(lambda step: pick(outgoing, lax.rem(place + step, sp_size)))

    def spread(block):
        middle = block.shape[0] // 2
        by_fs, by_grp = swap(block, "fs"), swap(block, "grp")
        return (
            block,
            by_fs,
            by_grp,
            swap(by_grp[:middle], "fs"),
            swap(by_fs[middle:], "grp"),
        )

    blocks = spread(pick(outgoing, place)) + spread(jnp.concatenate(received, axis=0))

    sequence = tokens.reshape(rows, width).astype(f32)
    normed = (sequence * rms_scale(sequence) * pre_gain).astype(bf16)
    part = width // tp_size
    normed_part = lax.dynamic_slice_in_dim(normed, tp_at * part, part, 1)
    mine = from_sp(lambda step: normed_part)
    theirs = [swap(piece, "tp") for piece in mine]

    delta_other, latent_other = swap(delta_out, "fs"), swap(latent_out, "fs")

    first_head = (tp_at * sp_size + place) * heads
    gates = [
        lax.dynamic_slice_in_dim(w, first_head, heads, 1) for w in (beta_weight, decay_weight)
    ]
    rope_half = rope_weight.shape[1] // 2
    swapped_rope = jnp.concatenate([rope_weight[:, rope_half:], rope_weight[:, :rope_half]], axis=1)
    filler = -(2 * ROPE + 2 * heads) % 128
    extra = jnp.concatenate(
        [rope_weight, swapped_rope, *gates, jnp.zeros((width, filler), bf16)], axis=1
    )
    rates = lax.dynamic_slice_in_dim(decay_rate, first_head, heads, 0)

    fine, lat, ext = project(
        ids,
        normed,
        mine,
        theirs,
        blocks,
        extra,
        (sp_size, seq_count, token_count, half, 3 * own_width, q_cols, kv_cols),
    )

    lat_mine = [lat] + from_sp(lambda step: lat)
    lat_pieces = []
    for piece in lat_mine:
        lat_pieces += [piece, swap(piece, "tp")]

    delta_heads = delta_mix(rates, fine, ext, delta_gain[None, :], 2 * ROPE, heads)
    delta_pieces = [delta_heads] + from_sp(lambda step: delta_heads)

    def in_received_order(array, per):
        shaped = array.reshape((sp_size, tp_size, per) + array.shape[1:])
        shaped = jnp.roll(shaped, -place, axis=0)
        shaped = jnp.where(tp_at == 0, shaped, shaped[:, ::-1])
        return shaped.reshape(array.shape)

    latent_heads = query_up.shape[1] // (NOPE + ROPE) // sp_size
    up = query_up.reshape(query_up.shape[0], sp_size, latent_heads, NOPE + ROPE)
    up = lax.dynamic_index_in_dim(up, place, 1, False)
    turn = up[..., NOPE:]
    back = jnp.concatenate([turn[..., ROPE // 2 :], turn[..., : ROPE // 2]], axis=-1)
    q_up = jnp.concatenate(
        [a.reshape(up.shape[0], -1) for a in (up[..., :NOPE], turn, back)], axis=1
    )
    q_up = in_received_order(q_up, q_cols)
    kv_width = latent_up.shape[1] // sp_size
    kv_up = lax.dynamic_slice_in_dim(latent_up, place * kv_width, kv_width, 1)
    kv_up = in_received_order(kv_up, kv_cols)
    gains = (
        in_received_order(query_gain, q_cols)[None, :],
        in_received_order(latent_gain, kv_cols)[None, :],
    )
    cosine, sine = rope_tables(jnp.arange(sp_size * token_count), ROPE)
    tables = (
        jnp.tile(jnp.concatenate([cosine, cosine], axis=1), (1, latent_heads)),
        jnp.tile(jnp.concatenate([-sine, sine], axis=1), (1, latent_heads)),
    )
    latent = latent_mix(lat_pieces, ext, tables, gains, (q_up, kv_up), q_cols, kv_cols, latent_heads)
    latent_pieces = [latent] + from_sp(lambda step: latent)

    partial = output_partial(
        ids,
        delta_pieces,
        latent_pieces,
        (delta_out, delta_other, latent_out, latent_other),
        (sp_size, seq_count, token_count),
    )
    mixed = partial.astype(f32) + swap(partial, "tp").astype(f32)
    mixed_b = mixed.astype(bf16)
    per_tp = sp_size // tp_size
    ends = []
    for step in range(sp_size - 1, 0, -1):
        pairs = []
        for source in range(sp_size):
            core = source // per_tp
            target = (source + step) % sp_size
            pairs.append((source * tp_size + core, target * tp_size + core))
        ends.append(
            lax.ppermute(pick(mixed_b, lax.rem(place + step, sp_size)), ("sp", "tp"), pairs)
        )
    stacked = jnp.stack([pick(mixed_b, place)] + ends)
    final = jnp.concatenate(
        [
            pick(stacked, lax.rem(tp_at * per_tp + k + sp_size - place, sp_size))
            for k in range(per_tp)
        ],
        axis=1,
    ).astype(f32)
    squares = jnp.sum(final * final, axis=1, keepdims=True)
    squares = squares + swap(squares, "tp")
    result = final * lax.rsqrt(squares / D + NORM_EPS) * post_gain
    return result.astype(bf16).reshape(seq_count, token_count, final.shape[1])


def fits_whole(mesh):
    shape = mesh.shape
    pairs = all(shape[name] == 2 for name in ("grp", "fs", "tp"))
    return pairs and shape["sp"] % shape["tp"] == 0


def solution(mesh):
    def chosen(*args):
        head_count = args[2].shape[1] // HEAD
        latent_count = args[14].shape[1] // (NOPE + ROPE)
        sp_size = mesh.shape["sp"]
        whole = fits_whole(mesh) and head_count % sp_size == 0 and latent_count % sp_size == 0
        return (whole_sequences if whole else local)(*args)

    return jax.shard_map(
        chosen,
        mesh=mesh,
        in_specs=(
            P(("grp", "fs"), "sp", None),
            P(),
            P(("sp", "fs"), "tp"),
            P(("sp", "fs"), "tp"),
            P(("sp", "fs"), "tp"),
            P(),
            P(),
            P(),
            P(),
            P(("sp", "fs"), None),
            P(("sp", "fs"), None),
            P(),
            P(),
            P(),
            P(None, "tp"),
            P(None, "tp"),
            P("tp", ("sp", "fs")),
            P("tp", ("sp", "fs")),
            P("tp"),
        ),
        out_specs=P(("grp", "fs"), "sp", "tp"),
        check_vma=False,
    )
```

```python
import math

import jax
import jax.numpy as jnp
from jax import lax
from jax.experimental import pallas as pl
from jax.experimental.pallas import tpu as pltpu
from jax.sharding import PartitionSpec as P

D = 2048
HEAD = 128
NOPE = 64
ROPE = 32
VDIM = 64
BLOCK = 64


NORM_EPS = 1e-06
ROPE_THETA = 10000.0
HIGHEST = lax.Precision.HIGHEST


def prefix(array, axis, join, neutral):
    place = lax.axis_index(axis)
    gathered = jax.tree.map(
        lambda a, kind: lax.all_gather(a.astype(kind), axis), array, (jnp.bfloat16, jnp.bfloat16)
    )
    state = jax.tree.map(lambda a, e: jnp.zeros_like(a) + jnp.asarray(e, a.dtype), array, neutral)

    def one(step, state):
        return join(
            state,
            jax.tree.map(
                lambda a, own: lax.dynamic_index_in_dim(a, step, 0, False).astype(own.dtype),
                gathered,
                array,
            ),
        )

    return lax.fori_loop(0, place, one, state)


def stored(values):
    return lax.optimization_barrier(values.astype(jnp.bfloat16))


def rms_scale(values):
    return lax.rsqrt(jnp.mean(values * values, axis=-1, keepdims=True) + NORM_EPS)


def unit_rows(values):
    return values * lax.rsqrt(jnp.sum(values * values, axis=-1, keepdims=True) + NORM_EPS)


def rope_tables(positions, rope_width):
    frequency = ROPE_THETA ** (-jnp.arange(0, rope_width, 2, dtype=jnp.float32) / rope_width)
    angles = positions.astype(jnp.float32)[:, None] * frequency[None, :]
    return (jnp.cos(angles), jnp.sin(angles))


def rotate(values, cosine_table, sine_table):
    lower_half, upper_half = jnp.split(values, 2, axis=-1)
    return jnp.concatenate(
        [
            lower_half * cosine_table - upper_half * sine_table,
            upper_half * cosine_table + lower_half * sine_table,
        ],
        axis=-1,
    )


def delta_terms(query_vectors, key_vectors, value_vectors, beta_gate, log_decay):
    length, head_count, head_width = query_vectors.shape
    nblocks = length // BLOCK

    def split_blocks(tensor):
        return jnp.moveaxis(tensor.reshape((nblocks, BLOCK, head_count) + tensor.shape[2:]), 2, 0)

    query_vectors = split_blocks(query_vectors)
    key_vectors = split_blocks(key_vectors)
    value_vectors = split_blocks(value_vectors)
    beta_gate = split_blocks(beta_gate)
    gate_sum = jnp.cumsum(split_blocks(log_decay), axis=-1)
    position = jnp.arange(BLOCK)
    strict = position[:, None] > position[None, :]
    causal = position[:, None] >= position[None, :]
    gate_gap = gate_sum[..., :, None] - gate_sum[..., None, :]
    strict_decay = jnp.where(strict, jnp.exp(jnp.where(strict, gate_gap, 0.0)), 0.0)
    causal_decay = jnp.where(causal, jnp.exp(jnp.where(causal, gate_gap, 0.0)), 0.0)
    keys_scaled = key_vectors * beta_gate[..., None]
    lower_mat = (
        jnp.einsum("hnid,hnjd->hnij", keys_scaled, key_vectors, precision=HIGHEST) * strict_decay
    )
    identity = jnp.eye(BLOCK, dtype=jnp.float32)
    inverse = jax.scipy.linalg.solve_triangular(
        identity + lower_mat, jnp.broadcast_to(identity, lower_mat.shape), lower=True
    )
    new_values = jnp.einsum(
        "hnij,hnjd->hnid", inverse, value_vectors * beta_gate[..., None], precision=HIGHEST
    )
    key_weights = jnp.einsum(
        "hnij,hnjd->hnid", inverse, keys_scaled * jnp.exp(gate_sum)[..., None], precision=HIGHEST
    )
    scores = (
        jnp.einsum("hnid,hnjd->hnij", query_vectors, key_vectors, precision=HIGHEST) * causal_decay
    )
    last_gate = gate_sum[..., -1]
    query_decay = query_vectors * jnp.exp(gate_sum)[..., None]
    key_decay = key_vectors * jnp.exp(last_gate[..., None] - gate_sum)[..., None]
    return (query_decay, key_decay, new_values, key_weights, scores, last_gate)


def compose(earlier, following):
    return (
        jnp.einsum("hij,hjk->hik", following[0], earlier[0], precision=HIGHEST),
        jnp.einsum("hij,hjk->hik", following[0], earlier[1], precision=HIGHEST) + following[1],
    )


def keep_same(current):
    return current


def local(
    tokens,
    pre_gain,
    query_weight,
    key_weight,
    value_weight,
    beta_weight,
    decay_weight,
    decay_rate,
    delta_gain,
    query_down,
    latent_down,
    rope_weight,
    query_gain,
    latent_gain,
    query_up,
    latent_up,
    delta_out,
    latent_out,
    post_gain,
):
    f32 = jnp.float32
    seq_count, token_count = (tokens.shape[0], tokens.shape[1])
    row_total = seq_count * token_count
    sequence = tokens.reshape(row_total, tokens.shape[2]).astype(f32)
    query_start = lax.axis_index("sp") * token_count
    positions = query_start + jnp.arange(token_count)
    normed = (sequence * rms_scale(sequence) * pre_gain).astype(jnp.bfloat16)
    head_group = lax.axis_index("tp")
    q_width = query_down.shape[1] // lax.axis_size("tp")
    kv_width = latent_down.shape[1] // lax.axis_size("tp")
    q_own = lax.dynamic_slice_in_dim(query_down, head_group * q_width, q_width, 1)
    kv_own = lax.dynamic_slice_in_dim(latent_down, head_group * kv_width, kv_width, 1)
    weights = (query_weight, key_weight, value_weight, q_own, kv_own)
    portion = (
        lax.all_gather(query_weight, ("sp", "fs"), axis=0, tiled=True),
        lax.all_gather(key_weight, ("sp", "fs"), axis=0, tiled=True),
        lax.all_gather(value_weight, ("sp", "fs"), axis=0, tiled=True),
        lax.all_gather(q_own, ("sp", "fs"), axis=0, tiled=True),
        lax.all_gather(kv_own, ("sp", "fs"), axis=0, tiled=True),
    )
    row_count = portion[0].shape[0]
    projected = tuple((jnp.dot(normed, weight, preferred_element_type=f32) for weight in portion))
    raw_query, raw_key, raw_value, q_half, kv_half = tuple((stored(member) for member in projected))
    q_latent, kv_latent = (
        lax.all_gather(q_half, "tp", axis=1, tiled=True),
        lax.all_gather(kv_half, "tp", axis=1, tiled=True),
    )
    head_count = query_weight.shape[1] // HEAD
    lane_count = seq_count * head_count
    beta_full = jax.nn.sigmoid(jnp.dot(normed, beta_weight, preferred_element_type=f32))
    beta_gate = lax.dynamic_slice_in_dim(beta_full, head_group * head_count, head_count, 1)
    decay_full = jnp.dot(normed, decay_weight, preferred_element_type=f32)
    decay_pre = lax.dynamic_slice_in_dim(decay_full, head_group * head_count, head_count, 1)
    decay_local = lax.dynamic_slice_in_dim(decay_rate, head_group * head_count, head_count, 0)
    log_decay = -decay_local[None, :] * jax.nn.softplus(decay_pre)

    def by_position(values):
        shaped = values.reshape((seq_count, token_count) + values.shape[1:])
        shaped = jnp.moveaxis(shaped, 0, 1)
        return shaped.reshape((token_count, seq_count * values.shape[1]) + values.shape[2:])

    query_vectors = by_position(
        unit_rows(jax.nn.silu(raw_query.astype(f32)).reshape(row_total, head_count, HEAD))
        * HEAD ** (-0.5)
    )
    key_vectors = by_position(
        unit_rows(jax.nn.silu(raw_key.astype(f32)).reshape(row_total, head_count, HEAD))
    )
    value_vectors = by_position(
        jax.nn.silu(raw_value.astype(f32)).reshape(row_total, head_count, HEAD)
    )
    block_terms = delta_terms(
        query_vectors, key_vectors, value_vectors, by_position(beta_gate), by_position(log_decay)
    )
    inputs = tuple((jnp.moveaxis(tensor, 1, 0) for tensor in block_terms))

    def advance(totals, block_in):
        carried, transfer = totals
        query_decay, key_decay, new_values, key_weights, scores, last_gate = block_in
        corrected = new_values - jnp.einsum("hcd,hde->hce", key_weights, carried, precision=HIGHEST)
        output = jnp.einsum("hcd,hde->hce", query_decay, carried, precision=HIGHEST) + jnp.einsum(
            "hij,hje->hie", scores, corrected, precision=HIGHEST
        )
        reader_rows = query_decay - jnp.einsum(
            "hij,hjd->hid", scores, key_weights, precision=HIGHEST
        )
        reader = jnp.einsum("hcd,hde->hce", reader_rows, transfer, precision=HIGHEST)
        factor = jnp.exp(last_gate)[:, None, None]
        carried = carried * factor + jnp.einsum(
            "hcd,hce->hde", key_decay, corrected, precision=HIGHEST
        )
        moved = jnp.einsum("hcd,hde->hce", key_weights, transfer, precision=HIGHEST)
        transfer = transfer * factor - jnp.einsum(
            "hcd,hce->hde", key_decay, moved, precision=HIGHEST
        )
        return ((carried, transfer), (output, reader))

    eye_stack = jnp.broadcast_to(jnp.eye(HEAD, dtype=f32), (lane_count, HEAD, HEAD))
    zero_state = jnp.zeros((lane_count, HEAD, HEAD), f32)
    (state_end, transfer_end), (outputs, readers) = lax.scan(
        advance, (zero_state, eye_stack), inputs
    )
    _, incoming = prefix((transfer_end, state_end), "sp", compose, (eye_stack, zero_state))
    outputs = outputs + jnp.einsum("nhcd,hde->nhce", readers, incoming, precision=HIGHEST)
    delta_raw = jnp.transpose(outputs, (0, 2, 1, 3)).reshape(
        token_count, seq_count, head_count, HEAD
    )
    delta_raw = jnp.moveaxis(delta_raw, 1, 0).reshape(row_total, head_count, HEAD)
    delta_heads = (
        (delta_raw * rms_scale(delta_raw) * delta_gain)
        .astype(jnp.bfloat16)
        .reshape(row_total, head_count * HEAD)
    )
    q_lat32 = q_latent.astype(f32)
    kv_lat32 = kv_latent.astype(f32)
    q_normed = (q_lat32 * rms_scale(q_lat32) * query_gain).astype(jnp.bfloat16)
    kv_normed = (kv_lat32 * rms_scale(kv_lat32) * latent_gain).astype(jnp.bfloat16)
    rope_raw = stored(jnp.dot(normed, rope_weight, preferred_element_type=f32))
    cosine_table, sine_table = rope_tables(positions, rope_raw.shape[1])
    rope_keys = rotate(
        rope_raw.astype(f32).reshape(seq_count, token_count, rope_raw.shape[1]),
        cosine_table,
        sine_table,
    ).astype(jnp.bfloat16)
    latent_count = query_up.shape[1] // (NOPE + ROPE)
    query_all = stored(jnp.dot(q_normed, query_up, preferred_element_type=f32)).reshape(
        seq_count, token_count, latent_count, NOPE + ROPE
    )
    query_plain = query_all[..., :NOPE]
    query_turned = rotate(
        query_all[..., NOPE:].astype(f32), cosine_table[:, None, :], sine_table[:, None, :]
    ).astype(jnp.bfloat16)
    score_scale = (NOPE + ROPE) ** (-0.5)
    query_block = positions // BLOCK
    kv_seq = kv_normed.reshape(seq_count, token_count, kv_normed.shape[1])

    def attend_block(totals, key_plain, value_rows, rope_rows, key_start):
        row_max, row_sum, weighted = totals
        key_block = (key_start + jnp.arange(key_plain.shape[1])) // BLOCK
        allowed = key_block[None, :] <= query_block[:, None]
        logits = (
            jnp.einsum("sqhd,skhd->shqk", query_plain, key_plain, preferred_element_type=f32)
            + jnp.einsum("sqhd,skd->shqk", query_turned, rope_rows, preferred_element_type=f32)
        ) * score_scale
        logits = jnp.where(allowed[None, None], logits, -jnp.inf)
        new_max = jnp.maximum(row_max, jnp.max(logits, axis=-1))
        shift = jnp.where(jnp.isfinite(new_max), new_max, 0.0)
        weights = jnp.where(allowed[None, None], jnp.exp(logits - shift[..., None]), 0.0)
        rescale = jnp.exp(row_max - shift)
        row_sum = row_sum * rescale + jnp.sum(weights, axis=-1)
        weighted = weighted * rescale[..., None] + jnp.einsum(
            "shqk,skhd->shqd", weights.astype(jnp.bfloat16), value_rows, preferred_element_type=f32
        )
        return (new_max, row_sum, weighted)

    start_stats = (
        jnp.full((seq_count, latent_count, token_count), -jnp.inf, f32),
        jnp.zeros((seq_count, latent_count, token_count), f32),
        jnp.zeros((seq_count, latent_count, token_count, VDIM), f32),
    )

    def expand_latent(portion, row_start, span_rows):
        latent_rows = lax.dynamic_slice_in_dim(portion[0], row_start, span_rows, 1)
        expanded = jnp.dot(
            latent_rows.reshape(seq_count * span_rows, latent_rows.shape[2]),
            latent_up,
            preferred_element_type=f32,
        ).astype(jnp.bfloat16)
        expanded = expanded.reshape(seq_count, span_rows, latent_count, NOPE + VDIM)
        return (
            expanded[..., :NOPE],
            expanded[..., NOPE:],
            lax.dynamic_slice_in_dim(portion[1], row_start, span_rows, 1),
        )

    portion = (
        lax.all_gather(kv_seq, "sp", axis=1, tiled=True),
        lax.all_gather(rope_keys, "sp", axis=1, tiled=True),
    )
    row_count = portion[0].shape[1]
    span_rows = math.gcd(row_count, token_count * max(1, 512 // token_count))

    def visit_rows(current):

        def visit_block(block_index, stats):
            row_start = block_index * span_rows
            key_plain, value_rows, rope_rows = expand_latent(portion, row_start, span_rows)
            return attend_block(stats, key_plain, value_rows, rope_rows, row_start)

        return lax.fori_loop(0, row_count // span_rows, visit_block, current)

    row_max, row_sum, weighted = lax.cond(
        jnp.int32(0) < query_start + token_count, visit_rows, keep_same, start_stats
    )
    latent_heads = (
        jnp.transpose(weighted / row_sum[..., None], (0, 2, 1, 3))
        .reshape(row_total, latent_count * VDIM)
        .astype(jnp.bfloat16)
    )
    heads_joined = jnp.concatenate([delta_heads, latent_heads], axis=1)
    out_rows = jnp.concatenate([delta_out, latent_out], axis=0)
    partial_value = jnp.dot(
        heads_joined,
        lax.all_gather(out_rows, ("sp", "fs"), axis=1, tiled=True),
        preferred_element_type=f32,
    )
    mixed_half = lax.psum_scatter(
        partial_value.astype(jnp.bfloat16), "tp", scatter_dimension=1, tiled=True
    ).astype(jnp.float32)
    squares = lax.psum(jnp.sum(mixed_half * mixed_half, axis=1), "tp")
    row_scale = lax.rsqrt(squares / D + NORM_EPS)
    result = mixed_half * row_scale[:, None] * post_gain
    return result.astype(jnp.bfloat16).reshape(seq_count, token_count, result.shape[1])


def pick(array, index):
    return lax.dynamic_index_in_dim(array, index, 0, False)


def dot32(left, right):
    return jnp.dot(left, right, preferred_element_type=jnp.float32)


def dot_t(left, right):
    return lax.dot_general(
        left, right, (((1,), (1,)), ((), ())), preferred_element_type=jnp.float32
    )


def two_parts(values):
    high = values.astype(jnp.bfloat16)
    return high, (values - high.astype(jnp.float32)).astype(jnp.bfloat16)


def fine_dot(left, right, product=dot32):
    left_high, left_low = two_parts(left)
    right_high, right_low = two_parts(right)
    return product(left_high, right_high) + (
        product(left_high, right_low) + product(left_low, right_high)
    )


def kernel_call(body, out_shapes, args, scratch=(), scalars=1, name=None):
    specs = [
        pl.BlockSpec(memory_space=pltpu.SMEM if i < scalars else pltpu.VMEM)
        for i in range(len(args))
    ]
    return pl.pallas_call(
        body,
        out_shape=out_shapes,
        in_specs=specs,
        out_specs=jax.tree.map(lambda _: pl.BlockSpec(memory_space=pltpu.VMEM), out_shapes),
        scratch_shapes=scratch,
        name=name,
        compiler_params=pltpu.CompilerParams(vmem_limit_bytes=56 * 1024 * 1024),
    )(*args)


def outgoing_weights(ids, mixers, lats, sp_size):
    half = mixers[0].shape[0] // 2
    per_mixer = mixers[0].shape[1] // sp_size
    per_lat = [w.shape[1] // sp_size // 2 for w in lats]
    columns = len(mixers) * per_mixer + sum(per_lat)

    def body(ids_ref, *refs):
        rows = pl.ds(pl.multiple_of(ids_ref[2] * half, half), half)
        first = ids_ref[3] == 0
        out_ref = refs[-1]
        for s in range(sp_size):
            begin = 0
            for ref in refs[: len(mixers)]:
                out_ref[s, :, begin : begin + per_mixer] = ref[
                    rows, s * per_mixer : (s + 1) * per_mixer
                ]
                begin += per_mixer
            for ref, per in zip(refs[len(mixers) : -1], per_lat):
                pair = ref[rows, 2 * s * per : 2 * (s + 1) * per]
                out_ref[s, :, begin : begin + per] = jnp.where(first, pair[:, :per], pair[:, per:])
                begin += per

    return kernel_call(
        body,
        jax.ShapeDtypeStruct((sp_size, half, columns), jnp.bfloat16),
        (ids, *mixers, *lats),
        name="outgoing_weights",
    )


def outgoing_tokens(ids, tokens, gain, sp_size):
    rows, width = tokens.shape
    block = width // (sp_size * 4)

    def body(ids_ref, token_ref, gain_ref, out_ref):
        values = token_ref[...].astype(jnp.float32)
        normed = (values * rms_scale(values) * gain_ref[...]).astype(jnp.bfloat16)
        first = ids_ref[3] == 0
        for f in range(2):
            for s in range(sp_size):
                begin = (s * 2 + f) * 2 * block
                piece = jnp.where(
                    first,
                    normed[:, begin : begin + block],
                    normed[:, begin + block : begin + 2 * block],
                )
                at = (f * sp_size + s) * block
                for n in range(sp_size):
                    out_ref[n, :, at : at + block] = piece

    return kernel_call(
        body,
        jax.ShapeDtypeStruct((sp_size, rows, width // 2), jnp.bfloat16),
        (ids, tokens, gain),
        name="outgoing_tokens",
    )


def project(ids, mine, theirs, weights, extra, sizes):
    seq_count, token_count, fine, q_cols, kv_cols = sizes
    sp_size, rows, part = mine.shape
    span = sp_size * token_count
    extra_width = extra.shape[1]

    def body(ids_ref, mine_ref, their_ref, weight_ref, extra_ref, fine_ref, lat_ref, ext_ref):
        mine_at = pl.ds(pl.multiple_of(ids_ref[3] * part, part), part)
        their_at = pl.ds(pl.multiple_of((1 - ids_ref[3]) * part, part), part)
        for s in range(sp_size):
            value = dot32(mine_ref[s], weight_ref[mine_at, :])
            value = (value + dot32(their_ref[s], weight_ref[their_at, :])).astype(jnp.bfloat16)
            outer = dot32(mine_ref[s], extra_ref[mine_at, :])
            outer = outer + dot32(their_ref[s], extra_ref[their_at, :])
            for n in range(seq_count):
                cut = slice(n * token_count, (n + 1) * token_count)
                at = slice(s * token_count, (s + 1) * token_count)
                fine_ref[n, at, :] = value[cut, :fine]
                ext_ref[n, at, :] = outer[cut]
                for j in range(sp_size):
                    lat_ref[j, n, at, :] = value[cut, fine:]

    return kernel_call(
        body,
        (
            jax.ShapeDtypeStruct((seq_count, span, fine), jnp.bfloat16),
            jax.ShapeDtypeStruct((sp_size, seq_count, span, q_cols + kv_cols), jnp.bfloat16),
            jax.ShapeDtypeStruct((seq_count, span, extra_width), jnp.float32),
        ),
        (ids, mine, theirs, weights, extra),
        name="project",
    )


def lower_inverses(lowers, base):
    size = lowers[0].shape[0]
    row = lax.broadcasted_iota(jnp.int32, (size, size), 0)
    col = lax.broadcasted_iota(jnp.int32, (size, size), 1)
    unit = jnp.where(row == col, 1.0, 0.0)
    powers = [jnp.where(row // base == col // base, low, 0.0) for low in lowers]
    inverses = [unit - p for p in powers]
    reach = 2
    while reach < base:
        powers = [fine_dot(p, p) for p in powers]
        inverses = [i + fine_dot(i, p) for i, p in zip(inverses, powers)]
        reach *= 2
    block = base
    while block < size:
        joint = (row // (2 * block) == col // (2 * block)) & (row // block != col // block)
        moved = [fine_dot(i, jnp.where(joint, low, 0.0)) for i, low in zip(inverses, lowers)]
        inverses = [i - fine_dot(m, i) for i, m in zip(inverses, moved)]
        block *= 2
    return inverses


def delta_mix(scalars, fine, ext, gain, rates, gate_at, heads, copies):
    seq_count, span, _ = fine.shape
    tile = math.gcd(span, 128)
    tiles = span // tile
    gates = rates.shape[1]

    def terms(raw_query, raw_key, raw_value, beta_pre, decay_pre, rate):
        query = unit_rows(jax.nn.silu(raw_query)) * HEAD ** (-0.5)
        key = unit_rows(jax.nn.silu(raw_key))
        value = jax.nn.silu(raw_value)
        beta = jax.nn.sigmoid(beta_pre)
        log_decay = -rate * jax.nn.softplus(decay_pre)
        row = lax.broadcasted_iota(jnp.int32, (span, span), 0)
        col = lax.broadcasted_iota(jnp.int32, (span, span), 1)
        as_row = jnp.sum(jnp.where(row == col, log_decay, 0.0), axis=0, keepdims=True)
        gate = jnp.sum(jnp.where(row >= col, as_row, 0.0), axis=1, keepdims=True)
        gate_row = jnp.sum(jnp.where(row == col, gate, 0.0), axis=0, keepdims=True)
        decay = jnp.where(row >= col, jnp.exp(jnp.where(row >= col, gate - gate_row, 0.0)), 0.0)
        lower = fine_dot(key * beta, key, dot_t) * jnp.where(row > col, decay, 0.0)
        scores = fine_dot(query, key, dot_t) * decay
        return lower, scores, value * beta

    def body(ids_ref, fine_ref, ext_ref, gain_ref, rate_ref, out_ref):
        lane = lax.broadcasted_iota(jnp.int32, (span, ext.shape[2]), 1)
        rate_lane = lax.broadcasted_iota(jnp.int32, (1, gates), 1)
        chains = []
        for n in range(seq_count):
            for h in range(heads):
                raw = [
                    fine_ref[n, :, (k * heads + h) * HEAD : (k * heads + h + 1) * HEAD].astype(
                        jnp.float32
                    )
                    for k in range(3)
                ]
                head = ids_ref[4] + h
                outer = ext_ref[n]
                beta_pre, decay_pre = (
                    jnp.sum(
                        jnp.where(lane == gate_at + k * gates + head, outer, 0.0),
                        axis=1,
                        keepdims=True,
                    )
                    for k in range(2)
                )
                rate = jnp.sum(
                    jnp.where(rate_lane == head, rate_ref[...], 0.0), axis=1, keepdims=True
                )
                chains.append(terms(*raw, beta_pre, decay_pre, rate))
        cuts = [slice(j * tile, (j + 1) * tile) for j in range(tiles)]
        inverses = lower_inverses([c[0][cut, cut] for c in chains for cut in cuts], 8)
        solved = [[] for _ in chains]
        for j, cut in enumerate(cuts):
            for i, (lower, _, wanted) in enumerate(chains):
                rest = wanted[cut]
                if j:
                    rest = rest - fine_dot(
                        lower[cut, : j * tile], jnp.concatenate(solved[i], axis=0)
                    )
                solved[i].append(fine_dot(inverses[i * tiles + j], rest))
        for i, (_, scores, _) in enumerate(chains):
            n, h = divmod(i, heads)
            out = fine_dot(scores, jnp.concatenate(solved[i], axis=0))
            out = (out * rms_scale(out) * gain_ref[...]).astype(jnp.bfloat16)
            for j in range(copies):
                out_ref[j, n * span : (n + 1) * span, h * HEAD : (h + 1) * HEAD] = out

    return kernel_call(
        body,
        jax.ShapeDtypeStruct((copies, seq_count * span, heads * HEAD), jnp.bfloat16),
        (scalars, fine, ext, gain, rates),
        name="delta_mix",
    )


def latent_mix(ids, mine, theirs, ext, tables, gains, ups, q_cols, heads):
    sp_size, seq_count, span, _ = mine.shape
    scale = (NOPE + ROPE) ** (-0.5)

    def body(ids_ref, mine_ref, their_ref, ext_ref, cos_ref, sin_ref, *refs):
        qg_ref, kg_ref, qup_ref, kup_ref, out_ref = refs
        first = ids_ref[3] == 0
        row = lax.broadcasted_iota(jnp.int32, (span, span), 0) // BLOCK
        col = lax.broadcasted_iota(jnp.int32, (span, span), 1) // BLOCK
        allowed = col <= row
        cosine, sine = cos_ref[...], sin_ref[...]
        for n in range(seq_count):
            q_parts, kv_parts = [], []
            for s in range(sp_size):
                own, other = mine_ref[s, n], their_ref[s, n]
                pair = (jnp.where(first, own, other), jnp.where(first, other, own))
                q_parts += [p[:, :q_cols] for p in pair]
                kv_parts += [p[:, q_cols:] for p in pair]
            q_lat = jnp.concatenate(q_parts, axis=1).astype(jnp.float32)
            kv_lat = jnp.concatenate(kv_parts, axis=1).astype(jnp.float32)
            q_norm = (q_lat * rms_scale(q_lat) * qg_ref[...]).astype(jnp.bfloat16)
            kv_norm = (kv_lat * rms_scale(kv_lat) * kg_ref[...]).astype(jnp.bfloat16)
            q_all = dot32(q_norm, qup_ref[...]).astype(jnp.bfloat16)
            kv_all = dot32(kv_norm, kup_ref[...]).astype(jnp.bfloat16)
            plain_width, turn_width = heads * NOPE, heads * ROPE
            plain = q_all[:, :plain_width]
            turn = q_all[:, plain_width : plain_width + turn_width].astype(jnp.float32)
            swapped = q_all[:, plain_width + turn_width :].astype(jnp.float32)
            turned = (turn * cosine + swapped * sine).astype(jnp.bfloat16)
            raw = ext_ref[n, :, :ROPE].astype(jnp.bfloat16).astype(jnp.float32)
            back = jnp.concatenate([raw[:, ROPE // 2 :], raw[:, : ROPE // 2]], axis=1)
            key_turn = (raw * cosine[:, :ROPE] + back * sine[:, :ROPE]).astype(jnp.bfloat16)
            results = []
            for h in range(heads):
                key_plain = kv_all[:, h * (NOPE + VDIM) : h * (NOPE + VDIM) + NOPE]
                values = kv_all[:, h * (NOPE + VDIM) + NOPE : (h + 1) * (NOPE + VDIM)]
                logits = (
                    dot_t(plain[:, h * NOPE : (h + 1) * NOPE], key_plain)
                    + dot_t(turned[:, h * ROPE : (h + 1) * ROPE], key_turn)
                ) * scale
                logits = jnp.where(allowed, logits, -jnp.inf)
                peak = jnp.max(logits, axis=-1, keepdims=True)
                weights = jnp.exp(logits - peak)
                total = jnp.sum(weights, axis=-1, keepdims=True)
                results.append(dot32(weights.astype(jnp.bfloat16), values) / total)
            joined = jnp.concatenate(results, axis=1).astype(jnp.bfloat16)
            for j in range(sp_size):
                out_ref[j, n * span : (n + 1) * span, :] = joined

    return kernel_call(
        body,
        jax.ShapeDtypeStruct((sp_size, seq_count * span, heads * VDIM), jnp.bfloat16),
        (ids, mine, theirs, ext, *tables, *gains, *ups),
        name="latent_mix",
    )


def output_partial(ids, delta_all, latent_all, weights, sizes):
    seq_count, token_count = sizes
    sp_size, rows, d_width = delta_all.shape
    l_width = latent_all.shape[2]
    span = sp_size * token_count
    d_total, l_total = d_width * sp_size, l_width * sp_size
    columns = weights[0].shape[1]

    def body(ids_ref, d_ref, l_ref, d_own, d_other, l_own, l_other, keep_ref, pass_ref, lhs_ref):
        for s in range(sp_size):
            lhs_ref[:, s * d_width : (s + 1) * d_width] = d_ref[s]
            lhs_ref[:, d_total + s * l_width : d_total + (s + 1) * l_width] = l_ref[s]
        own = dot32(lhs_ref[:, :d_total], d_own[...]) + dot32(lhs_ref[:, d_total:], l_own[...])
        other = dot32(lhs_ref[:, :d_total], d_other[...]) + dot32(
            lhs_ref[:, d_total:], l_other[...]
        )
        own, other = own.astype(jnp.bfloat16), other.astype(jnp.bfloat16)
        straight = ids_ref[1] == ids_ref[3]
        keep, onward = jnp.where(straight, own, other), jnp.where(straight, other, own)
        for n in range(seq_count):
            for s in range(sp_size):
                first = n * span + s * token_count
                at = slice(n * token_count, (n + 1) * token_count)
                keep_ref[s, at, :] = keep[first : first + token_count]
                pass_ref[s, at, :] = onward[first : first + token_count]

    shape = jax.ShapeDtypeStruct((sp_size, seq_count * token_count, columns), jnp.bfloat16)
    return kernel_call(
        body,
        (shape, shape),
        (ids, delta_all, latent_all, *weights),
        scratch=(pltpu.VMEM((rows, d_total + l_total), jnp.bfloat16),),
        name="output_partial",
    )


def whole_sequences(
    tokens,
    pre_gain,
    query_weight,
    key_weight,
    value_weight,
    beta_weight,
    decay_weight,
    decay_rate,
    delta_gain,
    query_down,
    latent_down,
    rope_weight,
    query_gain,
    latent_gain,
    query_up,
    latent_up,
    delta_out,
    latent_out,
    post_gain,
):
    f32, bf16 = jnp.float32, jnp.bfloat16
    sp_size, tp_size = lax.axis_size("sp"), lax.axis_size("tp")
    place, fs_at = lax.axis_index("sp"), lax.axis_index("fs")
    grp_at, tp_at = lax.axis_index("grp"), lax.axis_index("tp")
    seq_count, token_count, width = tokens.shape
    rows = seq_count * token_count
    heads = query_weight.shape[1] // HEAD // sp_size
    first_head = (tp_at * sp_size + place) * heads
    ids = jnp.stack([place, fs_at, grp_at, tp_at, first_head]).astype(jnp.int32)
    shares = sp_size * tp_size
    q_cols, kv_cols = query_down.shape[1] // shares, latent_down.shape[1] // shares

    def exchange(values, axis):
        return lax.all_to_all(values, axis, 0, 0, tiled=True)

    def swap(values, axis):
        return lax.ppermute(values, axis, [(0, 1), (1, 0)])

    outgoing = outgoing_weights(
        ids, (query_weight, key_weight, value_weight), (query_down, latent_down), sp_size
    )
    block = exchange(outgoing, "sp")
    block = jnp.broadcast_to(block.reshape(1, -1, outgoing.shape[2]), (4,) + (block.shape[0] * block.shape[1], outgoing.shape[2]))
    weights = exchange(block, ("grp", "fs")).reshape(width, outgoing.shape[2])

    token_rows, outgoing = lax.optimization_barrier((tokens.reshape(rows, width), outgoing))
    mine = exchange(outgoing_tokens(ids, token_rows, pre_gain[None, :], sp_size), "sp")
    theirs = swap(mine, "tp")

    delta_other, latent_other = swap(delta_out, "fs"), swap(latent_out, "fs")

    gate_at = rope_weight.shape[1]
    filler = -(gate_at + 2 * beta_weight.shape[1]) % 128
    extra = jnp.concatenate(
        [rope_weight, beta_weight, decay_weight, jnp.zeros((width, filler), bf16)], axis=1
    )
    extra = extra.reshape(sp_size, 2, 2, width // (4 * sp_size), extra.shape[1])
    extra = jnp.transpose(extra, (2, 1, 0, 3, 4)).reshape(width, extra.shape[4])

    fine, lat, ext = project(
        ids,
        mine,
        theirs,
        weights,
        extra,
        (seq_count, token_count, 3 * heads * HEAD, q_cols, kv_cols),
    )
    lat_mine = exchange(lat, "sp")
    lat_theirs = swap(lat_mine, "tp")

    delta_heads = delta_mix(
        ids, fine, ext, delta_gain[None, :], decay_rate[None, :], gate_at, heads, sp_size
    )
    delta_all = exchange(delta_heads, "sp")

    latent_heads = query_up.shape[1] // (NOPE + ROPE) // sp_size
    up = query_up.reshape(query_up.shape[0], sp_size, latent_heads, NOPE + ROPE)
    up = lax.dynamic_index_in_dim(up, place, 1, False)
    turn = up[..., NOPE:]
    back = jnp.concatenate([turn[..., ROPE // 2 :], turn[..., : ROPE // 2]], axis=-1)
    q_up = jnp.concatenate(
        [a.reshape(up.shape[0], -1) for a in (up[..., :NOPE], turn, back)], axis=1
    )
    kv_width = latent_up.shape[1] // sp_size
    kv_up = lax.dynamic_slice_in_dim(latent_up, place * kv_width, kv_width, 1)
    cosine, sine = rope_tables(jnp.arange(sp_size * token_count), ROPE)
    tables = (
        jnp.tile(jnp.concatenate([cosine, cosine], axis=1), (1, latent_heads)),
        jnp.tile(jnp.concatenate([-sine, sine], axis=1), (1, latent_heads)),
    )
    latent = latent_mix(
        ids,
        lat_mine,
        lat_theirs,
        ext,
        tables,
        (query_gain[None, :], latent_gain[None, :]),
        (q_up, kv_up),
        q_cols,
        latent_heads,
    )
    latent_all = exchange(latent, "sp")

    keep, onward = output_partial(
        ids,
        delta_all,
        latent_all,
        (delta_out, delta_other, latent_out, latent_other),
        (seq_count, token_count),
    )
    mixed = (keep.astype(f32) + swap(onward, "tp").astype(f32)).astype(bf16)
    landed = exchange(mixed, "sp")
    per_tp = sp_size // tp_size
    squares = jnp.sum(landed.astype(f32) * landed.astype(f32), axis=(0, 2))[:, None]
    squares = squares + swap(squares, "tp")
    here = lax.dynamic_slice_in_dim(landed, tp_at * per_tp, per_tp, 0)
    there = swap(lax.dynamic_slice_in_dim(landed, (1 - tp_at) * per_tp, per_tp, 0), "tp")
    low, high = jnp.where(tp_at == 0, here, there), jnp.where(tp_at == 0, there, here)
    final = jnp.concatenate(
        [half[k] for k in range(per_tp) for half in (low, high)], axis=1
    ).astype(f32)
    result = final * lax.rsqrt(squares / D + NORM_EPS) * post_gain
    return result.astype(bf16).reshape(seq_count, token_count, final.shape[1])


def fits_whole(mesh):
    shape = mesh.shape
    pairs = all(shape[name] == 2 for name in ("grp", "fs", "tp"))
    return pairs and shape["sp"] % shape["tp"] == 0


def solution(mesh):
    def chosen(*args):
        head_count = args[2].shape[1] // HEAD
        latent_count = args[14].shape[1] // (NOPE + ROPE)
        sp_size = mesh.shape["sp"]
        whole = fits_whole(mesh) and head_count % sp_size == 0 and latent_count % sp_size == 0
        return (whole_sequences if whole else local)(*args)

    return jax.shard_map(
        chosen,
        mesh=mesh,
        in_specs=(
            P(("grp", "fs"), "sp", None),
            P(),
            P(("sp", "fs"), "tp"),
            P(("sp", "fs"), "tp"),
            P(("sp", "fs"), "tp"),
            P(),
            P(),
            P(),
            P(),
            P(("sp", "fs"), None),
            P(("sp", "fs"), None),
            P(),
            P(),
            P(),
            P(None, "tp"),
            P(None, "tp"),
            P("tp", ("sp", "fs")),
            P("tp", ("sp", "fs")),
            P("tp"),
        ),
        out_specs=P(("grp", "fs"), "sp", "tp"),
        check_vma=False,
    )
```

```python
import math

import jax
import jax.numpy as jnp
import numpy as np
from jax import lax
from jax.experimental import pallas as pl
from jax.experimental.pallas import tpu as pltpu
from jax.sharding import PartitionSpec as P

D = 2048
HEAD = 128
NOPE = 64
ROPE = 32
VDIM = 64
BLOCK = 64


NORM_EPS = 1e-06
ROPE_THETA = 10000.0
HIGHEST = lax.Precision.HIGHEST


def prefix(array, axis, join, neutral):
    place = lax.axis_index(axis)
    gathered = jax.tree.map(
        lambda a, kind: lax.all_gather(a.astype(kind), axis), array, (jnp.bfloat16, jnp.bfloat16)
    )
    state = jax.tree.map(lambda a, e: jnp.zeros_like(a) + jnp.asarray(e, a.dtype), array, neutral)

    def one(step, state):
        return join(
            state,
            jax.tree.map(
                lambda a, own: lax.dynamic_index_in_dim(a, step, 0, False).astype(own.dtype),
                gathered,
                array,
            ),
        )

    return lax.fori_loop(0, place, one, state)


def stored(values):
    return lax.optimization_barrier(values.astype(jnp.bfloat16))


def rms_scale(values):
    return lax.rsqrt(jnp.mean(values * values, axis=-1, keepdims=True) + NORM_EPS)


def unit_rows(values):
    return values * lax.rsqrt(jnp.sum(values * values, axis=-1, keepdims=True) + NORM_EPS)


def rope_tables(positions, rope_width):
    frequency = ROPE_THETA ** (-jnp.arange(0, rope_width, 2, dtype=jnp.float32) / rope_width)
    angles = positions.astype(jnp.float32)[:, None] * frequency[None, :]
    return (jnp.cos(angles), jnp.sin(angles))


def rotate(values, cosine_table, sine_table):
    lower_half, upper_half = jnp.split(values, 2, axis=-1)
    return jnp.concatenate(
        [
            lower_half * cosine_table - upper_half * sine_table,
            upper_half * cosine_table + lower_half * sine_table,
        ],
        axis=-1,
    )


def delta_terms(query_vectors, key_vectors, value_vectors, beta_gate, log_decay):
    length, head_count, head_width = query_vectors.shape
    nblocks = length // BLOCK

    def split_blocks(tensor):
        return jnp.moveaxis(tensor.reshape((nblocks, BLOCK, head_count) + tensor.shape[2:]), 2, 0)

    query_vectors = split_blocks(query_vectors)
    key_vectors = split_blocks(key_vectors)
    value_vectors = split_blocks(value_vectors)
    beta_gate = split_blocks(beta_gate)
    gate_sum = jnp.cumsum(split_blocks(log_decay), axis=-1)
    position = jnp.arange(BLOCK)
    strict = position[:, None] > position[None, :]
    causal = position[:, None] >= position[None, :]
    gate_gap = gate_sum[..., :, None] - gate_sum[..., None, :]
    strict_decay = jnp.where(strict, jnp.exp(jnp.where(strict, gate_gap, 0.0)), 0.0)
    causal_decay = jnp.where(causal, jnp.exp(jnp.where(causal, gate_gap, 0.0)), 0.0)
    keys_scaled = key_vectors * beta_gate[..., None]
    lower_mat = (
        jnp.einsum("hnid,hnjd->hnij", keys_scaled, key_vectors, precision=HIGHEST) * strict_decay
    )
    identity = jnp.eye(BLOCK, dtype=jnp.float32)
    inverse = jax.scipy.linalg.solve_triangular(
        identity + lower_mat, jnp.broadcast_to(identity, lower_mat.shape), lower=True
    )
    new_values = jnp.einsum(
        "hnij,hnjd->hnid", inverse, value_vectors * beta_gate[..., None], precision=HIGHEST
    )
    key_weights = jnp.einsum(
        "hnij,hnjd->hnid", inverse, keys_scaled * jnp.exp(gate_sum)[..., None], precision=HIGHEST
    )
    scores = (
        jnp.einsum("hnid,hnjd->hnij", query_vectors, key_vectors, precision=HIGHEST) * causal_decay
    )
    last_gate = gate_sum[..., -1]
    query_decay = query_vectors * jnp.exp(gate_sum)[..., None]
    key_decay = key_vectors * jnp.exp(last_gate[..., None] - gate_sum)[..., None]
    return (query_decay, key_decay, new_values, key_weights, scores, last_gate)


def compose(earlier, following):
    return (
        jnp.einsum("hij,hjk->hik", following[0], earlier[0], precision=HIGHEST),
        jnp.einsum("hij,hjk->hik", following[0], earlier[1], precision=HIGHEST) + following[1],
    )


def keep_same(current):
    return current


def local(
    tokens,
    pre_gain,
    query_weight,
    key_weight,
    value_weight,
    beta_weight,
    decay_weight,
    decay_rate,
    delta_gain,
    query_down,
    latent_down,
    rope_weight,
    query_gain,
    latent_gain,
    query_up,
    latent_up,
    delta_out,
    latent_out,
    post_gain,
):
    f32 = jnp.float32
    seq_count, token_count = (tokens.shape[0], tokens.shape[1])
    row_total = seq_count * token_count
    sequence = tokens.reshape(row_total, tokens.shape[2]).astype(f32)
    query_start = lax.axis_index("sp") * token_count
    positions = query_start + jnp.arange(token_count)
    normed = (sequence * rms_scale(sequence) * pre_gain).astype(jnp.bfloat16)
    head_group = lax.axis_index("tp")
    q_width = query_down.shape[1] // lax.axis_size("tp")
    kv_width = latent_down.shape[1] // lax.axis_size("tp")
    q_own = lax.dynamic_slice_in_dim(query_down, head_group * q_width, q_width, 1)
    kv_own = lax.dynamic_slice_in_dim(latent_down, head_group * kv_width, kv_width, 1)
    weights = (query_weight, key_weight, value_weight, q_own, kv_own)
    portion = (
        lax.all_gather(query_weight, ("sp", "fs"), axis=0, tiled=True),
        lax.all_gather(key_weight, ("sp", "fs"), axis=0, tiled=True),
        lax.all_gather(value_weight, ("sp", "fs"), axis=0, tiled=True),
        lax.all_gather(q_own, ("sp", "fs"), axis=0, tiled=True),
        lax.all_gather(kv_own, ("sp", "fs"), axis=0, tiled=True),
    )
    row_count = portion[0].shape[0]
    projected = tuple((jnp.dot(normed, weight, preferred_element_type=f32) for weight in portion))
    raw_query, raw_key, raw_value, q_half, kv_half = tuple((stored(member) for member in projected))
    q_latent, kv_latent = (
        lax.all_gather(q_half, "tp", axis=1, tiled=True),
        lax.all_gather(kv_half, "tp", axis=1, tiled=True),
    )
    head_count = query_weight.shape[1] // HEAD
    lane_count = seq_count * head_count
    beta_full = jax.nn.sigmoid(jnp.dot(normed, beta_weight, preferred_element_type=f32))
    beta_gate = lax.dynamic_slice_in_dim(beta_full, head_group * head_count, head_count, 1)
    decay_full = jnp.dot(normed, decay_weight, preferred_element_type=f32)
    decay_pre = lax.dynamic_slice_in_dim(decay_full, head_group * head_count, head_count, 1)
    decay_local = lax.dynamic_slice_in_dim(decay_rate, head_group * head_count, head_count, 0)
    log_decay = -decay_local[None, :] * jax.nn.softplus(decay_pre)

    def by_position(values):
        shaped = values.reshape((seq_count, token_count) + values.shape[1:])
        shaped = jnp.moveaxis(shaped, 0, 1)
        return shaped.reshape((token_count, seq_count * values.shape[1]) + values.shape[2:])

    query_vectors = by_position(
        unit_rows(jax.nn.silu(raw_query.astype(f32)).reshape(row_total, head_count, HEAD))
        * HEAD ** (-0.5)
    )
    key_vectors = by_position(
        unit_rows(jax.nn.silu(raw_key.astype(f32)).reshape(row_total, head_count, HEAD))
    )
    value_vectors = by_position(
        jax.nn.silu(raw_value.astype(f32)).reshape(row_total, head_count, HEAD)
    )
    block_terms = delta_terms(
        query_vectors, key_vectors, value_vectors, by_position(beta_gate), by_position(log_decay)
    )
    inputs = tuple((jnp.moveaxis(tensor, 1, 0) for tensor in block_terms))

    def advance(totals, block_in):
        carried, transfer = totals
        query_decay, key_decay, new_values, key_weights, scores, last_gate = block_in
        corrected = new_values - jnp.einsum("hcd,hde->hce", key_weights, carried, precision=HIGHEST)
        output = jnp.einsum("hcd,hde->hce", query_decay, carried, precision=HIGHEST) + jnp.einsum(
            "hij,hje->hie", scores, corrected, precision=HIGHEST
        )
        reader_rows = query_decay - jnp.einsum(
            "hij,hjd->hid", scores, key_weights, precision=HIGHEST
        )
        reader = jnp.einsum("hcd,hde->hce", reader_rows, transfer, precision=HIGHEST)
        factor = jnp.exp(last_gate)[:, None, None]
        carried = carried * factor + jnp.einsum(
            "hcd,hce->hde", key_decay, corrected, precision=HIGHEST
        )
        moved = jnp.einsum("hcd,hde->hce", key_weights, transfer, precision=HIGHEST)
        transfer = transfer * factor - jnp.einsum(
            "hcd,hce->hde", key_decay, moved, precision=HIGHEST
        )
        return ((carried, transfer), (output, reader))

    eye_stack = jnp.broadcast_to(jnp.eye(HEAD, dtype=f32), (lane_count, HEAD, HEAD))
    zero_state = jnp.zeros((lane_count, HEAD, HEAD), f32)
    (state_end, transfer_end), (outputs, readers) = lax.scan(
        advance, (zero_state, eye_stack), inputs
    )
    _, incoming = prefix((transfer_end, state_end), "sp", compose, (eye_stack, zero_state))
    outputs = outputs + jnp.einsum("nhcd,hde->nhce", readers, incoming, precision=HIGHEST)
    delta_raw = jnp.transpose(outputs, (0, 2, 1, 3)).reshape(
        token_count, seq_count, head_count, HEAD
    )
    delta_raw = jnp.moveaxis(delta_raw, 1, 0).reshape(row_total, head_count, HEAD)
    delta_heads = (
        (delta_raw * rms_scale(delta_raw) * delta_gain)
        .astype(jnp.bfloat16)
        .reshape(row_total, head_count * HEAD)
    )
    q_lat32 = q_latent.astype(f32)
    kv_lat32 = kv_latent.astype(f32)
    q_normed = (q_lat32 * rms_scale(q_lat32) * query_gain).astype(jnp.bfloat16)
    kv_normed = (kv_lat32 * rms_scale(kv_lat32) * latent_gain).astype(jnp.bfloat16)
    rope_raw = stored(jnp.dot(normed, rope_weight, preferred_element_type=f32))
    cosine_table, sine_table = rope_tables(positions, rope_raw.shape[1])
    rope_keys = rotate(
        rope_raw.astype(f32).reshape(seq_count, token_count, rope_raw.shape[1]),
        cosine_table,
        sine_table,
    ).astype(jnp.bfloat16)
    latent_count = query_up.shape[1] // (NOPE + ROPE)
    query_all = stored(jnp.dot(q_normed, query_up, preferred_element_type=f32)).reshape(
        seq_count, token_count, latent_count, NOPE + ROPE
    )
    query_plain = query_all[..., :NOPE]
    query_turned = rotate(
        query_all[..., NOPE:].astype(f32), cosine_table[:, None, :], sine_table[:, None, :]
    ).astype(jnp.bfloat16)
    score_scale = (NOPE + ROPE) ** (-0.5)
    query_block = positions // BLOCK
    kv_seq = kv_normed.reshape(seq_count, token_count, kv_normed.shape[1])

    def attend_block(totals, key_plain, value_rows, rope_rows, key_start):
        row_max, row_sum, weighted = totals
        key_block = (key_start + jnp.arange(key_plain.shape[1])) // BLOCK
        allowed = key_block[None, :] <= query_block[:, None]
        logits = (
            jnp.einsum("sqhd,skhd->shqk", query_plain, key_plain, preferred_element_type=f32)
            + jnp.einsum("sqhd,skd->shqk", query_turned, rope_rows, preferred_element_type=f32)
        ) * score_scale
        logits = jnp.where(allowed[None, None], logits, -jnp.inf)
        new_max = jnp.maximum(row_max, jnp.max(logits, axis=-1))
        shift = jnp.where(jnp.isfinite(new_max), new_max, 0.0)
        weights = jnp.where(allowed[None, None], jnp.exp(logits - shift[..., None]), 0.0)
        rescale = jnp.exp(row_max - shift)
        row_sum = row_sum * rescale + jnp.sum(weights, axis=-1)
        weighted = weighted * rescale[..., None] + jnp.einsum(
            "shqk,skhd->shqd", weights.astype(jnp.bfloat16), value_rows, preferred_element_type=f32
        )
        return (new_max, row_sum, weighted)

    start_stats = (
        jnp.full((seq_count, latent_count, token_count), -jnp.inf, f32),
        jnp.zeros((seq_count, latent_count, token_count), f32),
        jnp.zeros((seq_count, latent_count, token_count, VDIM), f32),
    )

    def expand_latent(portion, row_start, span_rows):
        latent_rows = lax.dynamic_slice_in_dim(portion[0], row_start, span_rows, 1)
        expanded = jnp.dot(
            latent_rows.reshape(seq_count * span_rows, latent_rows.shape[2]),
            latent_up,
            preferred_element_type=f32,
        ).astype(jnp.bfloat16)
        expanded = expanded.reshape(seq_count, span_rows, latent_count, NOPE + VDIM)
        return (
            expanded[..., :NOPE],
            expanded[..., NOPE:],
            lax.dynamic_slice_in_dim(portion[1], row_start, span_rows, 1),
        )

    portion = (
        lax.all_gather(kv_seq, "sp", axis=1, tiled=True),
        lax.all_gather(rope_keys, "sp", axis=1, tiled=True),
    )
    row_count = portion[0].shape[1]
    span_rows = math.gcd(row_count, token_count * max(1, 512 // token_count))

    def visit_rows(current):

        def visit_block(block_index, stats):
            row_start = block_index * span_rows
            key_plain, value_rows, rope_rows = expand_latent(portion, row_start, span_rows)
            return attend_block(stats, key_plain, value_rows, rope_rows, row_start)

        return lax.fori_loop(0, row_count // span_rows, visit_block, current)

    row_max, row_sum, weighted = lax.cond(
        jnp.int32(0) < query_start + token_count, visit_rows, keep_same, start_stats
    )
    latent_heads = (
        jnp.transpose(weighted / row_sum[..., None], (0, 2, 1, 3))
        .reshape(row_total, latent_count * VDIM)
        .astype(jnp.bfloat16)
    )
    heads_joined = jnp.concatenate([delta_heads, latent_heads], axis=1)
    out_rows = jnp.concatenate([delta_out, latent_out], axis=0)
    partial_value = jnp.dot(
        heads_joined,
        lax.all_gather(out_rows, ("sp", "fs"), axis=1, tiled=True),
        preferred_element_type=f32,
    )
    mixed_half = lax.psum_scatter(
        partial_value.astype(jnp.bfloat16), "tp", scatter_dimension=1, tiled=True
    ).astype(jnp.float32)
    squares = lax.psum(jnp.sum(mixed_half * mixed_half, axis=1), "tp")
    row_scale = lax.rsqrt(squares / D + NORM_EPS)
    result = mixed_half * row_scale[:, None] * post_gain
    return result.astype(jnp.bfloat16).reshape(seq_count, token_count, result.shape[1])


def pick(array, index):
    return lax.dynamic_index_in_dim(array, index, 0, False)


def dot32(left, right):
    return jnp.dot(left, right, preferred_element_type=jnp.float32)


def dot_t(left, right):
    return lax.dot_general(
        left, right, (((1,), (1,)), ((), ())), preferred_element_type=jnp.float32
    )


def two_parts(values):
    high = values.astype(jnp.bfloat16)
    return high, (values - high.astype(jnp.float32)).astype(jnp.bfloat16)


def fine_dot(left, right, product=dot32):
    left_high, left_low = two_parts(left)
    right_high, right_low = two_parts(right)
    return product(left_high, right_high) + (
        product(left_high, right_low) + product(left_low, right_high)
    )


def kernel_call(body, out_shapes, args, scratch=(), name=None):
    specs = [pl.BlockSpec(memory_space=pltpu.VMEM) for _ in args]
    return pl.pallas_call(
        body,
        out_shape=out_shapes,
        in_specs=specs,
        out_specs=jax.tree.map(lambda _: pl.BlockSpec(memory_space=pltpu.VMEM), out_shapes),
        scratch_shapes=scratch,
        name=name,
        compiler_params=pltpu.CompilerParams(vmem_limit_bytes=56 * 1024 * 1024),
    )(*args)


def outgoing_weights(mixers, lats, sp_size):
    half = mixers[0].shape[0] // 2
    per_mixer = mixers[0].shape[1] // sp_size
    per_lat = [w.shape[1] // sp_size // 2 for w in lats]
    columns = len(mixers) * per_mixer + sum(per_lat)
    padded = -(-columns // 128) * 128

    def body(*refs):
        rows = pl.ds(pl.multiple_of(lax.axis_index("grp") * half, half), half)
        first = lax.axis_index("tp") == 0
        out_ref = refs[-1]
        for s in range(sp_size):
            begin = 0
            for ref in refs[: len(mixers)]:
                out_ref[s, :, begin : begin + per_mixer] = ref[
                    rows, s * per_mixer : (s + 1) * per_mixer
                ]
                begin += per_mixer
            rest = []
            for ref, per in zip(refs[len(mixers) : -1], per_lat):
                pair = ref[rows, 2 * s * per : 2 * (s + 1) * per]
                rest.append(jnp.where(first, pair[:, :per], pair[:, per:]))
            rest.append(jnp.zeros((half, padded - columns), jnp.bfloat16))
            out_ref[s, :, begin:] = jnp.concatenate(rest, axis=1)

    return kernel_call(
        body,
        jax.ShapeDtypeStruct((sp_size, half, padded), jnp.bfloat16),
        (*mixers, *lats),
        name="outgoing_weights",
    )


def outgoing_tokens(tokens, gain, sp_size):
    rows, width = tokens.shape
    block = width // (sp_size * 4)

    def body(token_ref, gain_ref, mine_ref, their_ref):
        values = token_ref[...].astype(jnp.float32)
        normed = (values * rms_scale(values) * gain_ref[...]).astype(jnp.bfloat16)
        first = lax.axis_index("tp") == 0
        for f in range(2):
            for s in range(sp_size):
                begin = (s * 2 + f) * 2 * block
                low = normed[:, begin : begin + block]
                high = normed[:, begin + block : begin + 2 * block]
                at = (f * sp_size + s) * block
                mine_ref[:, at : at + block] = jnp.where(first, low, high)
                their_ref[:, at : at + block] = jnp.where(first, high, low)

    shape = jax.ShapeDtypeStruct((rows, width // 2), jnp.bfloat16)
    return kernel_call(body, (shape, shape), (tokens, gain), name="outgoing_tokens")


def project(mine, theirs, blocks, extra, sizes):
    seq_count, token_count, fine, q_cols, kv_cols = sizes
    sp_size = len(mine)
    span = sp_size * token_count
    rows = seq_count * span
    part = mine[0].shape[1]
    middle = part // 2
    extra_width = extra.shape[1]
    q_stack, kv_stack = 128 // q_cols, 128 // kv_cols
    packed = rows // q_stack + rows // kv_stack
    lat_width = q_cols + kv_cols

    def body(*refs):
        mine_refs, refs = refs[:sp_size], refs[sp_size:]
        their_refs, refs = refs[:sp_size], refs[sp_size:]
        block_refs, extra_ref, fine_ref, pack_ref, ext_ref, lat_ref = refs[:5], *refs[5:]
        place, fs_at = lax.axis_index("sp"), lax.axis_index("fs")
        tp_at = lax.axis_index("tp")
        straight = tp_at == lax.axis_index("grp")

        def lanes(fs_from):
            return pl.ds(pl.multiple_of(fs_from * middle, middle), middle)

        for o in range(sp_size):
            def half_of(same_grp, same_fs):
                at = lanes(fs_at if same_fs else 1 - fs_at)
                one, two = mine_refs[o][:, at], their_refs[o][:, at]
                if not same_grp:
                    one, two = two, one
                return jnp.where(straight, one, two)

            far = half_of(False, False)
            cut = block_refs[3].shape[0]
            value = (
                dot32(half_of(True, True), block_refs[0][...])
                + dot32(half_of(True, False), block_refs[1][...])
                + dot32(half_of(False, True), block_refs[2][...])
                + dot32(far[:, :cut], block_refs[3][...])
                + dot32(far[:, cut:], block_refs[4][...])
            ).astype(jnp.bfloat16)
            mine_at = pl.ds(pl.multiple_of(tp_at * part, part), part)
            their_at = pl.ds(pl.multiple_of((1 - tp_at) * part, part), part)
            outer = dot32(mine_refs[o][...], extra_ref[mine_at, :])
            outer = outer + dot32(their_refs[o][...], extra_ref[their_at, :])
            source = lax.rem(place + o, sp_size)
            for n in range(seq_count):
                of = slice(n * token_count, (n + 1) * token_count)
                at = pl.ds(pl.multiple_of(source * token_count, token_count), token_count)
                fine_ref[n, at, :] = value[of, :fine]
                ext_ref[n, at, :] = outer[of]
                at = pl.ds(
                    pl.multiple_of(n * span + source * token_count, token_count), token_count
                )
                lat_ref[at, :] = value[of, fine : fine + 128]
        group = rows // q_stack
        for base, first, width, count in (
            (0, 0, q_cols, q_stack),
            (rows // q_stack, q_cols, kv_cols, kv_stack),
        ):
            group = rows // count
            joined = jnp.concatenate(
                [
                    lat_ref[k * group : (k + 1) * group, first : first + width]
                    for k in range(count)
                ],
                axis=1,
            )
            for j in range(sp_size):
                pack_ref[j, base : base + group, :] = joined

    return kernel_call(
        body,
        (
            jax.ShapeDtypeStruct((seq_count, span, fine), jnp.bfloat16),
            jax.ShapeDtypeStruct((sp_size, packed, 128), jnp.bfloat16),
            jax.ShapeDtypeStruct((seq_count, span, extra_width), jnp.float32),
        ),
        (*mine, *theirs, *blocks, extra),
        scratch=(pltpu.VMEM((rows, 128), jnp.bfloat16),),
        name="project",
    )


def send_by_pair(out_refs, pieces, sp_size, token_count):
    place = lax.axis_index("sp")
    for step, out_ref in enumerate(out_refs):
        second = lax.rem(place + step, sp_size) >= sp_size // 2
        for n, (low, high) in enumerate(pieces):
            rows = low.shape[0]
            out_ref[n * rows : (n + 1) * rows, :] = jnp.where(second, high, low)


def lower_inverses(lowers, base):
    size = lowers[0].shape[0]
    row = lax.broadcasted_iota(jnp.int32, (size, size), 0)
    col = lax.broadcasted_iota(jnp.int32, (size, size), 1)
    unit = jnp.where(row == col, 1.0, 0.0)
    powers = [jnp.where(row // base == col // base, low, 0.0) for low in lowers]
    inverses = [unit - p for p in powers]
    reach = 2
    while reach < base:
        powers = [fine_dot(p, p) for p in powers]
        inverses = [i + fine_dot(i, p) for i, p in zip(inverses, powers)]
        reach *= 2
    block = base
    while block < size:
        joint = (row // (2 * block) == col // (2 * block)) & (row // block != col // block)
        moved = [fine_dot(i, jnp.where(joint, low, 0.0)) for i, low in zip(inverses, lowers)]
        inverses = [i - fine_dot(m, i) for i, m in zip(inverses, moved)]
        block *= 2
    return inverses


def delta_mix(fine, ext, gain, rates, gate_at, heads, sp_size):
    seq_count, span, _ = fine.shape
    tile = math.gcd(span, 128)
    tiles = span // tile
    gates = rates.shape[1]

    def terms(raw_query, raw_key, raw_value, beta_pre, decay_pre, rate):
        query = unit_rows(jax.nn.silu(raw_query)) * HEAD ** (-0.5)
        key = unit_rows(jax.nn.silu(raw_key))
        value = jax.nn.silu(raw_value)
        beta = jax.nn.sigmoid(beta_pre)
        log_decay = -rate * jax.nn.softplus(decay_pre)
        row = lax.broadcasted_iota(jnp.int32, (span, span), 0)
        col = lax.broadcasted_iota(jnp.int32, (span, span), 1)
        as_row = jnp.sum(jnp.where(row == col, log_decay, 0.0), axis=0, keepdims=True)
        gate = jnp.sum(jnp.where(row >= col, as_row, 0.0), axis=1, keepdims=True)
        gate_row = jnp.sum(jnp.where(row == col, gate, 0.0), axis=0, keepdims=True)
        decay = jnp.where(row >= col, jnp.exp(jnp.where(row >= col, gate - gate_row, 0.0)), 0.0)
        lower = fine_dot(key * beta, key, dot_t) * jnp.where(row > col, decay, 0.0)
        scores = fine_dot(query, key, dot_t) * decay
        return lower, scores, value * beta

    def body(fine_ref, ext_ref, gain_ref, rate_ref, *out_refs):
        first_head = (lax.axis_index("tp") * sp_size + lax.axis_index("sp")) * heads
        lane = lax.broadcasted_iota(jnp.int32, (span, ext.shape[2]), 1)
        rate_lane = lax.broadcasted_iota(jnp.int32, (1, gates), 1)
        chains = []
        for n in range(seq_count):
            for h in range(heads):
                raw = [
                    fine_ref[n, :, (k * heads + h) * HEAD : (k * heads + h + 1) * HEAD].astype(
                        jnp.float32
                    )
                    for k in range(3)
                ]
                head = first_head + h
                outer = ext_ref[n]
                beta_pre, decay_pre = (
                    jnp.sum(
                        jnp.where(lane == gate_at + k * gates + head, outer, 0.0),
                        axis=1,
                        keepdims=True,
                    )
                    for k in range(2)
                )
                rate = jnp.sum(
                    jnp.where(rate_lane == head, rate_ref[...], 0.0), axis=1, keepdims=True
                )
                chains.append(terms(*raw, beta_pre, decay_pre, rate))
        cuts = [slice(j * tile, (j + 1) * tile) for j in range(tiles)]
        inverses = lower_inverses([c[0][cut, cut] for c in chains for cut in cuts], 8)
        solved = [[] for _ in chains]
        for j, cut in enumerate(cuts):
            for i, (lower, _, wanted) in enumerate(chains):
                rest = wanted[cut]
                if j:
                    rest = rest - fine_dot(
                        lower[cut, : j * tile], jnp.concatenate(solved[i], axis=0)
                    )
                solved[i].append(fine_dot(inverses[i * tiles + j], rest))
        pieces = []
        for i, (_, scores, _) in enumerate(chains):
            out = fine_dot(scores, jnp.concatenate(solved[i], axis=0))
            out = (out * rms_scale(out) * gain_ref[...]).astype(jnp.bfloat16)
            pieces.append((out[: span // 2], out[span // 2 :]))
        for h in range(heads):
            columns = slice(h * HEAD, (h + 1) * HEAD)
            views = [ref.at[:, columns] for ref in out_refs] if heads > 1 else out_refs
            send_by_pair(views, pieces[h::heads], sp_size, span // sp_size)

    shape = jax.ShapeDtypeStruct((seq_count * span // 2, heads * HEAD), jnp.bfloat16)
    return kernel_call(
        body, (shape,) * sp_size, (fine, ext, gain, rates), name="delta_mix"
    )


def latent_mix(mine, theirs, ext, tables, gains, ups, q_cols, kv_cols, heads):
    sp_size = mine.shape[0]
    seq_count, span, _ = ext.shape
    rows = seq_count * span
    scale = (NOPE + ROPE) ** (-0.5)

    def unpack(value, n, base, width):
        group = rows * width // 128
        pieces = []
        for k in range(128 // width):
            if n * span < (k + 1) * group and k * group < (n + 1) * span:
                low = max(n * span - k * group, 0)
                high = min((n + 1) * span - k * group, group)
                pieces.append(
                    value[base + low : base + high, k * width : (k + 1) * width]
                )
        return jnp.concatenate(pieces, axis=0) if len(pieces) > 1 else pieces[0]

    def body(mine_ref, their_ref, ext_ref, cos_ref, sin_ref, *refs):
        qg_ref, kg_ref, qup_ref, kup_ref, *out_refs = refs
        first = lax.axis_index("tp") == 0
        row = lax.broadcasted_iota(jnp.int32, (span, span), 0) // BLOCK
        col = lax.broadcasted_iota(jnp.int32, (span, span), 1) // BLOCK
        allowed = col <= row
        cosine, sine = cos_ref[...], sin_ref[...]
        pairs = []
        for s in range(sp_size):
            own, other = mine_ref[s], their_ref[s]
            pairs += [jnp.where(first, own, other), jnp.where(first, other, own)]
        joins = []
        for n in range(seq_count):
            q_parts = [unpack(p, n, 0, q_cols) for p in pairs]
            kv_parts = [unpack(p, n, rows * q_cols // 128, kv_cols) for p in pairs]
            q_lat = jnp.concatenate(q_parts, axis=1).astype(jnp.float32)
            kv_lat = jnp.concatenate(kv_parts, axis=1).astype(jnp.float32)
            q_norm = (q_lat * rms_scale(q_lat) * qg_ref[...]).astype(jnp.bfloat16)
            kv_norm = (kv_lat * rms_scale(kv_lat) * kg_ref[...]).astype(jnp.bfloat16)
            q_all = dot32(q_norm, qup_ref[...]).astype(jnp.bfloat16)
            kv_all = dot32(kv_norm, kup_ref[...]).astype(jnp.bfloat16)
            plain_width, turn_width = heads * NOPE, heads * ROPE
            plain = q_all[:, :plain_width]
            turn = q_all[:, plain_width : plain_width + turn_width].astype(jnp.float32)
            swapped = q_all[:, plain_width + turn_width :].astype(jnp.float32)
            turned = (turn * cosine + swapped * sine).astype(jnp.bfloat16)
            raw = ext_ref[n, :, :ROPE].astype(jnp.bfloat16).astype(jnp.float32)
            back = jnp.concatenate([raw[:, ROPE // 2 :], raw[:, : ROPE // 2]], axis=1)
            key_turn = (raw * cosine[:, :ROPE] + back * sine[:, :ROPE]).astype(jnp.bfloat16)
            results = []
            for h in range(heads):
                key_plain = kv_all[:, h * (NOPE + VDIM) : h * (NOPE + VDIM) + NOPE]
                values = kv_all[:, h * (NOPE + VDIM) + NOPE : (h + 1) * (NOPE + VDIM)]
                logits = (
                    dot_t(plain[:, h * NOPE : (h + 1) * NOPE], key_plain)
                    + dot_t(turned[:, h * ROPE : (h + 1) * ROPE], key_turn)
                ) * scale
                logits = jnp.where(allowed, logits, -jnp.inf)
                peak = jnp.max(logits, axis=-1, keepdims=True)
                weights = jnp.exp(logits - peak)
                total = jnp.sum(weights, axis=-1, keepdims=True)
                results.append(dot32(weights.astype(jnp.bfloat16), values) / total)
            joined = jnp.concatenate(results, axis=1).astype(jnp.bfloat16)
            joins.append((joined[: span // 2], joined[span // 2 :]))
        send_by_pair(out_refs, joins, sp_size, span // sp_size)

    shape = jax.ShapeDtypeStruct((rows // 2, heads * VDIM), jnp.bfloat16)
    return kernel_call(
        body,
        (shape,) * sp_size,
        (mine, theirs, ext, *tables, *gains, *ups),
        name="latent_mix",
    )


def output_partial(delta_all, latent_all, near, near_fs, far, far_fs, sizes):
    seq_count, token_count = sizes
    sp_size = len(delta_all)
    rows, d_width = delta_all[0].shape
    l_width = latent_all[0].shape[1]
    total, columns = near.shape
    half = total // 2
    per_half = sp_size // 2

    def body(*refs):
        d_refs, refs = refs[:sp_size], refs[sp_size:]
        l_refs, refs = refs[:sp_size], refs[sp_size:]
        near_ref, near_fs_ref, far_ref, far_fs_ref, keep_ref, pass_ref, lhs_ref = refs
        place, fs_at = lax.axis_index("sp"), lax.axis_index("fs")
        grp_at = lax.axis_index("grp")
        for o in range(sp_size):
            source = lax.rem(place + o, sp_size)
            base = (source // per_half) * half
            within = lax.rem(source, per_half)
            at = pl.multiple_of(base + within * d_width, 128)
            lhs_ref[:, pl.ds(at, d_width)] = d_refs[o][...]
            at = pl.multiple_of(base + per_half * d_width + within * l_width, 128)
            lhs_ref[:, pl.ds(at, l_width)] = l_refs[o][...]
        lhs = lhs_ref[...]
        own = lhs_ref[:, pl.ds(pl.multiple_of(grp_at * half, half), half)]
        other = lhs_ref[:, pl.ds(pl.multiple_of((1 - grp_at) * half, half), half)]
        close = (
            dot32(lhs, near_ref[...]).astype(jnp.bfloat16),
            dot32(lhs, near_fs_ref[...]).astype(jnp.bfloat16),
        )
        away = tuple(
            (dot32(own, ref[:half, :]) + dot32(other, ref[half:, :])).astype(jnp.bfloat16)
            for ref in (far_ref, far_fs_ref)
        )
        straight = place // per_half == lax.axis_index("tp")
        for k in range(2):
            begin = (1 - fs_at) if k else fs_at
            at = pl.ds(pl.multiple_of(begin * columns, columns), columns)
            keep = jnp.where(straight, close[k], away[k])
            onward = jnp.where(straight, away[k], close[k])
            pair_rows = 2 * token_count
            for n in range(seq_count):
                for p in range(2):
                    of = slice(n * pair_rows + p * token_count, n * pair_rows + (p + 1) * token_count)
                    to = slice(n * token_count, (n + 1) * token_count)
                    keep_ref[p, to, at] = keep[of]
                    pass_ref[p, to, at] = onward[of]

    shape = jax.ShapeDtypeStruct((2, rows // 2, 2 * columns), jnp.bfloat16)
    return kernel_call(
        body,
        (shape, shape),
        (*delta_all, *latent_all, near, near_fs, far, far_fs),
        scratch=(pltpu.VMEM((rows, total), jnp.bfloat16),),
        name="output_partial",
    )


def whole_tables(length, repeats):
    frequency = ROPE_THETA ** (-np.arange(0, ROPE, 2, dtype=np.float32) / np.float32(ROPE))
    angles = np.arange(length, dtype=np.float32)[:, None] * frequency[None, :].astype(np.float32)
    cosine, sine = np.cos(angles), np.sin(angles)
    return tuple(
        jnp.asarray(np.tile(np.concatenate(pair, axis=1), (1, repeats)), jnp.float32)
        for pair in ((cosine, cosine), (-sine, sine))
    )


def whole_sequences(
    tokens,
    pre_gain,
    query_weight,
    key_weight,
    value_weight,
    beta_weight,
    decay_weight,
    decay_rate,
    delta_gain,
    query_down,
    latent_down,
    rope_weight,
    query_gain,
    latent_gain,
    query_up,
    latent_up,
    delta_out,
    latent_out,
    post_gain,
):
    f32, bf16 = jnp.float32, jnp.bfloat16
    sp_size, tp_size = lax.axis_size("sp"), lax.axis_size("tp")
    place, grp_at = lax.axis_index("sp"), lax.axis_index("grp")
    seq_count, token_count, width = tokens.shape
    rows = seq_count * token_count
    heads = query_weight.shape[1] // HEAD // sp_size
    shares = sp_size * tp_size
    q_cols, kv_cols = query_down.shape[1] // shares, latent_down.shape[1] // shares

    def exchange(values, axis):
        return lax.all_to_all(values, axis, 0, 0, tiled=True)

    def swap(values, axis):
        return lax.ppermute(values, axis, [(0, 1), (1, 0)])

    def along(values, step):
        return lax.ppermute(values, "sp", [(i, (i + step) % sp_size) for i in range(sp_size)])

    def from_sp(sends):
        return [sends[0]] + [along(sends[step], step) for step in range(sp_size - 1, 0, -1)]

    with jax.named_scope("weights_out"):
        outgoing = outgoing_weights(
            (query_weight, key_weight, value_weight), (query_down, latent_down), sp_size
        )
        block = exchange(outgoing, "sp").reshape(-1, outgoing.shape[2])
    token_rows, outgoing = lax.optimization_barrier((tokens.reshape(rows, width), outgoing))

    quarter = delta_out.shape[0] // 2
    near = jnp.concatenate(
        [w[k * quarter : (k + 1) * quarter] for k in range(2) for w in (delta_out, latent_out)]
    )
    with jax.named_scope("near_out"):
        near_fs = swap(near, "fs")

    own_half, other_half = outgoing_tokens(token_rows, pre_gain[None, :], sp_size)
    with jax.named_scope("tokens_out"):
        mine = from_sp([own_half] * sp_size)
    theirs = [other_half] + [swap(piece, "tp") for piece in mine[1:]]

    with jax.named_scope("far_out"):
        far_half = lax.dynamic_slice_in_dim(near, grp_at * 2 * quarter, 2 * quarter, 0)
        far_half = along(far_half, sp_size // 2)

    middle = block.shape[0] // 2
    by_fs, by_grp = swap(block, "fs"), swap(block, "grp")
    blocks = (block, by_fs, by_grp, swap(by_grp[:middle], "fs"), swap(by_fs[middle:], "grp"))

    far = jnp.concatenate([far_half, swap(far_half, "grp")])
    far_fs = swap(far, "fs")

    gate_at = rope_weight.shape[1]
    filler = -(gate_at + 2 * beta_weight.shape[1]) % 128
    extra = jnp.concatenate(
        [rope_weight, beta_weight, decay_weight, jnp.zeros((width, filler), bf16)], axis=1
    )
    extra = extra.reshape(sp_size, 2, 2, width // (4 * sp_size), extra.shape[1])
    extra = jnp.transpose(extra, (2, 1, 0, 3, 4)).reshape(width, extra.shape[4])

    latent_heads = query_up.shape[1] // (NOPE + ROPE) // sp_size
    up = query_up.reshape(query_up.shape[0], sp_size, latent_heads, NOPE + ROPE)
    up = lax.dynamic_index_in_dim(up, place, 1, False)
    turn = up[..., NOPE:]
    back = jnp.concatenate([turn[..., ROPE // 2 :], turn[..., : ROPE // 2]], axis=-1)
    q_up = jnp.concatenate(
        [a.reshape(up.shape[0], -1) for a in (up[..., :NOPE], turn, back)], axis=1
    )
    kv_width = latent_up.shape[1] // sp_size
    kv_up = lax.dynamic_slice_in_dim(latent_up, place * kv_width, kv_width, 1)
    tables = whole_tables(sp_size * token_count, latent_heads)
    mine[1], extra, q_up, kv_up, far_half = lax.optimization_barrier(
        (mine[1], extra, q_up, kv_up, far_half)
    )

    fine, lat, ext = project(
        mine, theirs, blocks, extra, (seq_count, token_count, 3 * heads * HEAD, q_cols, kv_cols)
    )
    lat_mine = exchange(lat, "sp")
    lat_theirs = swap(lat_mine, "tp")

    delta_all = from_sp(
        delta_mix(fine, ext, delta_gain[None, :], decay_rate[None, :], gate_at, heads, sp_size)
    )
    latent_all = from_sp(
        latent_mix(
            lat_mine,
            lat_theirs,
            ext,
            tables,
            (query_gain[None, :], latent_gain[None, :]),
            (q_up, kv_up),
            q_cols,
            kv_cols,
            latent_heads,
        )
    )

    keep, onward = output_partial(
        delta_all, latent_all, near, near_fs, far, far_fs, (seq_count, token_count)
    )
    mixed = (keep.astype(f32) + swap(onward, "tp").astype(f32)).astype(bf16)
    side = lax.rem(place, 2)
    here = pick(mixed, side)
    there = lax.ppermute(pick(mixed, 1 - side), "sp", [(i, i ^ 1) for i in range(sp_size)])
    here, there = here.astype(f32), there.astype(f32)
    squares = jnp.sum(here * here, axis=1, keepdims=True) + jnp.sum(
        there * there, axis=1, keepdims=True
    )
    squares = squares + swap(squares, "tp")
    final = jnp.concatenate(
        [jnp.where(side == 0, here, there), jnp.where(side == 0, there, here)], axis=1
    )
    result = final * lax.rsqrt(squares / D + NORM_EPS) * post_gain
    return result.astype(bf16).reshape(seq_count, token_count, final.shape[1])


def fits_whole(mesh):
    shape = mesh.shape
    return all(shape[name] == 2 for name in ("grp", "fs", "tp")) and shape["sp"] == 4


def solution(mesh):
    def chosen(*args):
        head_count = args[2].shape[1] // HEAD
        latent_count = args[14].shape[1] // (NOPE + ROPE)
        sp_size = mesh.shape["sp"]
        whole = fits_whole(mesh) and head_count % sp_size == 0 and latent_count % sp_size == 0
        return (whole_sequences if whole else local)(*args)

    return jax.shard_map(
        chosen,
        mesh=mesh,
        in_specs=(
            P(("grp", "fs"), "sp", None),
            P(),
            P(("sp", "fs"), "tp"),
            P(("sp", "fs"), "tp"),
            P(("sp", "fs"), "tp"),
            P(),
            P(),
            P(),
            P(),
            P(("sp", "fs"), None),
            P(("sp", "fs"), None),
            P(),
            P(),
            P(),
            P(None, "tp"),
            P(None, "tp"),
            P("tp", ("sp", "fs")),
            P("tp", ("sp", "fs")),
            P("tp"),
        ),
        out_specs=P(("grp", "fs"), "sp", "tp"),
        check_vma=False,
    )
```

```python
import math

import jax
import jax.numpy as jnp
import numpy as np
from jax import lax
from jax.experimental import pallas as pl
from jax.experimental.pallas import tpu as pltpu
from jax.sharding import PartitionSpec as P


D = 2048
HEAD = 128
NOPE = 64
ROPE = 32
VDIM = 64
BLOCK = 64


NORM_EPS = 1e-06
ROPE_THETA = 10000.0
HIGHEST = lax.Precision.HIGHEST


def prefix(array, axis, join, neutral):
    place = lax.axis_index(axis)
    gathered = jax.tree.map(
        lambda a, kind: lax.all_gather(a.astype(kind), axis), array, (jnp.bfloat16, jnp.bfloat16)
    )
    state = jax.tree.map(lambda a, e: jnp.zeros_like(a) + jnp.asarray(e, a.dtype), array, neutral)

    def one(step, state):
        return join(
            state,
            jax.tree.map(
                lambda a, own: lax.dynamic_index_in_dim(a, step, 0, False).astype(own.dtype),
                gathered,
                array,
            ),
        )

    return lax.fori_loop(0, place, one, state)


def stored(values):
    return lax.optimization_barrier(values.astype(jnp.bfloat16))


def rms_scale(values):
    return lax.rsqrt(jnp.mean(values * values, axis=-1, keepdims=True) + NORM_EPS)


def unit_rows(values):
    return values * lax.rsqrt(jnp.sum(values * values, axis=-1, keepdims=True) + NORM_EPS)


def rope_tables(positions, rope_width):
    frequency = ROPE_THETA ** (-jnp.arange(0, rope_width, 2, dtype=jnp.float32) / rope_width)
    angles = positions.astype(jnp.float32)[:, None] * frequency[None, :]
    return (jnp.cos(angles), jnp.sin(angles))


def rotate(values, cosine_table, sine_table):
    lower_half, upper_half = jnp.split(values, 2, axis=-1)
    return jnp.concatenate(
        [
            lower_half * cosine_table - upper_half * sine_table,
            upper_half * cosine_table + lower_half * sine_table,
        ],
        axis=-1,
    )


def delta_terms(query_vectors, key_vectors, value_vectors, beta_gate, log_decay):
    length, head_count, _ = query_vectors.shape
    nblocks = length // BLOCK

    def split_blocks(tensor):
        return jnp.moveaxis(tensor.reshape((nblocks, BLOCK, head_count) + tensor.shape[2:]), 2, 0)

    query_vectors = split_blocks(query_vectors)
    key_vectors = split_blocks(key_vectors)
    value_vectors = split_blocks(value_vectors)
    beta_gate = split_blocks(beta_gate)
    gate_sum = jnp.cumsum(split_blocks(log_decay), axis=-1)
    position = jnp.arange(BLOCK)
    strict = position[:, None] > position[None, :]
    causal = position[:, None] >= position[None, :]
    gate_gap = gate_sum[..., :, None] - gate_sum[..., None, :]
    strict_decay = jnp.where(strict, jnp.exp(jnp.where(strict, gate_gap, 0.0)), 0.0)
    causal_decay = jnp.where(causal, jnp.exp(jnp.where(causal, gate_gap, 0.0)), 0.0)
    keys_scaled = key_vectors * beta_gate[..., None]
    lower_mat = (
        jnp.einsum("hnid,hnjd->hnij", keys_scaled, key_vectors, precision=HIGHEST) * strict_decay
    )
    identity = jnp.eye(BLOCK, dtype=jnp.float32)
    inverse = jax.scipy.linalg.solve_triangular(
        identity + lower_mat, jnp.broadcast_to(identity, lower_mat.shape), lower=True
    )
    new_values = jnp.einsum(
        "hnij,hnjd->hnid", inverse, value_vectors * beta_gate[..., None], precision=HIGHEST
    )
    key_weights = jnp.einsum(
        "hnij,hnjd->hnid", inverse, keys_scaled * jnp.exp(gate_sum)[..., None], precision=HIGHEST
    )
    scores = (
        jnp.einsum("hnid,hnjd->hnij", query_vectors, key_vectors, precision=HIGHEST) * causal_decay
    )
    last_gate = gate_sum[..., -1]
    query_decay = query_vectors * jnp.exp(gate_sum)[..., None]
    key_decay = key_vectors * jnp.exp(last_gate[..., None] - gate_sum)[..., None]
    return (query_decay, key_decay, new_values, key_weights, scores, last_gate)


def compose(earlier, following):
    return (
        jnp.einsum("hij,hjk->hik", following[0], earlier[0], precision=HIGHEST),
        jnp.einsum("hij,hjk->hik", following[0], earlier[1], precision=HIGHEST) + following[1],
    )


def keep_same(current):
    return current


def local(
    tokens,
    pre_gain,
    query_weight,
    key_weight,
    value_weight,
    beta_weight,
    decay_weight,
    decay_rate,
    delta_gain,
    query_down,
    latent_down,
    rope_weight,
    query_gain,
    latent_gain,
    query_up,
    latent_up,
    delta_out,
    latent_out,
    post_gain,
):
    f32 = jnp.float32
    seq_count, token_count = (tokens.shape[0], tokens.shape[1])
    row_total = seq_count * token_count
    sequence = tokens.reshape(row_total, tokens.shape[2]).astype(f32)
    query_start = lax.axis_index("sp") * token_count
    positions = query_start + jnp.arange(token_count)
    normed = (sequence * rms_scale(sequence) * pre_gain).astype(jnp.bfloat16)
    head_group = lax.axis_index("tp")
    q_width = query_down.shape[1] // lax.axis_size("tp")
    kv_width = latent_down.shape[1] // lax.axis_size("tp")
    q_own = lax.dynamic_slice_in_dim(query_down, head_group * q_width, q_width, 1)
    kv_own = lax.dynamic_slice_in_dim(latent_down, head_group * kv_width, kv_width, 1)
    portion = (
        lax.all_gather(query_weight, ("sp", "fs"), axis=0, tiled=True),
        lax.all_gather(key_weight, ("sp", "fs"), axis=0, tiled=True),
        lax.all_gather(value_weight, ("sp", "fs"), axis=0, tiled=True),
        lax.all_gather(q_own, ("sp", "fs"), axis=0, tiled=True),
        lax.all_gather(kv_own, ("sp", "fs"), axis=0, tiled=True),
    )
    row_count = portion[0].shape[0]
    projected = tuple((jnp.dot(normed, weight, preferred_element_type=f32) for weight in portion))
    raw_query, raw_key, raw_value, q_half, kv_half = tuple((stored(member) for member in projected))
    q_latent, kv_latent = (
        lax.all_gather(q_half, "tp", axis=1, tiled=True),
        lax.all_gather(kv_half, "tp", axis=1, tiled=True),
    )
    head_count = query_weight.shape[1] // HEAD
    lane_count = seq_count * head_count
    beta_full = jax.nn.sigmoid(jnp.dot(normed, beta_weight, preferred_element_type=f32))
    beta_gate = lax.dynamic_slice_in_dim(beta_full, head_group * head_count, head_count, 1)
    decay_full = jnp.dot(normed, decay_weight, preferred_element_type=f32)
    decay_pre = lax.dynamic_slice_in_dim(decay_full, head_group * head_count, head_count, 1)
    decay_local = lax.dynamic_slice_in_dim(decay_rate, head_group * head_count, head_count, 0)
    log_decay = -decay_local[None, :] * jax.nn.softplus(decay_pre)

    def by_position(values):
        shaped = values.reshape((seq_count, token_count) + values.shape[1:])
        shaped = jnp.moveaxis(shaped, 0, 1)
        return shaped.reshape((token_count, seq_count * values.shape[1]) + values.shape[2:])

    query_vectors = by_position(
        unit_rows(jax.nn.silu(raw_query.astype(f32)).reshape(row_total, head_count, HEAD))
        * HEAD ** (-0.5)
    )
    key_vectors = by_position(
        unit_rows(jax.nn.silu(raw_key.astype(f32)).reshape(row_total, head_count, HEAD))
    )
    value_vectors = by_position(
        jax.nn.silu(raw_value.astype(f32)).reshape(row_total, head_count, HEAD)
    )
    block_terms = delta_terms(
        query_vectors, key_vectors, value_vectors, by_position(beta_gate), by_position(log_decay)
    )
    inputs = tuple((jnp.moveaxis(tensor, 1, 0) for tensor in block_terms))

    def advance(totals, block_in):
        carried, transfer = totals
        query_decay, key_decay, new_values, key_weights, scores, last_gate = block_in
        corrected = new_values - jnp.einsum("hcd,hde->hce", key_weights, carried, precision=HIGHEST)
        output = jnp.einsum("hcd,hde->hce", query_decay, carried, precision=HIGHEST) + jnp.einsum(
            "hij,hje->hie", scores, corrected, precision=HIGHEST
        )
        reader_rows = query_decay - jnp.einsum(
            "hij,hjd->hid", scores, key_weights, precision=HIGHEST
        )
        reader = jnp.einsum("hcd,hde->hce", reader_rows, transfer, precision=HIGHEST)
        factor = jnp.exp(last_gate)[:, None, None]
        carried = carried * factor + jnp.einsum(
            "hcd,hce->hde", key_decay, corrected, precision=HIGHEST
        )
        moved = jnp.einsum("hcd,hde->hce", key_weights, transfer, precision=HIGHEST)
        transfer = transfer * factor - jnp.einsum(
            "hcd,hce->hde", key_decay, moved, precision=HIGHEST
        )
        return ((carried, transfer), (output, reader))

    eye_stack = jnp.broadcast_to(jnp.eye(HEAD, dtype=f32), (lane_count, HEAD, HEAD))
    zero_state = jnp.zeros((lane_count, HEAD, HEAD), f32)
    (state_end, transfer_end), (outputs, readers) = lax.scan(
        advance, (zero_state, eye_stack), inputs
    )
    _, incoming = prefix((transfer_end, state_end), "sp", compose, (eye_stack, zero_state))
    outputs = outputs + jnp.einsum("nhcd,hde->nhce", readers, incoming, precision=HIGHEST)
    delta_raw = jnp.transpose(outputs, (0, 2, 1, 3)).reshape(
        token_count, seq_count, head_count, HEAD
    )
    delta_raw = jnp.moveaxis(delta_raw, 1, 0).reshape(row_total, head_count, HEAD)
    delta_heads = (
        (delta_raw * rms_scale(delta_raw) * delta_gain)
        .astype(jnp.bfloat16)
        .reshape(row_total, head_count * HEAD)
    )
    q_lat32 = q_latent.astype(f32)
    kv_lat32 = kv_latent.astype(f32)
    q_normed = (q_lat32 * rms_scale(q_lat32) * query_gain).astype(jnp.bfloat16)
    kv_normed = (kv_lat32 * rms_scale(kv_lat32) * latent_gain).astype(jnp.bfloat16)
    rope_raw = stored(jnp.dot(normed, rope_weight, preferred_element_type=f32))
    cosine_table, sine_table = rope_tables(positions, rope_raw.shape[1])
    rope_keys = rotate(
        rope_raw.astype(f32).reshape(seq_count, token_count, rope_raw.shape[1]),
        cosine_table,
        sine_table,
    ).astype(jnp.bfloat16)
    latent_count = query_up.shape[1] // (NOPE + ROPE)
    query_all = stored(jnp.dot(q_normed, query_up, preferred_element_type=f32)).reshape(
        seq_count, token_count, latent_count, NOPE + ROPE
    )
    query_plain = query_all[..., :NOPE]
    query_turned = rotate(
        query_all[..., NOPE:].astype(f32), cosine_table[:, None, :], sine_table[:, None, :]
    ).astype(jnp.bfloat16)
    score_scale = (NOPE + ROPE) ** (-0.5)
    query_block = positions // BLOCK
    kv_seq = kv_normed.reshape(seq_count, token_count, kv_normed.shape[1])

    def attend_block(totals, key_plain, value_rows, rope_rows, key_start):
        row_max, row_sum, weighted = totals
        key_block = (key_start + jnp.arange(key_plain.shape[1])) // BLOCK
        allowed = key_block[None, :] <= query_block[:, None]
        logits = (
            jnp.einsum("sqhd,skhd->shqk", query_plain, key_plain, preferred_element_type=f32)
            + jnp.einsum("sqhd,skd->shqk", query_turned, rope_rows, preferred_element_type=f32)
        ) * score_scale
        logits = jnp.where(allowed[None, None], logits, -jnp.inf)
        new_max = jnp.maximum(row_max, jnp.max(logits, axis=-1))
        shift = jnp.where(jnp.isfinite(new_max), new_max, 0.0)
        weights = jnp.where(allowed[None, None], jnp.exp(logits - shift[..., None]), 0.0)
        rescale = jnp.exp(row_max - shift)
        row_sum = row_sum * rescale + jnp.sum(weights, axis=-1)
        weighted = weighted * rescale[..., None] + jnp.einsum(
            "shqk,skhd->shqd", weights.astype(jnp.bfloat16), value_rows, preferred_element_type=f32
        )
        return (new_max, row_sum, weighted)

    start_stats = (
        jnp.full((seq_count, latent_count, token_count), -jnp.inf, f32),
        jnp.zeros((seq_count, latent_count, token_count), f32),
        jnp.zeros((seq_count, latent_count, token_count, VDIM), f32),
    )

    def expand_latent(portion, row_start, span_rows):
        latent_rows = lax.dynamic_slice_in_dim(portion[0], row_start, span_rows, 1)
        expanded = jnp.dot(
            latent_rows.reshape(seq_count * span_rows, latent_rows.shape[2]),
            latent_up,
            preferred_element_type=f32,
        ).astype(jnp.bfloat16)
        expanded = expanded.reshape(seq_count, span_rows, latent_count, NOPE + VDIM)
        return (
            expanded[..., :NOPE],
            expanded[..., NOPE:],
            lax.dynamic_slice_in_dim(portion[1], row_start, span_rows, 1),
        )

    portion = (
        lax.all_gather(kv_seq, "sp", axis=1, tiled=True),
        lax.all_gather(rope_keys, "sp", axis=1, tiled=True),
    )
    row_count = portion[0].shape[1]
    span_rows = math.gcd(row_count, token_count * max(1, 512 // token_count))

    def visit_rows(current):

        def visit_block(block_index, stats):
            row_start = block_index * span_rows
            key_plain, value_rows, rope_rows = expand_latent(portion, row_start, span_rows)
            return attend_block(stats, key_plain, value_rows, rope_rows, row_start)

        return lax.fori_loop(0, row_count // span_rows, visit_block, current)

    _, row_sum, weighted = lax.cond(
        jnp.int32(0) < query_start + token_count, visit_rows, keep_same, start_stats
    )
    latent_heads = (
        jnp.transpose(weighted / row_sum[..., None], (0, 2, 1, 3))
        .reshape(row_total, latent_count * VDIM)
        .astype(jnp.bfloat16)
    )
    heads_joined = jnp.concatenate([delta_heads, latent_heads], axis=1)
    out_rows = jnp.concatenate([delta_out, latent_out], axis=0)
    partial_value = jnp.dot(
        heads_joined,
        lax.all_gather(out_rows, ("sp", "fs"), axis=1, tiled=True),
        preferred_element_type=f32,
    )
    mixed_half = lax.psum_scatter(
        partial_value.astype(jnp.bfloat16), "tp", scatter_dimension=1, tiled=True
    ).astype(jnp.float32)
    squares = lax.psum(jnp.sum(mixed_half * mixed_half, axis=1), "tp")
    row_scale = lax.rsqrt(squares / D + NORM_EPS)
    result = mixed_half * row_scale[:, None] * post_gain
    return result.astype(jnp.bfloat16).reshape(seq_count, token_count, result.shape[1])


def pick(array, index):
    return lax.dynamic_index_in_dim(array, index, 0, False)


def dot32(left, right):
    return jnp.dot(left, right, preferred_element_type=jnp.float32)


def dot_t(left, right):
    return lax.dot_general(
        left, right, (((1,), (1,)), ((), ())), preferred_element_type=jnp.float32
    )


def two_parts(values):
    high = values.astype(jnp.bfloat16)
    return high, (values - high.astype(jnp.float32)).astype(jnp.bfloat16)


def fine_dot(left, right, product=dot32):
    left_high, left_low = two_parts(left)
    right_high, right_low = two_parts(right)
    return product(left_high, right_high) + (
        product(left_high, right_low) + product(left_low, right_high)
    )


def kernel_call(body, out_shapes, args, scratch=(), inside=(True, True)):
    space = pl.BlockSpec(memory_space=pltpu.VMEM)
    operand_space, result_space = (pltpu.VMEM if here else pltpu.HBM for here in inside)
    return pl.pallas_call(
        body,
        out_shape=jax.tree.map(lambda leaf: result_space(leaf.shape, leaf.dtype), out_shapes),
        in_specs=[space] * len(args),
        out_specs=jax.tree.map(lambda _: space, out_shapes),
        scratch_shapes=scratch,
        compiler_params=pltpu.CompilerParams(vmem_limit_bytes=16 * 1024 * 1024),
    )(*(pltpu.with_memory_space_constraint(arg, operand_space) for arg in args))


def outgoing_weights(mixers, lats, sp_size):
    half = mixers[0].shape[0] // 2
    per_mixer = mixers[0].shape[1] // sp_size
    per_lat = [w.shape[1] // sp_size // 2 for w in lats]
    columns = len(mixers) * per_mixer + sum(per_lat)
    padded = -(-columns // 128) * 128

    def body(*refs):
        rows = pl.ds(pl.multiple_of(lax.axis_index("grp") * half, half), half)
        first = lax.axis_index("tp") == 0
        out_ref = refs[-1]
        for s in range(sp_size):
            begin = 0
            for ref in refs[: len(mixers)]:
                out_ref[s, :, begin : begin + per_mixer] = ref[
                    rows, s * per_mixer : (s + 1) * per_mixer
                ]
                begin += per_mixer
            rest = []
            for ref, per in zip(refs[len(mixers) : -1], per_lat):
                pair = ref[rows, 2 * s * per : 2 * (s + 1) * per]
                rest.append(jnp.where(first, pair[:, :per], pair[:, per:]))
            rest.append(jnp.zeros((half, padded - columns), jnp.bfloat16))
            out_ref[s, :, begin:] = jnp.concatenate(rest, axis=1)

    return kernel_call(
        body,
        jax.ShapeDtypeStruct((sp_size, half, padded), jnp.bfloat16),
        (*mixers, *lats),
        inside=(False, False),
    )


def outgoing_tokens(tokens, gain, sp_size):
    rows, width = tokens.shape
    block = width // (sp_size * 4)

    def body(token_ref, gain_ref, mine_ref, their_ref):
        values = token_ref[...].astype(jnp.float32)
        normed = (values * rms_scale(values) * gain_ref[...]).astype(jnp.bfloat16)
        first = lax.axis_index("tp") == 0
        for f in range(2):
            for s in range(sp_size):
                begin = (s * 2 + f) * 2 * block
                low = normed[:, begin : begin + block]
                high = normed[:, begin + block : begin + 2 * block]
                at = (f * sp_size + s) * block
                mine_ref[:, at : at + block] = jnp.where(first, low, high)
                their_ref[:, at : at + block] = jnp.where(first, high, low)

    shape = jax.ShapeDtypeStruct((rows, width // 2), jnp.bfloat16)
    return kernel_call(body, (shape, shape), (tokens, gain))


def project(mine, theirs, blocks, extra, sizes):
    seq_count, token_count, fine, q_cols, kv_cols = sizes
    sp_size = len(mine)
    span = sp_size * token_count
    rows = seq_count * span
    part = mine[0].shape[1]
    middle = part // 2
    extra_width = extra.shape[1]
    q_stack, kv_stack = 128 // q_cols, 128 // kv_cols
    packed = rows // q_stack + rows // kv_stack

    def body(*refs):
        mine_refs, refs = refs[:sp_size], refs[sp_size:]
        their_refs, refs = refs[:sp_size], refs[sp_size:]
        block_refs, refs = refs[:7], refs[7:]
        extra_ref, fine_ref, pack_ref, ext_ref, lat_ref = refs
        place, fs_at = lax.axis_index("sp"), lax.axis_index("fs")
        tp_at = lax.axis_index("tp")
        straight = tp_at == lax.axis_index("grp")

        def lanes(fs_from):
            return pl.ds(pl.multiple_of(fs_from * middle, middle), middle)

        for o in range(sp_size):
            def half_of(same_grp, same_fs):
                at = lanes(fs_at if same_fs else 1 - fs_at)
                one, two = mine_refs[o][:, at], their_refs[o][:, at]
                if not same_grp:
                    one, two = two, one
                return jnp.where(straight, one, two)

            value = dot32(half_of(True, True), block_refs[0][...])
            for k, (same_grp, same_fs) in enumerate(((True, False), (False, True), (False, False))):
                lhs = half_of(same_grp, same_fs)
                value = value + dot32(lhs[:, : middle // 2], block_refs[2 * k + 1][...])
                value = value + dot32(lhs[:, middle // 2 :], block_refs[2 * k + 2][...])
            value = value.astype(jnp.bfloat16)
            mine_at = pl.ds(pl.multiple_of(tp_at * part, part), part)
            their_at = pl.ds(pl.multiple_of((1 - tp_at) * part, part), part)
            outer = dot32(mine_refs[o][...], extra_ref[mine_at, :])
            outer = outer + dot32(their_refs[o][...], extra_ref[their_at, :])
            source = lax.rem(place + o, sp_size)
            for n in range(seq_count):
                of = slice(n * token_count, (n + 1) * token_count)
                at = pl.ds(pl.multiple_of(source * token_count, token_count), token_count)
                fine_ref[n, at, :] = value[of, :fine]
                ext_ref[n, at, :] = outer[of]
                at = pl.ds(
                    pl.multiple_of(n * span + source * token_count, token_count), token_count
                )
                lat_ref[at, :] = value[of, fine : fine + 128]
        group = rows // q_stack
        for base, first, width, count in (
            (0, 0, q_cols, q_stack),
            (rows // q_stack, q_cols, kv_cols, kv_stack),
        ):
            group = rows // count
            joined = jnp.concatenate(
                [
                    lat_ref[k * group : (k + 1) * group, first : first + width]
                    for k in range(count)
                ],
                axis=1,
            )
            for j in range(sp_size):
                pack_ref[j, base : base + group, :] = joined

    return kernel_call(
        body,
        (
            jax.ShapeDtypeStruct((seq_count, span, fine), jnp.bfloat16),
            jax.ShapeDtypeStruct((sp_size, packed, 128), jnp.bfloat16),
            jax.ShapeDtypeStruct((seq_count, span, extra_width), jnp.float32),
        ),
        (*mine, *theirs, *blocks, extra),
        scratch=(pltpu.VMEM((rows, 128), jnp.bfloat16),),
    )


def send_by_pair(out_refs, pieces, sp_size):
    place = lax.axis_index("sp")
    for step, out_ref in enumerate(out_refs):
        second = lax.rem(place + step, sp_size) >= sp_size // 2
        for n, (low, high) in enumerate(pieces):
            rows = low.shape[0]
            out_ref[n * rows : (n + 1) * rows, :] = jnp.where(second, high, low)


def lower_inverses(lowers, base):
    size = lowers[0].shape[0]
    row = lax.broadcasted_iota(jnp.int32, (size, size), 0)
    col = lax.broadcasted_iota(jnp.int32, (size, size), 1)
    unit = jnp.where(row == col, 1.0, 0.0)
    powers = [jnp.where(row // base == col // base, low, 0.0) for low in lowers]
    inverses = [unit - p for p in powers]
    reach = 2
    while reach < base:
        powers = [fine_dot(p, p) for p in powers]
        inverses = [i + fine_dot(i, p) for i, p in zip(inverses, powers)]
        reach *= 2
    block = base
    while block < size:
        joint = (row // (2 * block) == col // (2 * block)) & (row // block != col // block)
        moved = [fine_dot(i, jnp.where(joint, low, 0.0)) for i, low in zip(inverses, lowers)]
        inverses = [i - fine_dot(m, i) for i, m in zip(inverses, moved)]
        block *= 2
    return inverses


def delta_mix(fine, ext, gain, rates, gate_at, heads, sp_size):
    seq_count, span, _ = fine.shape
    tile = math.gcd(span, 128)
    tiles = span // tile
    gates = rates.shape[1]

    def terms(raw_query, raw_key, raw_value, beta_pre, decay_pre, rate):
        query = unit_rows(jax.nn.silu(raw_query)) * HEAD ** (-0.5)
        key = unit_rows(jax.nn.silu(raw_key))
        value = jax.nn.silu(raw_value)
        beta = jax.nn.sigmoid(beta_pre)
        log_decay = -rate * jax.nn.softplus(decay_pre)
        row = lax.broadcasted_iota(jnp.int32, (span, span), 0)
        col = lax.broadcasted_iota(jnp.int32, (span, span), 1)
        as_row = jnp.sum(jnp.where(row == col, log_decay, 0.0), axis=0, keepdims=True)
        gate = jnp.sum(jnp.where(row >= col, as_row, 0.0), axis=1, keepdims=True)
        gate_row = jnp.sum(jnp.where(row == col, gate, 0.0), axis=0, keepdims=True)
        decay = jnp.where(row >= col, jnp.exp(jnp.where(row >= col, gate - gate_row, 0.0)), 0.0)
        lower = fine_dot(key * beta, key, dot_t) * jnp.where(row > col, decay, 0.0)
        scores = fine_dot(query, key, dot_t) * decay
        return lower, scores, value * beta

    def body(fine_ref, ext_ref, gain_ref, rate_ref, *out_refs):
        first_head = (lax.axis_index("tp") * sp_size + lax.axis_index("sp")) * heads
        lane = lax.broadcasted_iota(jnp.int32, (span, ext.shape[2]), 1)
        rate_lane = lax.broadcasted_iota(jnp.int32, (1, gates), 1)
        chains = []
        for n in range(seq_count):
            for h in range(heads):
                raw = [
                    fine_ref[n, :, (k * heads + h) * HEAD : (k * heads + h + 1) * HEAD].astype(
                        jnp.float32
                    )
                    for k in range(3)
                ]
                head = first_head + h
                outer = ext_ref[n]
                beta_pre, decay_pre = (
                    jnp.sum(
                        jnp.where(lane == gate_at + k * gates + head, outer, 0.0),
                        axis=1,
                        keepdims=True,
                    )
                    for k in range(2)
                )
                rate = jnp.sum(
                    jnp.where(rate_lane == head, rate_ref[...], 0.0), axis=1, keepdims=True
                )
                chains.append(terms(*raw, beta_pre, decay_pre, rate))
        cuts = [slice(j * tile, (j + 1) * tile) for j in range(tiles)]
        inverses = lower_inverses([c[0][cut, cut] for c in chains for cut in cuts], 8)
        solved = [[] for _ in chains]
        for j, cut in enumerate(cuts):
            for i, (lower, _, wanted) in enumerate(chains):
                rest = wanted[cut]
                if j:
                    rest = rest - fine_dot(
                        lower[cut, : j * tile], jnp.concatenate(solved[i], axis=0)
                    )
                solved[i].append(fine_dot(inverses[i * tiles + j], rest))
        pieces = []
        for i, (_, scores, _) in enumerate(chains):
            out = fine_dot(scores, jnp.concatenate(solved[i], axis=0))
            out = (out * rms_scale(out) * gain_ref[...]).astype(jnp.bfloat16)
            pieces.append((out[: span // 2], out[span // 2 :]))
        for h in range(heads):
            columns = slice(h * HEAD, (h + 1) * HEAD)
            views = [ref.at[:, columns] for ref in out_refs] if heads > 1 else out_refs
            send_by_pair(views, pieces[h::heads], sp_size)

    shape = jax.ShapeDtypeStruct((seq_count * span // 2, heads * HEAD), jnp.bfloat16)
    return kernel_call(body, (shape,) * sp_size, (fine, ext, gain, rates), inside=(True, False))


def latent_mix(mine, theirs, ext, tables, gains, ups, q_cols, kv_cols, heads):
    sp_size = mine.shape[0]
    seq_count, span, _ = ext.shape
    rows = seq_count * span
    scale = (NOPE + ROPE) ** (-0.5)

    def unpack(value, n, base, width):
        group = rows * width // 128
        pieces = []
        for k in range(128 // width):
            if n * span < (k + 1) * group and k * group < (n + 1) * span:
                low = max(n * span - k * group, 0)
                high = min((n + 1) * span - k * group, group)
                pieces.append(
                    value[base + low : base + high, k * width : (k + 1) * width]
                )
        return jnp.concatenate(pieces, axis=0) if len(pieces) > 1 else pieces[0]

    def body(mine_ref, their_ref, ext_ref, cos_ref, sin_ref, *refs):
        qg_ref, kg_ref, qup_ref, kup_ref, *out_refs = refs
        first = lax.axis_index("tp") == 0
        row = lax.broadcasted_iota(jnp.int32, (span, span), 0) // BLOCK
        col = lax.broadcasted_iota(jnp.int32, (span, span), 1) // BLOCK
        allowed = col <= row
        cosine, sine = cos_ref[...], sin_ref[...]
        pairs = []
        for s in range(sp_size):
            own, other = mine_ref[s], their_ref[s]
            pairs += [jnp.where(first, own, other), jnp.where(first, other, own)]
        joins = []
        for n in range(seq_count):
            q_parts = [unpack(p, n, 0, q_cols) for p in pairs]
            kv_parts = [unpack(p, n, rows * q_cols // 128, kv_cols) for p in pairs]
            q_lat = jnp.concatenate(q_parts, axis=1).astype(jnp.float32)
            kv_lat = jnp.concatenate(kv_parts, axis=1).astype(jnp.float32)
            q_norm = (q_lat * rms_scale(q_lat) * qg_ref[...]).astype(jnp.bfloat16)
            kv_norm = (kv_lat * rms_scale(kv_lat) * kg_ref[...]).astype(jnp.bfloat16)
            q_all = dot32(q_norm, qup_ref[...]).astype(jnp.bfloat16)
            kv_all = dot32(kv_norm, kup_ref[...]).astype(jnp.bfloat16)
            plain_width, turn_width = heads * NOPE, heads * ROPE
            plain = q_all[:, :plain_width]
            turn = q_all[:, plain_width : plain_width + turn_width].astype(jnp.float32)
            swapped = q_all[:, plain_width + turn_width :].astype(jnp.float32)
            turned = (turn * cosine + swapped * sine).astype(jnp.bfloat16)
            raw = ext_ref[n, :, :ROPE].astype(jnp.bfloat16).astype(jnp.float32)
            back = jnp.concatenate([raw[:, ROPE // 2 :], raw[:, : ROPE // 2]], axis=1)
            key_turn = (raw * cosine[:, :ROPE] + back * sine[:, :ROPE]).astype(jnp.bfloat16)
            results = []
            for h in range(heads):
                key_plain = kv_all[:, h * (NOPE + VDIM) : h * (NOPE + VDIM) + NOPE]
                values = kv_all[:, h * (NOPE + VDIM) + NOPE : (h + 1) * (NOPE + VDIM)]
                logits = (
                    dot_t(plain[:, h * NOPE : (h + 1) * NOPE], key_plain)
                    + dot_t(turned[:, h * ROPE : (h + 1) * ROPE], key_turn)
                ) * scale
                logits = jnp.where(allowed, logits, -jnp.inf)
                peak = jnp.max(logits, axis=-1, keepdims=True)
                weights = jnp.exp(logits - peak)
                total = jnp.sum(weights, axis=-1, keepdims=True)
                results.append(dot32(weights.astype(jnp.bfloat16), values) / total)
            joined = jnp.concatenate(results, axis=1).astype(jnp.bfloat16)
            joins.append((joined[: span // 2], joined[span // 2 :]))
        send_by_pair(out_refs, joins, sp_size)

    shape = jax.ShapeDtypeStruct((rows // 2, heads * VDIM), jnp.bfloat16)
    return kernel_call(body, (shape,) * sp_size, (mine, theirs, ext, *tables, *gains, *ups))


def output_partial(delta_all, latent_all, near, near_fs, far, sizes):
    seq_count, token_count = sizes
    sp_size = len(delta_all)
    rows, d_width = delta_all[0].shape
    l_width = latent_all[0].shape[1]
    total, columns = near.shape
    half = total // 2
    per_half = sp_size // 2

    def body(*refs):
        d_refs, refs = refs[:sp_size], refs[sp_size:]
        l_refs, refs = refs[:sp_size], refs[sp_size:]
        near_ref, near_fs_ref, *far_refs, keep_ref, pass_ref, lhs_ref = refs
        place, fs_at = lax.axis_index("sp"), lax.axis_index("fs")
        grp_at = lax.axis_index("grp")
        for o in range(sp_size):
            source = lax.rem(place + o, sp_size)
            base = (source // per_half) * half
            within = lax.rem(source, per_half)
            at = pl.multiple_of(base + within * d_width, 128)
            lhs_ref[:, pl.ds(at, d_width)] = d_refs[o][...]
            at = pl.multiple_of(base + per_half * d_width + within * l_width, 128)
            lhs_ref[:, pl.ds(at, l_width)] = l_refs[o][...]
        lhs = lhs_ref[...]
        own = lhs_ref[:, pl.ds(pl.multiple_of(grp_at * half, half), half)]
        other = lhs_ref[:, pl.ds(pl.multiple_of((1 - grp_at) * half, half), half)]
        close = (
            dot32(lhs, near_ref[...]).astype(jnp.bfloat16),
            dot32(lhs, near_fs_ref[...]).astype(jnp.bfloat16),
        )
        away = tuple(
            (dot32(own, far_refs[k][...]) + dot32(other, far_refs[k + 1][...])).astype(jnp.bfloat16)
            for k in (0, 2)
        )
        straight = place // per_half == lax.axis_index("tp")
        for k in range(2):
            begin = (1 - fs_at) if k else fs_at
            at = pl.ds(pl.multiple_of(begin * columns, columns), columns)
            keep = jnp.where(straight, close[k], away[k])
            onward = jnp.where(straight, away[k], close[k])
            pair_rows = 2 * token_count
            for n in range(seq_count):
                for p in range(2):
                    of = slice(n * pair_rows + p * token_count, n * pair_rows + (p + 1) * token_count)
                    to = slice(n * token_count, (n + 1) * token_count)
                    keep_ref[p, to, at] = keep[of]
                    pass_ref[p, to, at] = onward[of]

    shape = jax.ShapeDtypeStruct((2, rows // 2, 2 * columns), jnp.bfloat16)
    return kernel_call(
        body,
        (shape, shape),
        (*delta_all, *latent_all, near, near_fs, *far),
        scratch=(pltpu.VMEM((rows, total), jnp.bfloat16),),
    )


def whole_tables(length, repeats):
    frequency = ROPE_THETA ** (-np.arange(0, ROPE, 2, dtype=np.float32) / np.float32(ROPE))
    angles = np.arange(length, dtype=np.float32)[:, None] * frequency[None, :].astype(np.float32)
    cosine, sine = np.cos(angles), np.sin(angles)
    return tuple(
        jnp.asarray(np.tile(np.concatenate(pair, axis=1), (1, repeats)), jnp.float32)
        for pair in ((cosine, cosine), (-sine, sine))
    )


def whole_sequences(
    tokens,
    pre_gain,
    query_weight,
    key_weight,
    value_weight,
    beta_weight,
    decay_weight,
    decay_rate,
    delta_gain,
    query_down,
    latent_down,
    rope_weight,
    query_gain,
    latent_gain,
    query_up,
    latent_up,
    delta_out,
    latent_out,
    post_gain,
):
    f32, bf16 = jnp.float32, jnp.bfloat16
    sp_size, tp_size = lax.axis_size("sp"), lax.axis_size("tp")
    place, grp_at = lax.axis_index("sp"), lax.axis_index("grp")
    seq_count, token_count, width = tokens.shape
    rows = seq_count * token_count
    heads = query_weight.shape[1] // HEAD // sp_size
    shares = sp_size * tp_size
    q_cols, kv_cols = query_down.shape[1] // shares, latent_down.shape[1] // shares

    def exchange(values, axis):
        return lax.all_to_all(values, axis, 0, 0, tiled=True)

    def swap(values, axis):
        return lax.ppermute(values, axis, [(0, 1), (1, 0)])

    def along(values, step):
        return lax.ppermute(values, "sp", [(i, (i + step) % sp_size) for i in range(sp_size)])

    def from_sp(sends):
        return [sends[0]] + [along(sends[step], step) for step in range(sp_size - 1, 0, -1)]

    outgoing = outgoing_weights(
        (query_weight, key_weight, value_weight), (query_down, latent_down), sp_size
    )
    block = exchange(outgoing, "sp").reshape(-1, outgoing.shape[2])
    token_rows, outgoing = lax.optimization_barrier((tokens.reshape(rows, width), outgoing))

    own_half, other_half = outgoing_tokens(token_rows, pre_gain[None, :], sp_size)
    mine = [own_half] + [along(own_half, step) for step in range(sp_size - 1, 0, -1)]
    quarter = delta_out.shape[0] // 2
    near = jnp.concatenate(
        [w[k * quarter : (k + 1) * quarter] for k in range(2) for w in (delta_out, latent_out)]
    )
    near_fs = swap(near, "fs")

    middle = block.shape[0] // 2
    low, high = block[:middle], block[middle:]
    low_grp = swap(low, "grp")
    high_fs = swap(high, "fs")
    low_fs = swap(low, "fs")
    high_grp = swap(high, "grp")
    corner = swap(low_grp, "fs"), swap(high_fs, "grp")
    blocks = (block, low_fs, high_fs, low_grp, high_grp, *corner)
    theirs = [other_half] + [swap(piece, "tp") for piece in mine[1:]]

    far_own = lax.dynamic_slice_in_dim(near, grp_at * 2 * quarter, 2 * quarter, 0)
    far_own = along(far_own, sp_size // 2)
    far_other = swap(far_own, "grp")
    far = (far_own, far_other, swap(far_own, "fs"))
    far = (*far, swap(far_other, "fs"))

    gate_at = rope_weight.shape[1]
    filler = -(gate_at + 2 * beta_weight.shape[1]) % 128
    extra = jnp.concatenate(
        [rope_weight, beta_weight, decay_weight, jnp.zeros((width, filler), bf16)], axis=1
    )
    extra = extra.reshape(sp_size, 2, 2, width // (4 * sp_size), extra.shape[1])
    extra = jnp.transpose(extra, (2, 1, 0, 3, 4)).reshape(width, extra.shape[4])

    latent_heads = query_up.shape[1] // (NOPE + ROPE) // sp_size
    up = query_up.reshape(query_up.shape[0], sp_size, latent_heads, NOPE + ROPE)
    up = lax.dynamic_index_in_dim(up, place, 1, False)
    turn = up[..., NOPE:]
    back = jnp.concatenate([turn[..., ROPE // 2 :], turn[..., : ROPE // 2]], axis=-1)
    parts = [a.reshape(up.shape[0], -1) for a in (up[..., :NOPE], turn, back)]
    q_up = jnp.concatenate(parts, axis=1)
    kv_width = latent_up.shape[1] // sp_size
    kv_up = lax.dynamic_slice_in_dim(latent_up, place * kv_width, kv_width, 1)
    tables = whole_tables(sp_size * token_count, latent_heads)
    mine[1], extra, q_up, kv_up = lax.optimization_barrier((mine[1], extra, q_up, kv_up))

    fine, lat, ext = project(
        mine,
        theirs,
        blocks,
        extra,
        (seq_count, token_count, 3 * heads * HEAD, q_cols, kv_cols),
    )
    lat_mine = exchange(lat, "sp")
    delta_sends = delta_mix(
        fine, ext, delta_gain[None, :], decay_rate[None, :], gate_at, heads, sp_size
    )
    lat_mine, delta_sends = lax.optimization_barrier((lat_mine, delta_sends))
    lat_theirs = swap(lat_mine, "tp")
    delta_all = from_sp(delta_sends)
    latent_all = from_sp(
        latent_mix(
            lat_mine,
            lat_theirs,
            ext,
            tables,
            (query_gain[None, :], latent_gain[None, :]),
            (q_up, kv_up),
            q_cols,
            kv_cols,
            latent_heads,
        )
    )

    keep, onward = output_partial(
        delta_all, latent_all, near, near_fs, far, (seq_count, token_count)
    )
    mixed = (keep.astype(f32) + swap(onward, "tp").astype(f32)).astype(bf16)
    side = lax.rem(place, 2)
    here = pick(mixed, side)
    there = lax.ppermute(pick(mixed, 1 - side), "sp", [(i, i ^ 1) for i in range(sp_size)])
    here, there = here.astype(f32), there.astype(f32)
    squares = jnp.sum(here * here, axis=1, keepdims=True) + jnp.sum(
        there * there, axis=1, keepdims=True
    )
    squares = squares + swap(squares, "tp")
    final = jnp.concatenate(
        [jnp.where(side == 0, here, there), jnp.where(side == 0, there, here)], axis=1
    )
    result = final * lax.rsqrt(squares / D + NORM_EPS) * post_gain
    return result.astype(bf16).reshape(seq_count, token_count, final.shape[1])


def fits_whole(mesh):
    shape = mesh.shape
    return all(shape[name] == 2 for name in ("grp", "fs", "tp")) and shape["sp"] == 4


def solution(mesh):
    def chosen(*args):
        head_count = args[2].shape[1] // HEAD
        latent_count = args[14].shape[1] // (NOPE + ROPE)
        sp_size = mesh.shape["sp"]
        whole = fits_whole(mesh) and head_count % sp_size == 0 and latent_count % sp_size == 0
        return (whole_sequences if whole else local)(*args)

    return jax.shard_map(
        chosen,
        mesh=mesh,
        in_specs=(
            P(("grp", "fs"), "sp", None),
            P(),
            P(("sp", "fs"), "tp"),
            P(("sp", "fs"), "tp"),
            P(("sp", "fs"), "tp"),
            P(),
            P(),
            P(),
            P(),
            P(("sp", "fs"), None),
            P(("sp", "fs"), None),
            P(),
            P(),
            P(),
            P(None, "tp"),
            P(None, "tp"),
            P("tp", ("sp", "fs")),
            P("tp", ("sp", "fs")),
            P("tp"),
        ),
        out_specs=P(("grp", "fs"), "sp", "tp"),
        check_vma=False,
    )
```

```python
import math

import jax
import jax.numpy as jnp
import numpy as np
from jax import lax
from jax.experimental import pallas as pl
from jax.experimental.pallas import tpu as pltpu
from jax.sharding import PartitionSpec as P


D = 2048
HEAD = 128
NOPE = 64
ROPE = 32
VDIM = 64
BLOCK = 64


NORM_EPS = 1e-06
ROPE_THETA = 10000.0
HIGHEST = lax.Precision.HIGHEST


def prefix(array, axis, join, neutral):
    place = lax.axis_index(axis)
    gathered = jax.tree.map(
        lambda a, kind: lax.all_gather(a.astype(kind), axis), array, (jnp.bfloat16, jnp.bfloat16)
    )
    state = jax.tree.map(lambda a, e: jnp.zeros_like(a) + jnp.asarray(e, a.dtype), array, neutral)

    def one(step, state):
        return join(
            state,
            jax.tree.map(
                lambda a, own: lax.dynamic_index_in_dim(a, step, 0, False).astype(own.dtype),
                gathered,
                array,
            ),
        )

    return lax.fori_loop(0, place, one, state)


def stored(values):
    return lax.optimization_barrier(values.astype(jnp.bfloat16))


def rms_scale(values):
    return lax.rsqrt(jnp.mean(values * values, axis=-1, keepdims=True) + NORM_EPS)


def unit_rows(values):
    return values * lax.rsqrt(jnp.sum(values * values, axis=-1, keepdims=True) + NORM_EPS)


def rope_tables(positions, rope_width):
    frequency = ROPE_THETA ** (-jnp.arange(0, rope_width, 2, dtype=jnp.float32) / rope_width)
    angles = positions.astype(jnp.float32)[:, None] * frequency[None, :]
    return (jnp.cos(angles), jnp.sin(angles))


def rotate(values, cosine_table, sine_table):
    lower_half, upper_half = jnp.split(values, 2, axis=-1)
    return jnp.concatenate(
        [
            lower_half * cosine_table - upper_half * sine_table,
            upper_half * cosine_table + lower_half * sine_table,
        ],
        axis=-1,
    )


def delta_terms(query_vectors, key_vectors, value_vectors, beta_gate, log_decay):
    length, head_count, _ = query_vectors.shape
    nblocks = length // BLOCK

    def split_blocks(tensor):
        return jnp.moveaxis(tensor.reshape((nblocks, BLOCK, head_count) + tensor.shape[2:]), 2, 0)

    query_vectors = split_blocks(query_vectors)
    key_vectors = split_blocks(key_vectors)
    value_vectors = split_blocks(value_vectors)
    beta_gate = split_blocks(beta_gate)
    gate_sum = jnp.cumsum(split_blocks(log_decay), axis=-1)
    position = jnp.arange(BLOCK)
    strict = position[:, None] > position[None, :]
    causal = position[:, None] >= position[None, :]
    gate_gap = gate_sum[..., :, None] - gate_sum[..., None, :]
    strict_decay = jnp.where(strict, jnp.exp(jnp.where(strict, gate_gap, 0.0)), 0.0)
    causal_decay = jnp.where(causal, jnp.exp(jnp.where(causal, gate_gap, 0.0)), 0.0)
    keys_scaled = key_vectors * beta_gate[..., None]
    lower_mat = (
        jnp.einsum("hnid,hnjd->hnij", keys_scaled, key_vectors, precision=HIGHEST) * strict_decay
    )
    identity = jnp.eye(BLOCK, dtype=jnp.float32)
    inverse = jax.scipy.linalg.solve_triangular(
        identity + lower_mat, jnp.broadcast_to(identity, lower_mat.shape), lower=True
    )
    new_values = jnp.einsum(
        "hnij,hnjd->hnid", inverse, value_vectors * beta_gate[..., None], precision=HIGHEST
    )
    key_weights = jnp.einsum(
        "hnij,hnjd->hnid", inverse, keys_scaled * jnp.exp(gate_sum)[..., None], precision=HIGHEST
    )
    scores = (
        jnp.einsum("hnid,hnjd->hnij", query_vectors, key_vectors, precision=HIGHEST) * causal_decay
    )
    last_gate = gate_sum[..., -1]
    query_decay = query_vectors * jnp.exp(gate_sum)[..., None]
    key_decay = key_vectors * jnp.exp(last_gate[..., None] - gate_sum)[..., None]
    return (query_decay, key_decay, new_values, key_weights, scores, last_gate)


def compose(earlier, following):
    return (
        jnp.einsum("hij,hjk->hik", following[0], earlier[0], precision=HIGHEST),
        jnp.einsum("hij,hjk->hik", following[0], earlier[1], precision=HIGHEST) + following[1],
    )


def keep_same(current):
    return current


def local(
    tokens,
    pre_gain,
    query_weight,
    key_weight,
    value_weight,
    beta_weight,
    decay_weight,
    decay_rate,
    delta_gain,
    query_down,
    latent_down,
    rope_weight,
    query_gain,
    latent_gain,
    query_up,
    latent_up,
    delta_out,
    latent_out,
    post_gain,
):
    f32 = jnp.float32
    seq_count, token_count = (tokens.shape[0], tokens.shape[1])
    row_total = seq_count * token_count
    sequence = tokens.reshape(row_total, tokens.shape[2]).astype(f32)
    query_start = lax.axis_index("sp") * token_count
    positions = query_start + jnp.arange(token_count)
    normed = (sequence * rms_scale(sequence) * pre_gain).astype(jnp.bfloat16)
    head_group = lax.axis_index("tp")
    q_width = query_down.shape[1] // lax.axis_size("tp")
    kv_width = latent_down.shape[1] // lax.axis_size("tp")
    q_own = lax.dynamic_slice_in_dim(query_down, head_group * q_width, q_width, 1)
    kv_own = lax.dynamic_slice_in_dim(latent_down, head_group * kv_width, kv_width, 1)
    portion = (
        lax.all_gather(query_weight, ("sp", "fs"), axis=0, tiled=True),
        lax.all_gather(key_weight, ("sp", "fs"), axis=0, tiled=True),
        lax.all_gather(value_weight, ("sp", "fs"), axis=0, tiled=True),
        lax.all_gather(q_own, ("sp", "fs"), axis=0, tiled=True),
        lax.all_gather(kv_own, ("sp", "fs"), axis=0, tiled=True),
    )
    row_count = portion[0].shape[0]
    projected = tuple((jnp.dot(normed, weight, preferred_element_type=f32) for weight in portion))
    raw_query, raw_key, raw_value, q_half, kv_half = tuple((stored(member) for member in projected))
    q_latent, kv_latent = (
        lax.all_gather(q_half, "tp", axis=1, tiled=True),
        lax.all_gather(kv_half, "tp", axis=1, tiled=True),
    )
    head_count = query_weight.shape[1] // HEAD
    lane_count = seq_count * head_count
    beta_full = jax.nn.sigmoid(jnp.dot(normed, beta_weight, preferred_element_type=f32))
    beta_gate = lax.dynamic_slice_in_dim(beta_full, head_group * head_count, head_count, 1)
    decay_full = jnp.dot(normed, decay_weight, preferred_element_type=f32)
    decay_pre = lax.dynamic_slice_in_dim(decay_full, head_group * head_count, head_count, 1)
    decay_local = lax.dynamic_slice_in_dim(decay_rate, head_group * head_count, head_count, 0)
    log_decay = -decay_local[None, :] * jax.nn.softplus(decay_pre)

    def by_position(values):
        shaped = values.reshape((seq_count, token_count) + values.shape[1:])
        shaped = jnp.moveaxis(shaped, 0, 1)
        return shaped.reshape((token_count, seq_count * values.shape[1]) + values.shape[2:])

    query_vectors = by_position(
        unit_rows(jax.nn.silu(raw_query.astype(f32)).reshape(row_total, head_count, HEAD))
        * HEAD ** (-0.5)
    )
    key_vectors = by_position(
        unit_rows(jax.nn.silu(raw_key.astype(f32)).reshape(row_total, head_count, HEAD))
    )
    value_vectors = by_position(
        jax.nn.silu(raw_value.astype(f32)).reshape(row_total, head_count, HEAD)
    )
    block_terms = delta_terms(
        query_vectors, key_vectors, value_vectors, by_position(beta_gate), by_position(log_decay)
    )
    inputs = tuple((jnp.moveaxis(tensor, 1, 0) for tensor in block_terms))

    def advance(totals, block_in):
        carried, transfer = totals
        query_decay, key_decay, new_values, key_weights, scores, last_gate = block_in
        corrected = new_values - jnp.einsum("hcd,hde->hce", key_weights, carried, precision=HIGHEST)
        output = jnp.einsum("hcd,hde->hce", query_decay, carried, precision=HIGHEST) + jnp.einsum(
            "hij,hje->hie", scores, corrected, precision=HIGHEST
        )
        reader_rows = query_decay - jnp.einsum(
            "hij,hjd->hid", scores, key_weights, precision=HIGHEST
        )
        reader = jnp.einsum("hcd,hde->hce", reader_rows, transfer, precision=HIGHEST)
        factor = jnp.exp(last_gate)[:, None, None]
        carried = carried * factor + jnp.einsum(
            "hcd,hce->hde", key_decay, corrected, precision=HIGHEST
        )
        moved = jnp.einsum("hcd,hde->hce", key_weights, transfer, precision=HIGHEST)
        transfer = transfer * factor - jnp.einsum(
            "hcd,hce->hde", key_decay, moved, precision=HIGHEST
        )
        return ((carried, transfer), (output, reader))

    eye_stack = jnp.broadcast_to(jnp.eye(HEAD, dtype=f32), (lane_count, HEAD, HEAD))
    zero_state = jnp.zeros((lane_count, HEAD, HEAD), f32)
    (state_end, transfer_end), (outputs, readers) = lax.scan(
        advance, (zero_state, eye_stack), inputs
    )
    _, incoming = prefix((transfer_end, state_end), "sp", compose, (eye_stack, zero_state))
    outputs = outputs + jnp.einsum("nhcd,hde->nhce", readers, incoming, precision=HIGHEST)
    delta_raw = jnp.transpose(outputs, (0, 2, 1, 3)).reshape(
        token_count, seq_count, head_count, HEAD
    )
    delta_raw = jnp.moveaxis(delta_raw, 1, 0).reshape(row_total, head_count, HEAD)
    delta_heads = (
        (delta_raw * rms_scale(delta_raw) * delta_gain)
        .astype(jnp.bfloat16)
        .reshape(row_total, head_count * HEAD)
    )
    q_lat32 = q_latent.astype(f32)
    kv_lat32 = kv_latent.astype(f32)
    q_normed = (q_lat32 * rms_scale(q_lat32) * query_gain).astype(jnp.bfloat16)
    kv_normed = (kv_lat32 * rms_scale(kv_lat32) * latent_gain).astype(jnp.bfloat16)
    rope_raw = stored(jnp.dot(normed, rope_weight, preferred_element_type=f32))
    cosine_table, sine_table = rope_tables(positions, rope_raw.shape[1])
    rope_keys = rotate(
        rope_raw.astype(f32).reshape(seq_count, token_count, rope_raw.shape[1]),
        cosine_table,
        sine_table,
    ).astype(jnp.bfloat16)
    latent_count = query_up.shape[1] // (NOPE + ROPE)
    query_all = stored(jnp.dot(q_normed, query_up, preferred_element_type=f32)).reshape(
        seq_count, token_count, latent_count, NOPE + ROPE
    )
    query_plain = query_all[..., :NOPE]
    query_turned = rotate(
        query_all[..., NOPE:].astype(f32), cosine_table[:, None, :], sine_table[:, None, :]
    ).astype(jnp.bfloat16)
    score_scale = (NOPE + ROPE) ** (-0.5)
    query_block = positions // BLOCK
    kv_seq = kv_normed.reshape(seq_count, token_count, kv_normed.shape[1])

    def attend_block(totals, key_plain, value_rows, rope_rows, key_start):
        row_max, row_sum, weighted = totals
        key_block = (key_start + jnp.arange(key_plain.shape[1])) // BLOCK
        allowed = key_block[None, :] <= query_block[:, None]
        logits = (
            jnp.einsum("sqhd,skhd->shqk", query_plain, key_plain, preferred_element_type=f32)
            + jnp.einsum("sqhd,skd->shqk", query_turned, rope_rows, preferred_element_type=f32)
        ) * score_scale
        logits = jnp.where(allowed[None, None], logits, -jnp.inf)
        new_max = jnp.maximum(row_max, jnp.max(logits, axis=-1))
        shift = jnp.where(jnp.isfinite(new_max), new_max, 0.0)
        weights = jnp.where(allowed[None, None], jnp.exp(logits - shift[..., None]), 0.0)
        rescale = jnp.exp(row_max - shift)
        row_sum = row_sum * rescale + jnp.sum(weights, axis=-1)
        weighted = weighted * rescale[..., None] + jnp.einsum(
            "shqk,skhd->shqd", weights.astype(jnp.bfloat16), value_rows, preferred_element_type=f32
        )
        return (new_max, row_sum, weighted)

    start_stats = (
        jnp.full((seq_count, latent_count, token_count), -jnp.inf, f32),
        jnp.zeros((seq_count, latent_count, token_count), f32),
        jnp.zeros((seq_count, latent_count, token_count, VDIM), f32),
    )

    def expand_latent(portion, row_start, span_rows):
        latent_rows = lax.dynamic_slice_in_dim(portion[0], row_start, span_rows, 1)
        expanded = jnp.dot(
            latent_rows.reshape(seq_count * span_rows, latent_rows.shape[2]),
            latent_up,
            preferred_element_type=f32,
        ).astype(jnp.bfloat16)
        expanded = expanded.reshape(seq_count, span_rows, latent_count, NOPE + VDIM)
        return (
            expanded[..., :NOPE],
            expanded[..., NOPE:],
            lax.dynamic_slice_in_dim(portion[1], row_start, span_rows, 1),
        )

    portion = (
        lax.all_gather(kv_seq, "sp", axis=1, tiled=True),
        lax.all_gather(rope_keys, "sp", axis=1, tiled=True),
    )
    row_count = portion[0].shape[1]
    span_rows = math.gcd(row_count, token_count * max(1, 512 // token_count))

    def visit_rows(current):

        def visit_block(block_index, stats):
            row_start = block_index * span_rows
            key_plain, value_rows, rope_rows = expand_latent(portion, row_start, span_rows)
            return attend_block(stats, key_plain, value_rows, rope_rows, row_start)

        return lax.fori_loop(0, row_count // span_rows, visit_block, current)

    _, row_sum, weighted = lax.cond(
        jnp.int32(0) < query_start + token_count, visit_rows, keep_same, start_stats
    )
    latent_heads = (
        jnp.transpose(weighted / row_sum[..., None], (0, 2, 1, 3))
        .reshape(row_total, latent_count * VDIM)
        .astype(jnp.bfloat16)
    )
    heads_joined = jnp.concatenate([delta_heads, latent_heads], axis=1)
    out_rows = jnp.concatenate([delta_out, latent_out], axis=0)
    partial_value = jnp.dot(
        heads_joined,
        lax.all_gather(out_rows, ("sp", "fs"), axis=1, tiled=True),
        preferred_element_type=f32,
    )
    mixed_half = lax.psum_scatter(
        partial_value.astype(jnp.bfloat16), "tp", scatter_dimension=1, tiled=True
    ).astype(jnp.float32)
    squares = lax.psum(jnp.sum(mixed_half * mixed_half, axis=1), "tp")
    row_scale = lax.rsqrt(squares / D + NORM_EPS)
    result = mixed_half * row_scale[:, None] * post_gain
    return result.astype(jnp.bfloat16).reshape(seq_count, token_count, result.shape[1])


def pick(array, index):
    return lax.dynamic_index_in_dim(array, index, 0, False)


def dot32(left, right):
    return jnp.dot(left, right, preferred_element_type=jnp.float32)


def dot_t(left, right):
    return lax.dot_general(
        left, right, (((1,), (1,)), ((), ())), preferred_element_type=jnp.float32
    )


def two_parts(values):
    high = values.astype(jnp.bfloat16)
    return high, (values - high.astype(jnp.float32)).astype(jnp.bfloat16)


def fine_dot(left, right, product=dot32):
    left_high, left_low = two_parts(left)
    right_high, right_low = two_parts(right)
    return product(left_high, right_high) + (
        product(left_high, right_low) + product(left_low, right_high)
    )


def kernel_call(body, out_shapes, args, scratch=(), inside=(True, True), outside=0):
    space = pl.BlockSpec(memory_space=pltpu.VMEM)
    operand_space, result_space = (pltpu.VMEM if here else pltpu.HBM for here in inside)
    return pl.pallas_call(
        body,
        out_shape=jax.tree.map(lambda leaf: result_space(leaf.shape, leaf.dtype), out_shapes),
        in_specs=[space] * len(args),
        out_specs=jax.tree.map(lambda _: space, out_shapes),
        scratch_shapes=scratch,
        compiler_params=pltpu.CompilerParams(vmem_limit_bytes=16 * 1024 * 1024),
    )(
        *(
            pltpu.with_memory_space_constraint(arg, pltpu.HBM if i < outside else operand_space)
            for i, arg in enumerate(args)
        )
    )


def started(pairs, sems):
    copies = [pltpu.make_async_copy(*pair, sems.at[i]) for i, pair in enumerate(pairs)]
    for copy in copies:
        copy.start()
    return copies


def outgoing_weights(mixers, lats, sp_size):
    count = len(mixers)
    half = mixers[0].shape[0] // 2
    per_mixer = mixers[0].shape[1] // sp_size
    per_lat = [w.shape[1] // sp_size // 2 for w in lats]
    first_lat = count * per_mixer
    padded = first_lat + 128

    def body(*refs):
        out_ref, own_ref, *held_refs, sems = refs[count + 2 :]
        rows = pl.ds(pl.multiple_of(lax.axis_index("grp") * half, half), half)
        held = started([(ref.at[rows], to) for ref, to in zip(refs, held_refs)], sems)
        first = lax.axis_index("tp") == 0
        for copy in held:
            copy.wait()
        for s in range(sp_size):
            for k in range(count):
                out_ref[s, :, k * per_mixer : (k + 1) * per_mixer] = held_refs[k][
                    :, s * per_mixer : (s + 1) * per_mixer
                ]
            pieces = []
            for ref, per in zip(held_refs[count:], per_lat):
                pair = ref[:, 2 * s * per : 2 * (s + 1) * per]
                pieces.append(jnp.where(first, pair[:, :per], pair[:, per:]))
            pieces.append(jnp.zeros((half, 128 - sum(per_lat)), jnp.bfloat16))
            out_ref[s, :, first_lat:] = jnp.concatenate(pieces, axis=1)
        own_ref[...] = out_ref[lax.axis_index("sp")]

    space = pl.BlockSpec(memory_space=pltpu.VMEM)
    return pl.pallas_call(
        body,
        out_shape=(
            pltpu.HBM((sp_size, half, padded), jnp.bfloat16),
            pltpu.HBM((half, padded), jnp.bfloat16),
        ),
        in_specs=[pl.BlockSpec(memory_space=pl.ANY)] * (count + 2),
        out_specs=(space, space),
        scratch_shapes=(
            *(pltpu.VMEM((half, w.shape[1]), jnp.bfloat16) for w in (*mixers, *lats)),
            pltpu.SemaphoreType.DMA((count + 2,)),
        ),
        name="outgoing_weights",
        compiler_params=pltpu.CompilerParams(vmem_limit_bytes=16 * 1024 * 1024),
    )(*(pltpu.with_memory_space_constraint(w, pltpu.HBM) for w in (*mixers, *lats)))


def outgoing_tokens(tokens, gain, sp_size):
    rows, width = tokens.shape
    block = width // (sp_size * 4)

    def body(token_ref, gain_ref, mine_ref, their_ref):
        values = token_ref[...].astype(jnp.float32)
        normed = (values * rms_scale(values) * gain_ref[...]).astype(jnp.bfloat16)
        first = lax.axis_index("tp") == 0
        for f in range(2):
            for s in range(sp_size):
                begin = (s * 2 + f) * 2 * block
                low = normed[:, begin : begin + block]
                high = normed[:, begin + block : begin + 2 * block]
                at = (f * sp_size + s) * block
                mine_ref[:, at : at + block] = jnp.where(first, low, high)
                their_ref[:, at : at + block] = jnp.where(first, high, low)

    shape = jax.ShapeDtypeStruct((rows, width // 2), jnp.bfloat16)
    return kernel_call(body, (shape, shape), (tokens, gain))


def prepare(narrow, query_up, latent_up, sp_size):
    width = narrow[0].shape[1]
    block = width // (sp_size * 4)
    rank, query_width = query_up.shape
    per_query = query_width // sp_size
    heads = per_query // (NOPE + ROPE)
    per_latent = latent_up.shape[1] // sp_size

    def body(rope_ref, beta_ref, decay_ref, query_ref, latent_ref, narrow_ref, q_ref, kv_ref):
        place = lax.axis_index("sp")
        rows = jnp.concatenate([rope_ref[...], beta_ref[...], decay_ref[...]], axis=0)
        for s in range(sp_size):
            for f in range(2):
                for g in range(2):
                    begin = ((s * 2 + f) * 2 + g) * block
                    at = ((g * 2 + f) * sp_size + s) * block
                    narrow_ref[:, at : at + block] = rows[:, begin : begin + block]
        own = query_ref[:, :per_query]
        for s in range(1, sp_size):
            own = jnp.where(place == s, query_ref[:, s * per_query : (s + 1) * per_query], own)
        pairs = [
            (own[:, h * (NOPE + ROPE) :][:, :NOPE], own[:, h * (NOPE + ROPE) :][:, NOPE : NOPE + ROPE])
            for h in range(heads)
        ]
        parts = [plain for plain, _ in pairs] + [turn for _, turn in pairs]
        for _, turn in pairs:
            parts += [turn[:, ROPE // 2 :], turn[:, : ROPE // 2]]
        q_ref[...] = jnp.concatenate(parts, axis=1)
        kv_ref[...] = latent_ref[:, pl.ds(pl.multiple_of(place * per_latent, 128), per_latent)]

    bf16 = jnp.bfloat16
    return kernel_call(
        body,
        (
            jax.ShapeDtypeStruct((sum(n.shape[0] for n in narrow), width), bf16),
            jax.ShapeDtypeStruct((rank, heads * (NOPE + 2 * ROPE)), bf16),
            jax.ShapeDtypeStruct((latent_up.shape[0], per_latent), bf16),
        ),
        (*narrow, query_up, latent_up),
        inside=(False, True),
    )


def project(mine, theirs, block, peers, extra, sizes):
    seq_count, token_count, fine, q_cols, kv_cols = sizes
    sp_size = len(mine)
    chunk, part = mine[0].shape
    span = sp_size * token_count
    rows = seq_count * span
    piece, columns = peers[0].shape
    extra_width = extra.shape[0]
    q_stack, kv_stack = 128 // q_cols, 128 // kv_cols
    packed = rows // q_stack + rows // kv_stack
    copies = 1 + 3 * (sp_size + 1) + 2 * sp_size

    def body(*refs):
        mine_refs, refs = refs[:sp_size], refs[sp_size:]
        their_refs, refs = refs[:sp_size], refs[sp_size:]
        block_ref, refs = refs[0], refs[1:]
        peer_refs, refs = refs[:9], refs[9:]
        extra_ref, fine_ref, pack_ref, ext_ref, lat_ref, weight_ref, token_ref, sems = refs
        place, fs_at = lax.axis_index("sp"), lax.axis_index("fs")
        tp_at, grp_at = lax.axis_index("tp"), lax.axis_index("grp")
        step = piece // 2

        def rows_at(same_grp, same_fs, source, first, number):
            grp_from = grp_at if same_grp else 1 - grp_at
            block_from = (grp_from * 2 + (fs_at if same_fs else 1 - fs_at)) * sp_size + source
            return weight_ref.at[pl.ds(pl.multiple_of(block_from * piece + first, step), number)]

        moves = [(block_ref, rows_at(True, True, 0, 0, sp_size * piece))]
        half_rows = (sp_size - 1) * step
        for k, flips in enumerate(((True, False), (False, True), (False, False))):
            own_ref, low_ref, high_ref = peer_refs[3 * k : 3 * k + 3]
            moves.append((own_ref, rows_at(*flips, place, 0, piece)))
            for o in range(1, sp_size):
                source = lax.rem(place + o, sp_size)
                begin, end = (o - 1) * piece, o * piece
                cut = min(max(begin, half_rows), end)
                if cut > begin:
                    from_ref = low_ref.at[begin:cut]
                    moves.append((from_ref, rows_at(*flips, source, 0, cut - begin)))
                if end > cut:
                    from_ref = high_ref.at[cut - half_rows : end - half_rows]
                    moves.append((from_ref, rows_at(*flips, source, cut - begin, end - cut)))
        for o in range(sp_size):
            of = pl.ds(o * chunk, chunk)
            at = pl.ds(pl.multiple_of(tp_at * part, part), part)
            moves.append((mine_refs[o], token_ref.at[of, at]))
            at = pl.ds(pl.multiple_of((1 - tp_at) * part, part), part)
            moves.append((their_refs[o], token_ref.at[of, at]))
        assert len(moves) <= copies
        moves = started(moves, sems)
        for copy in moves[: -2 * sp_size]:
            copy.wait()
        for o in range(sp_size):
            for copy in moves[len(moves) - 2 * (sp_size - o) :][:2]:
                copy.wait()
            lhs = token_ref[o * chunk : (o + 1) * chunk, :]
            value = dot32(lhs, weight_ref[...]).astype(jnp.bfloat16)
            outer = dot_t(lhs, extra_ref[...])
            source = lax.bitwise_xor(place, o)
            for n in range(seq_count):
                of = slice(n * token_count, (n + 1) * token_count)
                at = pl.ds(pl.multiple_of(source * token_count, token_count), token_count)
                fine_ref[n, at, :] = value[of, :fine]
                ext_ref[n, at, :] = outer[of]
                at = pl.ds(
                    pl.multiple_of(n * span + source * token_count, token_count), token_count
                )
                lat_ref[at, :] = value[of, fine : fine + 128]
        for start, first, width, count in (
            (0, 0, q_cols, q_stack),
            (rows // q_stack, q_cols, kv_cols, kv_stack),
        ):
            group = rows // count
            joined = jnp.concatenate(
                [
                    lat_ref[k * group : (k + 1) * group, first : first + width]
                    for k in range(count)
                ],
                axis=1,
            )
            for j in range(sp_size):
                pack_ref[j, start : start + group, :] = joined

    space = pl.BlockSpec(memory_space=pltpu.VMEM)
    moved = tuple(
        pltpu.with_memory_space_constraint(array, pltpu.HBM)
        for array in (*mine, *theirs, block, *peers)
    )
    return pl.pallas_call(
        body,
        out_shape=(
            pltpu.VMEM((seq_count, span, fine), jnp.bfloat16),
            pltpu.VMEM((sp_size, packed, 128), jnp.bfloat16),
            pltpu.VMEM((seq_count, span, extra_width), jnp.float32),
        ),
        in_specs=[pl.BlockSpec(memory_space=pl.ANY)] * len(moved) + [space],
        out_specs=(space,) * 3,
        scratch_shapes=(
            pltpu.VMEM((rows, 128), jnp.bfloat16),
            pltpu.VMEM((2 * part, columns), jnp.bfloat16),
            pltpu.VMEM((rows, 2 * part), jnp.bfloat16),
            pltpu.SemaphoreType.DMA((copies,)),
        ),
        name="project",
        compiler_params=pltpu.CompilerParams(vmem_limit_bytes=16 * 1024 * 1024),
    )(*moved, pltpu.with_memory_space_constraint(extra, pltpu.VMEM))


def send_by_pair(out_refs, pieces, sp_size):
    place = lax.axis_index("sp")
    for step, out_ref in enumerate(out_refs):
        second = lax.rem(place + step, sp_size) >= sp_size // 2
        for n, (low, high) in enumerate(pieces):
            rows = low.shape[0]
            out_ref[n * rows : (n + 1) * rows, :] = jnp.where(second, high, low)


def lower_inverses(lowers, base):
    size = lowers[0].shape[0]
    row = lax.broadcasted_iota(jnp.int32, (size, size), 0)
    col = lax.broadcasted_iota(jnp.int32, (size, size), 1)
    unit = jnp.where(row == col, 1.0, 0.0)
    powers = [jnp.where(row // base == col // base, low, 0.0) for low in lowers]
    inverses = [unit - p for p in powers]
    reach = 2
    while reach < base:
        powers = [fine_dot(p, p) for p in powers]
        inverses = [i + fine_dot(i, p) for i, p in zip(inverses, powers)]
        reach *= 2
    block = base
    while block < size:
        joint = (row // (2 * block) == col // (2 * block)) & (row // block != col // block)
        moved = [fine_dot(i, jnp.where(joint, low, 0.0)) for i, low in zip(inverses, lowers)]
        inverses = [i - fine_dot(m, i) for i, m in zip(inverses, moved)]
        block *= 2
    return inverses


def delta_mix(fine, ext, gains, gain_at, gates, gate_at, heads, sp_size):
    seq_count, span, _ = fine.shape
    tile = math.gcd(span, 128)
    tiles = span // tile

    def terms(raw_query, raw_key, raw_value, beta_pre, decay_pre, rate):
        query = unit_rows(jax.nn.silu(raw_query)) * HEAD ** (-0.5)
        key = unit_rows(jax.nn.silu(raw_key))
        value = jax.nn.silu(raw_value)
        beta = jax.nn.sigmoid(beta_pre)
        log_decay = -rate * jax.nn.softplus(decay_pre)
        row = lax.broadcasted_iota(jnp.int32, (span, span), 0)
        col = lax.broadcasted_iota(jnp.int32, (span, span), 1)
        as_row = jnp.sum(jnp.where(row == col, log_decay, 0.0), axis=0, keepdims=True)
        gate = jnp.sum(jnp.where(row >= col, as_row, 0.0), axis=1, keepdims=True)
        gate_row = jnp.sum(jnp.where(row == col, gate, 0.0), axis=0, keepdims=True)
        decay = jnp.where(row >= col, jnp.exp(jnp.where(row >= col, gate - gate_row, 0.0)), 0.0)
        lower = fine_dot(key * beta, key, dot_t) * jnp.where(row > col, decay, 0.0)
        scores = fine_dot(query, key, dot_t) * decay
        return lower, scores, value * beta

    def body(fine_ref, ext_ref, gain_ref, *out_refs):
        gain_row = gain_ref[:, gain_at : gain_at + HEAD]
        rate_row = gain_ref[:, gain_at + HEAD : gain_at + 2 * HEAD]
        first_head = (lax.axis_index("tp") * sp_size + lax.axis_index("sp")) * heads
        lane = lax.broadcasted_iota(jnp.int32, (span, ext.shape[2]), 1)
        rate_lane = lax.broadcasted_iota(jnp.int32, (1, HEAD), 1)
        chains = []
        for n in range(seq_count):
            for h in range(heads):
                raw = [
                    fine_ref[n, :, (k * heads + h) * HEAD : (k * heads + h + 1) * HEAD].astype(
                        jnp.float32
                    )
                    for k in range(3)
                ]
                head = first_head + h
                outer = ext_ref[n]
                beta_pre, decay_pre = (
                    jnp.sum(
                        jnp.where(lane == gate_at + k * gates + head, outer, 0.0),
                        axis=1,
                        keepdims=True,
                    )
                    for k in range(2)
                )
                rate = jnp.sum(
                    jnp.where(rate_lane == head, rate_row, 0.0), axis=1, keepdims=True
                )
                chains.append(terms(*raw, beta_pre, decay_pre, rate))
        cuts = [slice(j * tile, (j + 1) * tile) for j in range(tiles)]
        inverses = lower_inverses([c[0][cut, cut] for c in chains for cut in cuts], 8)
        solved = [[] for _ in chains]
        for j, cut in enumerate(cuts):
            for i, (lower, _, wanted) in enumerate(chains):
                rest = wanted[cut]
                if j:
                    rest = rest - fine_dot(
                        lower[cut, : j * tile], jnp.concatenate(solved[i], axis=0)
                    )
                solved[i].append(fine_dot(inverses[i * tiles + j], rest))
        pieces = []
        for i, (_, scores, _) in enumerate(chains):
            out = fine_dot(scores, jnp.concatenate(solved[i], axis=0))
            out = (out * rms_scale(out) * gain_row).astype(jnp.bfloat16)
            pieces.append((out[: span // 2], out[span // 2 :]))
        for h in range(heads):
            columns = slice(h * HEAD, (h + 1) * HEAD)
            views = [ref.at[:, columns] for ref in out_refs] if heads > 1 else out_refs
            send_by_pair(views, pieces[h::heads], sp_size)

    shape = jax.ShapeDtypeStruct((seq_count * span // 2, heads * HEAD), jnp.bfloat16)
    return kernel_call(body, (shape,) * sp_size, (fine, ext, gains), inside=(True, False))


def latent_mix(mine, theirs, ext, tables, gains, ups, q_cols, kv_cols, heads):
    sp_size = mine.shape[0]
    seq_count, span, _ = ext.shape
    rows = seq_count * span
    q_rank, kv_rank = ups[0].shape[0], ups[1].shape[0]
    scale = (NOPE + ROPE) ** (-0.5)

    def unpack(value, n, base, width):
        group = rows * width // 128
        pieces = []
        for k in range(128 // width):
            if n * span < (k + 1) * group and k * group < (n + 1) * span:
                low = max(n * span - k * group, 0)
                high = min((n + 1) * span - k * group, group)
                pieces.append(
                    value[base + low : base + high, k * width : (k + 1) * width]
                )
        return jnp.concatenate(pieces, axis=0) if len(pieces) > 1 else pieces[0]

    def body(mine_ref, their_ref, ext_ref, cos_ref, sin_ref, *refs):
        gain_ref, qup_ref, kup_ref, *out_refs = refs
        q_gain = gain_ref[:, :q_rank]
        kv_gain = gain_ref[:, q_rank : q_rank + kv_rank]
        first = lax.axis_index("tp") == 0
        row = lax.broadcasted_iota(jnp.int32, (span, span), 0) // BLOCK
        col = lax.broadcasted_iota(jnp.int32, (span, span), 1) // BLOCK
        allowed = col <= row
        cosine, sine = cos_ref[...], sin_ref[...]
        pairs = []
        for s in range(sp_size):
            own, other = mine_ref[s], their_ref[s]
            pairs += [jnp.where(first, own, other), jnp.where(first, other, own)]
        joins = []
        for n in range(seq_count):
            q_parts = [unpack(p, n, 0, q_cols) for p in pairs]
            kv_parts = [unpack(p, n, rows * q_cols // 128, kv_cols) for p in pairs]
            q_lat = jnp.concatenate(q_parts, axis=1).astype(jnp.float32)
            kv_lat = jnp.concatenate(kv_parts, axis=1).astype(jnp.float32)
            q_norm = (q_lat * rms_scale(q_lat) * q_gain).astype(jnp.bfloat16)
            kv_norm = (kv_lat * rms_scale(kv_lat) * kv_gain).astype(jnp.bfloat16)
            q_all = dot32(q_norm, qup_ref[...]).astype(jnp.bfloat16)
            kv_all = dot32(kv_norm, kup_ref[...]).astype(jnp.bfloat16)
            plain_width, turn_width = heads * NOPE, heads * ROPE
            plain = q_all[:, :plain_width]
            turn = q_all[:, plain_width : plain_width + turn_width].astype(jnp.float32)
            swapped = q_all[:, plain_width + turn_width :].astype(jnp.float32)
            turned = (turn * cosine + swapped * sine).astype(jnp.bfloat16)
            raw = ext_ref[n, :, :ROPE].astype(jnp.bfloat16).astype(jnp.float32)
            back = jnp.concatenate([raw[:, ROPE // 2 :], raw[:, : ROPE // 2]], axis=1)
            key_turn = (raw * cosine[:, :ROPE] + back * sine[:, :ROPE]).astype(jnp.bfloat16)
            results = []
            for h in range(heads):
                key_plain = kv_all[:, h * (NOPE + VDIM) : h * (NOPE + VDIM) + NOPE]
                values = kv_all[:, h * (NOPE + VDIM) + NOPE : (h + 1) * (NOPE + VDIM)]
                logits = (
                    dot_t(plain[:, h * NOPE : (h + 1) * NOPE], key_plain)
                    + dot_t(turned[:, h * ROPE : (h + 1) * ROPE], key_turn)
                ) * scale
                logits = jnp.where(allowed, logits, -jnp.inf)
                peak = jnp.max(logits, axis=-1, keepdims=True)
                weights = jnp.exp(logits - peak)
                total = jnp.sum(weights, axis=-1, keepdims=True)
                results.append(dot32(weights.astype(jnp.bfloat16), values) / total)
            joined = jnp.concatenate(results, axis=1).astype(jnp.bfloat16)
            joins.append((joined[: span // 2], joined[span // 2 :]))
        send_by_pair(out_refs, joins, sp_size)

    shape = jax.ShapeDtypeStruct((rows // 2, heads * VDIM), jnp.bfloat16)
    return kernel_call(
        body, (shape,) * sp_size, (mine, theirs, ext, *tables, gains, *ups), outside=2
    )


def output_partial(delta_all, latent_all, near, near_fs, far, sizes):
    seq_count, token_count = sizes
    sp_size = len(delta_all)
    rows, d_width = delta_all[0].shape
    l_width = latent_all[0].shape[1]
    total, columns = near.shape
    half = total // 2
    per_half = sp_size // 2

    def body(*refs):
        d_refs, refs = refs[:sp_size], refs[sp_size:]
        l_refs, refs = refs[:sp_size], refs[sp_size:]
        near_ref, near_fs_ref, *far_refs, keep_ref, pass_ref, lhs_ref = refs
        place, fs_at = lax.axis_index("sp"), lax.axis_index("fs")
        grp_at = lax.axis_index("grp")
        for o in range(sp_size):
            source = lax.rem(place + o, sp_size)
            base = (source // per_half) * half
            within = lax.rem(source, per_half)
            at = pl.multiple_of(base + within * d_width, 128)
            lhs_ref[:, pl.ds(at, d_width)] = d_refs[o][...]
            at = pl.multiple_of(base + per_half * d_width + within * l_width, 128)
            lhs_ref[:, pl.ds(at, l_width)] = l_refs[o][...]
        lhs = lhs_ref[...]
        own = lhs_ref[:, pl.ds(pl.multiple_of(grp_at * half, half), half)]
        other = lhs_ref[:, pl.ds(pl.multiple_of((1 - grp_at) * half, half), half)]
        close = (
            dot32(lhs, near_ref[...]).astype(jnp.bfloat16),
            dot32(lhs, near_fs_ref[...]).astype(jnp.bfloat16),
        )
        away = tuple(
            (dot32(own, far_refs[k][...]) + dot32(other, far_refs[k + 1][...])).astype(jnp.bfloat16)
            for k in (0, 2)
        )
        straight = place // per_half == lax.axis_index("tp")
        for k in range(2):
            begin = (1 - fs_at) if k else fs_at
            at = pl.ds(pl.multiple_of(begin * columns, columns), columns)
            keep = jnp.where(straight, close[k], away[k])
            onward = jnp.where(straight, away[k], close[k])
            pair_rows = 2 * token_count
            for n in range(seq_count):
                for p in range(2):
                    of = slice(n * pair_rows + p * token_count, n * pair_rows + (p + 1) * token_count)
                    to = slice(n * token_count, (n + 1) * token_count)
                    keep_ref[p, to, at] = keep[of]
                    pass_ref[p, to, at] = onward[of]

    shape = jax.ShapeDtypeStruct((2, rows // 2, 2 * columns), jnp.bfloat16)
    return kernel_call(
        body,
        (shape, shape),
        (*delta_all, *latent_all, near, near_fs, *far),
        scratch=(pltpu.VMEM((rows, total), jnp.bfloat16),),
    )


def whole_tables(length, repeats):
    frequency = ROPE_THETA ** (-np.arange(0, ROPE, 2, dtype=np.float32) / np.float32(ROPE))
    angles = np.arange(length, dtype=np.float32)[:, None] * frequency[None, :].astype(np.float32)
    cosine, sine = np.cos(angles), np.sin(angles)
    return tuple(
        jnp.asarray(np.tile(np.concatenate(pair, axis=1), (1, repeats)), jnp.float32)
        for pair in ((cosine, cosine), (-sine, sine))
    )


def whole_sequences(
    tokens,
    pre_gain,
    query_weight,
    key_weight,
    value_weight,
    beta_weight,
    decay_weight,
    decay_rate,
    delta_gain,
    query_down,
    latent_down,
    rope_weight,
    query_gain,
    latent_gain,
    query_up,
    latent_up,
    delta_out,
    latent_out,
    post_gain,
):
    f32, bf16 = jnp.float32, jnp.bfloat16
    sp_size, tp_size = lax.axis_size("sp"), lax.axis_size("tp")
    place, grp_at = lax.axis_index("sp"), lax.axis_index("grp")
    seq_count, token_count, width = tokens.shape
    rows = seq_count * token_count
    heads = query_weight.shape[1] // HEAD // sp_size
    shares = sp_size * tp_size
    q_cols, kv_cols = query_down.shape[1] // shares, latent_down.shape[1] // shares

    def exchange(values, axis):
        return lax.all_to_all(values, axis, 0, 0, tiled=True)

    def swap(values, axis):
        return lax.ppermute(values, axis, [(0, 1), (1, 0)])

    def along(values, step):
        return lax.ppermute(values, "sp", [(i, (i + step) % sp_size) for i in range(sp_size)])

    def from_sp(sends):
        return [sends[0]] + [along(sends[step], step) for step in range(sp_size - 1, 0, -1)]

    outgoing, own_piece = outgoing_weights(
        (query_weight, key_weight, value_weight), (query_down, latent_down), sp_size
    )
    block = exchange(outgoing, "sp")
    token_rows, outgoing = lax.optimization_barrier((tokens.reshape(rows, width), outgoing))

    own_half, other_half = outgoing_tokens(token_rows, pre_gain[None, :], sp_size)

    def beside(values):
        return lax.ppermute(values, "sp", [(i, i ^ 1) for i in range(sp_size)])

    far_half = along(own_half, sp_size // 2)
    mine = [own_half, beside(own_half), far_half, beside(far_half)]
    theirs = [other_half] + [swap(piece, "tp") for piece in mine[1:]]

    quarter = delta_out.shape[0] // 2
    near = jnp.concatenate(
        [w[k * quarter : (k + 1) * quarter] for k in range(2) for w in (delta_out, latent_out)]
    )
    near_fs = swap(near, "fs")

    own_grp, own_fs = swap(own_piece, "grp"), swap(own_piece, "fs")
    own_corner = swap(own_grp, "fs")
    rest = lax.dynamic_slice_in_dim(jnp.concatenate([block, block]), place + 1, sp_size - 1, 0)
    rest = rest.reshape(-1, rest.shape[2])
    block = block.reshape(-1, block.shape[2])
    middle = rest.shape[0] // 2
    low, high = rest[:middle], rest[middle:]
    low_grp, high_fs = swap(low, "grp"), swap(high, "fs")
    high_grp, low_fs = swap(high, "grp"), swap(low, "fs")
    corner = swap(low_grp, "fs"), swap(high_fs, "grp")
    peers = (own_fs, low_fs, high_fs, own_grp, low_grp, high_grp, own_corner, *corner)

    far_own = lax.dynamic_slice_in_dim(near, grp_at * 2 * quarter, 2 * quarter, 0)
    far_own = along(far_own, sp_size // 2)
    far_other = swap(far_own, "grp")
    far = (far_own, far_other, swap(far_own, "fs"))
    far = (*far, swap(far_other, "fs"))

    gate_at = rope_weight.shape[1]
    latent_heads = query_up.shape[1] // (NOPE + ROPE) // sp_size
    extra, q_up, kv_up = prepare(
        (rope_weight.T, beta_weight.T, decay_weight.T), query_up, latent_up, sp_size
    )
    tables = whole_tables(sp_size * token_count, latent_heads)
    rates = jnp.pad(decay_rate, (0, HEAD - decay_rate.shape[0]))
    latent_gains = jnp.concatenate([query_gain, latent_gain])[None, :]
    gains = jnp.concatenate([delta_gain, rates, post_gain])[None, :]
    mine[1], gains, latent_gains = lax.optimization_barrier((mine[1], gains, latent_gains))

    fine, lat, ext = project(
        mine,
        theirs,
        block,
        peers,
        extra,
        (seq_count, token_count, 3 * heads * HEAD, q_cols, kv_cols),
    )
    lat_mine = exchange(lat, "sp")
    delta_sends = delta_mix(
        fine, ext, gains, 0, decay_rate.shape[0], gate_at, heads, sp_size
    )
    lat_mine, _ = lax.optimization_barrier((lat_mine, delta_sends))
    lat_theirs = swap(lat_mine, "tp")
    delta_all = from_sp(delta_sends)
    latent_sends = latent_mix(
        lat_mine,
        lat_theirs,
        ext,
        tables,
        latent_gains,
        (q_up, kv_up),
        q_cols,
        kv_cols,
        latent_heads,
    )
    latent_all = from_sp(latent_sends)

    keep, onward = output_partial(
        delta_all, latent_all, near, near_fs, far, (seq_count, token_count)
    )
    mixed = (keep.astype(f32) + swap(onward, "tp").astype(f32)).astype(bf16)
    side = lax.rem(place, 2)

    def across(values):
        return lax.ppermute(pick(values, 1 - side), "sp", [(i, i ^ 1) for i in range(sp_size)])

    there = across(mixed)
    squares = jnp.sum(mixed.astype(f32) * mixed.astype(f32), axis=2)
    squares = squares + swap(squares, "tp")
    squares = (pick(squares, side) + across(squares))[:, None]
    here, there = pick(mixed, side).astype(f32), there.astype(f32)
    final = jnp.concatenate(
        [jnp.where(side == 0, here, there), jnp.where(side == 0, there, here)], axis=1
    )
    result = final * lax.rsqrt(squares / D + NORM_EPS) * gains[:, 2 * HEAD :]
    return result.astype(bf16).reshape(seq_count, token_count, final.shape[1])


def fits_whole(mesh):
    shape = mesh.shape
    return all(shape[name] == 2 for name in ("grp", "fs", "tp")) and shape["sp"] == 4


def solution(mesh):
    def chosen(*args):
        head_count = args[2].shape[1] // HEAD
        latent_count = args[14].shape[1] // (NOPE + ROPE)
        sp_size = mesh.shape["sp"]
        whole = fits_whole(mesh) and head_count % sp_size == 0 and latent_count % sp_size == 0
        return (whole_sequences if whole else local)(*args)

    return jax.shard_map(
        chosen,
        mesh=mesh,
        in_specs=(
            P(("grp", "fs"), "sp", None),
            P(),
            P(("sp", "fs"), "tp"),
            P(("sp", "fs"), "tp"),
            P(("sp", "fs"), "tp"),
            P(),
            P(),
            P(),
            P(),
            P(("sp", "fs"), None),
            P(("sp", "fs"), None),
            P(),
            P(),
            P(),
            P(None, "tp"),
            P(None, "tp"),
            P("tp", ("sp", "fs")),
            P("tp", ("sp", "fs")),
            P("tp"),
        ),
        out_specs=P(("grp", "fs"), "sp", "tp"),
        check_vma=False,
    )
```

```python
import math

import jax
import jax.numpy as jnp
import numpy as np
from jax import lax
from jax.experimental import pallas as pl
from jax.experimental.pallas import tpu as pltpu
from jax.sharding import PartitionSpec as P


D = 2048
HEAD = 128
NOPE = 64
ROPE = 32
VDIM = 64
BLOCK = 64


NORM_EPS = 1e-06
ROPE_THETA = 10000.0
HIGHEST = lax.Precision.HIGHEST


def prefix(array, axis, join, neutral):
    place = lax.axis_index(axis)
    gathered = jax.tree.map(
        lambda a, kind: lax.all_gather(a.astype(kind), axis), array, (jnp.bfloat16, jnp.bfloat16)
    )
    state = jax.tree.map(lambda a, e: jnp.zeros_like(a) + jnp.asarray(e, a.dtype), array, neutral)

    def one(step, state):
        return join(
            state,
            jax.tree.map(
                lambda a, own: lax.dynamic_index_in_dim(a, step, 0, False).astype(own.dtype),
                gathered,
                array,
            ),
        )

    return lax.fori_loop(0, place, one, state)


def stored(values):
    return lax.optimization_barrier(values.astype(jnp.bfloat16))


def rms_scale(values):
    return lax.rsqrt(jnp.mean(values * values, axis=-1, keepdims=True) + NORM_EPS)


def unit_rows(values):
    return values * lax.rsqrt(jnp.sum(values * values, axis=-1, keepdims=True) + NORM_EPS)


def rope_tables(positions, rope_width):
    frequency = ROPE_THETA ** (-jnp.arange(0, rope_width, 2, dtype=jnp.float32) / rope_width)
    angles = positions.astype(jnp.float32)[:, None] * frequency[None, :]
    return (jnp.cos(angles), jnp.sin(angles))


def rotate(values, cosine_table, sine_table):
    lower_half, upper_half = jnp.split(values, 2, axis=-1)
    return jnp.concatenate(
        [
            lower_half * cosine_table - upper_half * sine_table,
            upper_half * cosine_table + lower_half * sine_table,
        ],
        axis=-1,
    )


def delta_terms(query_vectors, key_vectors, value_vectors, beta_gate, log_decay):
    length, head_count, _ = query_vectors.shape
    nblocks = length // BLOCK

    def split_blocks(tensor):
        return jnp.moveaxis(tensor.reshape((nblocks, BLOCK, head_count) + tensor.shape[2:]), 2, 0)

    query_vectors = split_blocks(query_vectors)
    key_vectors = split_blocks(key_vectors)
    value_vectors = split_blocks(value_vectors)
    beta_gate = split_blocks(beta_gate)
    gate_sum = jnp.cumsum(split_blocks(log_decay), axis=-1)
    position = jnp.arange(BLOCK)
    strict = position[:, None] > position[None, :]
    causal = position[:, None] >= position[None, :]
    gate_gap = gate_sum[..., :, None] - gate_sum[..., None, :]
    strict_decay = jnp.where(strict, jnp.exp(jnp.where(strict, gate_gap, 0.0)), 0.0)
    causal_decay = jnp.where(causal, jnp.exp(jnp.where(causal, gate_gap, 0.0)), 0.0)
    keys_scaled = key_vectors * beta_gate[..., None]
    lower_mat = (
        jnp.einsum("hnid,hnjd->hnij", keys_scaled, key_vectors, precision=HIGHEST) * strict_decay
    )
    identity = jnp.eye(BLOCK, dtype=jnp.float32)
    inverse = jax.scipy.linalg.solve_triangular(
        identity + lower_mat, jnp.broadcast_to(identity, lower_mat.shape), lower=True
    )
    new_values = jnp.einsum(
        "hnij,hnjd->hnid", inverse, value_vectors * beta_gate[..., None], precision=HIGHEST
    )
    key_weights = jnp.einsum(
        "hnij,hnjd->hnid", inverse, keys_scaled * jnp.exp(gate_sum)[..., None], precision=HIGHEST
    )
    scores = (
        jnp.einsum("hnid,hnjd->hnij", query_vectors, key_vectors, precision=HIGHEST) * causal_decay
    )
    last_gate = gate_sum[..., -1]
    query_decay = query_vectors * jnp.exp(gate_sum)[..., None]
    key_decay = key_vectors * jnp.exp(last_gate[..., None] - gate_sum)[..., None]
    return (query_decay, key_decay, new_values, key_weights, scores, last_gate)


def compose(earlier, following):
    return (
        jnp.einsum("hij,hjk->hik", following[0], earlier[0], precision=HIGHEST),
        jnp.einsum("hij,hjk->hik", following[0], earlier[1], precision=HIGHEST) + following[1],
    )


def keep_same(current):
    return current


def local(
    tokens,
    pre_gain,
    query_weight,
    key_weight,
    value_weight,
    beta_weight,
    decay_weight,
    decay_rate,
    delta_gain,
    query_down,
    latent_down,
    rope_weight,
    query_gain,
    latent_gain,
    query_up,
    latent_up,
    delta_out,
    latent_out,
    post_gain,
):
    f32 = jnp.float32
    seq_count, token_count = (tokens.shape[0], tokens.shape[1])
    row_total = seq_count * token_count
    sequence = tokens.reshape(row_total, tokens.shape[2]).astype(f32)
    query_start = lax.axis_index("sp") * token_count
    positions = query_start + jnp.arange(token_count)
    normed = (sequence * rms_scale(sequence) * pre_gain).astype(jnp.bfloat16)
    head_group = lax.axis_index("tp")
    q_width = query_down.shape[1] // lax.axis_size("tp")
    kv_width = latent_down.shape[1] // lax.axis_size("tp")
    q_own = lax.dynamic_slice_in_dim(query_down, head_group * q_width, q_width, 1)
    kv_own = lax.dynamic_slice_in_dim(latent_down, head_group * kv_width, kv_width, 1)
    portion = (
        lax.all_gather(query_weight, ("sp", "fs"), axis=0, tiled=True),
        lax.all_gather(key_weight, ("sp", "fs"), axis=0, tiled=True),
        lax.all_gather(value_weight, ("sp", "fs"), axis=0, tiled=True),
        lax.all_gather(q_own, ("sp", "fs"), axis=0, tiled=True),
        lax.all_gather(kv_own, ("sp", "fs"), axis=0, tiled=True),
    )
    row_count = portion[0].shape[0]
    projected = tuple((jnp.dot(normed, weight, preferred_element_type=f32) for weight in portion))
    raw_query, raw_key, raw_value, q_half, kv_half = tuple((stored(member) for member in projected))
    q_latent, kv_latent = (
        lax.all_gather(q_half, "tp", axis=1, tiled=True),
        lax.all_gather(kv_half, "tp", axis=1, tiled=True),
    )
    head_count = query_weight.shape[1] // HEAD
    lane_count = seq_count * head_count
    beta_full = jax.nn.sigmoid(jnp.dot(normed, beta_weight, preferred_element_type=f32))
    beta_gate = lax.dynamic_slice_in_dim(beta_full, head_group * head_count, head_count, 1)
    decay_full = jnp.dot(normed, decay_weight, preferred_element_type=f32)
    decay_pre = lax.dynamic_slice_in_dim(decay_full, head_group * head_count, head_count, 1)
    decay_local = lax.dynamic_slice_in_dim(decay_rate, head_group * head_count, head_count, 0)
    log_decay = -decay_local[None, :] * jax.nn.softplus(decay_pre)

    def by_position(values):
        shaped = values.reshape((seq_count, token_count) + values.shape[1:])
        shaped = jnp.moveaxis(shaped, 0, 1)
        return shaped.reshape((token_count, seq_count * values.shape[1]) + values.shape[2:])

    query_vectors = by_position(
        unit_rows(jax.nn.silu(raw_query.astype(f32)).reshape(row_total, head_count, HEAD))
        * HEAD ** (-0.5)
    )
    key_vectors = by_position(
        unit_rows(jax.nn.silu(raw_key.astype(f32)).reshape(row_total, head_count, HEAD))
    )
    value_vectors = by_position(
        jax.nn.silu(raw_value.astype(f32)).reshape(row_total, head_count, HEAD)
    )
    block_terms = delta_terms(
        query_vectors, key_vectors, value_vectors, by_position(beta_gate), by_position(log_decay)
    )
    inputs = tuple((jnp.moveaxis(tensor, 1, 0) for tensor in block_terms))

    def advance(totals, block_in):
        carried, transfer = totals
        query_decay, key_decay, new_values, key_weights, scores, last_gate = block_in
        corrected = new_values - jnp.einsum("hcd,hde->hce", key_weights, carried, precision=HIGHEST)
        output = jnp.einsum("hcd,hde->hce", query_decay, carried, precision=HIGHEST) + jnp.einsum(
            "hij,hje->hie", scores, corrected, precision=HIGHEST
        )
        reader_rows = query_decay - jnp.einsum(
            "hij,hjd->hid", scores, key_weights, precision=HIGHEST
        )
        reader = jnp.einsum("hcd,hde->hce", reader_rows, transfer, precision=HIGHEST)
        factor = jnp.exp(last_gate)[:, None, None]
        carried = carried * factor + jnp.einsum(
            "hcd,hce->hde", key_decay, corrected, precision=HIGHEST
        )
        moved = jnp.einsum("hcd,hde->hce", key_weights, transfer, precision=HIGHEST)
        transfer = transfer * factor - jnp.einsum(
            "hcd,hce->hde", key_decay, moved, precision=HIGHEST
        )
        return ((carried, transfer), (output, reader))

    eye_stack = jnp.broadcast_to(jnp.eye(HEAD, dtype=f32), (lane_count, HEAD, HEAD))
    zero_state = jnp.zeros((lane_count, HEAD, HEAD), f32)
    (state_end, transfer_end), (outputs, readers) = lax.scan(
        advance, (zero_state, eye_stack), inputs
    )
    _, incoming = prefix((transfer_end, state_end), "sp", compose, (eye_stack, zero_state))
    outputs = outputs + jnp.einsum("nhcd,hde->nhce", readers, incoming, precision=HIGHEST)
    delta_raw = jnp.transpose(outputs, (0, 2, 1, 3)).reshape(
        token_count, seq_count, head_count, HEAD
    )
    delta_raw = jnp.moveaxis(delta_raw, 1, 0).reshape(row_total, head_count, HEAD)
    delta_heads = (
        (delta_raw * rms_scale(delta_raw) * delta_gain)
        .astype(jnp.bfloat16)
        .reshape(row_total, head_count * HEAD)
    )
    q_lat32 = q_latent.astype(f32)
    kv_lat32 = kv_latent.astype(f32)
    q_normed = (q_lat32 * rms_scale(q_lat32) * query_gain).astype(jnp.bfloat16)
    kv_normed = (kv_lat32 * rms_scale(kv_lat32) * latent_gain).astype(jnp.bfloat16)
    rope_raw = stored(jnp.dot(normed, rope_weight, preferred_element_type=f32))
    cosine_table, sine_table = rope_tables(positions, rope_raw.shape[1])
    rope_keys = rotate(
        rope_raw.astype(f32).reshape(seq_count, token_count, rope_raw.shape[1]),
        cosine_table,
        sine_table,
    ).astype(jnp.bfloat16)
    latent_count = query_up.shape[1] // (NOPE + ROPE)
    query_all = stored(jnp.dot(q_normed, query_up, preferred_element_type=f32)).reshape(
        seq_count, token_count, latent_count, NOPE + ROPE
    )
    query_plain = query_all[..., :NOPE]
    query_turned = rotate(
        query_all[..., NOPE:].astype(f32), cosine_table[:, None, :], sine_table[:, None, :]
    ).astype(jnp.bfloat16)
    score_scale = (NOPE + ROPE) ** (-0.5)
    query_block = positions // BLOCK
    kv_seq = kv_normed.reshape(seq_count, token_count, kv_normed.shape[1])

    def attend_block(totals, key_plain, value_rows, rope_rows, key_start):
        row_max, row_sum, weighted = totals
        key_block = (key_start + jnp.arange(key_plain.shape[1])) // BLOCK
        allowed = key_block[None, :] <= query_block[:, None]
        logits = (
            jnp.einsum("sqhd,skhd->shqk", query_plain, key_plain, preferred_element_type=f32)
            + jnp.einsum("sqhd,skd->shqk", query_turned, rope_rows, preferred_element_type=f32)
        ) * score_scale
        logits = jnp.where(allowed[None, None], logits, -jnp.inf)
        new_max = jnp.maximum(row_max, jnp.max(logits, axis=-1))
        shift = jnp.where(jnp.isfinite(new_max), new_max, 0.0)
        weights = jnp.where(allowed[None, None], jnp.exp(logits - shift[..., None]), 0.0)
        rescale = jnp.exp(row_max - shift)
        row_sum = row_sum * rescale + jnp.sum(weights, axis=-1)
        weighted = weighted * rescale[..., None] + jnp.einsum(
            "shqk,skhd->shqd", weights.astype(jnp.bfloat16), value_rows, preferred_element_type=f32
        )
        return (new_max, row_sum, weighted)

    start_stats = (
        jnp.full((seq_count, latent_count, token_count), -jnp.inf, f32),
        jnp.zeros((seq_count, latent_count, token_count), f32),
        jnp.zeros((seq_count, latent_count, token_count, VDIM), f32),
    )

    def expand_latent(portion, row_start, span_rows):
        latent_rows = lax.dynamic_slice_in_dim(portion[0], row_start, span_rows, 1)
        expanded = jnp.dot(
            latent_rows.reshape(seq_count * span_rows, latent_rows.shape[2]),
            latent_up,
            preferred_element_type=f32,
        ).astype(jnp.bfloat16)
        expanded = expanded.reshape(seq_count, span_rows, latent_count, NOPE + VDIM)
        return (
            expanded[..., :NOPE],
            expanded[..., NOPE:],
            lax.dynamic_slice_in_dim(portion[1], row_start, span_rows, 1),
        )

    portion = (
        lax.all_gather(kv_seq, "sp", axis=1, tiled=True),
        lax.all_gather(rope_keys, "sp", axis=1, tiled=True),
    )
    row_count = portion[0].shape[1]
    span_rows = math.gcd(row_count, token_count * max(1, 512 // token_count))

    def visit_rows(current):

        def visit_block(block_index, stats):
            row_start = block_index * span_rows
            key_plain, value_rows, rope_rows = expand_latent(portion, row_start, span_rows)
            return attend_block(stats, key_plain, value_rows, rope_rows, row_start)

        return lax.fori_loop(0, row_count // span_rows, visit_block, current)

    _, row_sum, weighted = lax.cond(
        jnp.int32(0) < query_start + token_count, visit_rows, keep_same, start_stats
    )
    latent_heads = (
        jnp.transpose(weighted / row_sum[..., None], (0, 2, 1, 3))
        .reshape(row_total, latent_count * VDIM)
        .astype(jnp.bfloat16)
    )
    heads_joined = jnp.concatenate([delta_heads, latent_heads], axis=1)
    out_rows = jnp.concatenate([delta_out, latent_out], axis=0)
    partial_value = jnp.dot(
        heads_joined,
        lax.all_gather(out_rows, ("sp", "fs"), axis=1, tiled=True),
        preferred_element_type=f32,
    )
    mixed_half = lax.psum_scatter(
        partial_value.astype(jnp.bfloat16), "tp", scatter_dimension=1, tiled=True
    ).astype(jnp.float32)
    squares = lax.psum(jnp.sum(mixed_half * mixed_half, axis=1), "tp")
    row_scale = lax.rsqrt(squares / D + NORM_EPS)
    result = mixed_half * row_scale[:, None] * post_gain
    return result.astype(jnp.bfloat16).reshape(seq_count, token_count, result.shape[1])


def pick(array, index):
    return lax.dynamic_index_in_dim(array, index, 0, False)


def dot32(left, right):
    return jnp.dot(left, right, preferred_element_type=jnp.float32)


def dot_t(left, right):
    return lax.dot_general(
        left, right, (((1,), (1,)), ((), ())), preferred_element_type=jnp.float32
    )


def two_parts(values):
    high = values.astype(jnp.bfloat16)
    return high, (values - high.astype(jnp.float32)).astype(jnp.bfloat16)


def fine_dot(left, right, product=dot32):
    left_high, left_low = two_parts(left)
    right_high, right_low = two_parts(right)
    return product(left_high, right_high) + (
        product(left_high, right_low) + product(left_low, right_high)
    )


def kernel_call(body, out_shapes, args, scratch=(), inside=(True, True), outside=0):
    space = pl.BlockSpec(memory_space=pltpu.VMEM)
    operand_space, result_space = (pltpu.VMEM if here else pltpu.HBM for here in inside)
    return pl.pallas_call(
        body,
        out_shape=jax.tree.map(lambda leaf: result_space(leaf.shape, leaf.dtype), out_shapes),
        in_specs=[space] * len(args),
        out_specs=jax.tree.map(lambda _: space, out_shapes),
        scratch_shapes=scratch,
        compiler_params=pltpu.CompilerParams(vmem_limit_bytes=16 * 1024 * 1024),
    )(
        *(
            pltpu.with_memory_space_constraint(arg, pltpu.HBM if i < outside else operand_space)
            for i, arg in enumerate(args)
        )
    )


def started(pairs, sems):
    copies = [pltpu.make_async_copy(*pair, sems.at[i]) for i, pair in enumerate(pairs)]
    for copy in copies:
        copy.start()
    return copies


def outgoing_weights(mixers, lats, sp_size):
    count = len(mixers)
    half = mixers[0].shape[0] // 2
    per_mixer = mixers[0].shape[1] // sp_size
    per_lat = [w.shape[1] // sp_size // 2 for w in lats]
    first_lat = count * per_mixer
    padded = first_lat + 128

    def body(*refs):
        out_ref, own_ref, *held_refs, sems = refs[count + 2 :]
        rows = pl.ds(pl.multiple_of(lax.axis_index("grp") * half, half), half)
        held = started([(ref.at[rows], to) for ref, to in zip(refs, held_refs)], sems)
        first = lax.axis_index("tp") == 0
        for copy in held:
            copy.wait()
        for s in range(sp_size):
            for k in range(count):
                out_ref[s, :, k * per_mixer : (k + 1) * per_mixer] = held_refs[k][
                    :, s * per_mixer : (s + 1) * per_mixer
                ]
            pieces = []
            for ref, per in zip(held_refs[count:], per_lat):
                pair = ref[:, 2 * s * per : 2 * (s + 1) * per]
                pieces.append(jnp.where(first, pair[:, :per], pair[:, per:]))
            pieces.append(jnp.zeros((half, 128 - sum(per_lat)), jnp.bfloat16))
            out_ref[s, :, first_lat:] = jnp.concatenate(pieces, axis=1)
        own_ref[...] = out_ref[lax.axis_index("sp")]

    space = pl.BlockSpec(memory_space=pltpu.VMEM)
    return pl.pallas_call(
        body,
        out_shape=(
            pltpu.HBM((sp_size, half, padded), jnp.bfloat16),
            pltpu.HBM((half, padded), jnp.bfloat16),
        ),
        in_specs=[pl.BlockSpec(memory_space=pl.ANY)] * (count + 2),
        out_specs=(space, space),
        scratch_shapes=(
            *(pltpu.VMEM((half, w.shape[1]), jnp.bfloat16) for w in (*mixers, *lats)),
            pltpu.SemaphoreType.DMA((count + 2,)),
        ),
        name="outgoing_weights",
        compiler_params=pltpu.CompilerParams(vmem_limit_bytes=16 * 1024 * 1024),
    )(*(pltpu.with_memory_space_constraint(w, pltpu.HBM) for w in (*mixers, *lats)))


def outgoing_tokens(tokens, gain, sp_size):
    rows, width = tokens.shape
    block = width // (sp_size * 4)

    def body(token_ref, gain_ref, mine_ref, their_ref):
        values = token_ref[...].astype(jnp.float32)
        normed = (values * rms_scale(values) * gain_ref[...]).astype(jnp.bfloat16)
        first = lax.axis_index("tp") == 0
        for f in range(2):
            for s in range(sp_size):
                begin = (s * 2 + f) * 2 * block
                low = normed[:, begin : begin + block]
                high = normed[:, begin + block : begin + 2 * block]
                at = (f * sp_size + s) * block
                mine_ref[:, at : at + block] = jnp.where(first, low, high)
                their_ref[:, at : at + block] = jnp.where(first, high, low)

    shape = jax.ShapeDtypeStruct((rows, width // 2), jnp.bfloat16)
    return kernel_call(body, (shape, shape), (tokens, gain))


def prepare(narrow, query_up, latent_up, sp_size):
    width = narrow[0].shape[1]
    block = width // (sp_size * 4)
    rank, query_width = query_up.shape
    per_query = query_width // sp_size
    heads = per_query // (NOPE + ROPE)
    per_latent = latent_up.shape[1] // sp_size

    def body(rope_ref, beta_ref, decay_ref, query_ref, latent_ref, narrow_ref, q_ref, kv_ref):
        place = lax.axis_index("sp")
        rows = jnp.concatenate([rope_ref[...], beta_ref[...], decay_ref[...]], axis=0)
        for s in range(sp_size):
            for f in range(2):
                for g in range(2):
                    begin = ((s * 2 + f) * 2 + g) * block
                    at = ((g * 2 + f) * sp_size + s) * block
                    narrow_ref[:, at : at + block] = rows[:, begin : begin + block]
        own = query_ref[:, :per_query]
        for s in range(1, sp_size):
            own = jnp.where(place == s, query_ref[:, s * per_query : (s + 1) * per_query], own)
        pairs = [
            (own[:, h * (NOPE + ROPE) :][:, :NOPE], own[:, h * (NOPE + ROPE) :][:, NOPE : NOPE + ROPE])
            for h in range(heads)
        ]
        parts = [plain for plain, _ in pairs] + [turn for _, turn in pairs]
        for _, turn in pairs:
            parts += [turn[:, ROPE // 2 :], turn[:, : ROPE // 2]]
        q_ref[...] = jnp.concatenate(parts, axis=1)
        kv_ref[...] = latent_ref[:, pl.ds(pl.multiple_of(place * per_latent, 128), per_latent)]

    bf16 = jnp.bfloat16
    return kernel_call(
        body,
        (
            jax.ShapeDtypeStruct((sum(n.shape[0] for n in narrow), width), bf16),
            jax.ShapeDtypeStruct((rank, heads * (NOPE + 2 * ROPE)), bf16),
            jax.ShapeDtypeStruct((latent_up.shape[0], per_latent), bf16),
        ),
        (*narrow, query_up, latent_up),
        inside=(False, True),
    )


def project(mine, theirs, block, peers, extra, sizes):
    seq_count, token_count, fine, q_cols, kv_cols = sizes
    sp_size = len(mine)
    chunk, part = mine[0].shape
    span = sp_size * token_count
    rows = seq_count * span
    piece, columns = peers[0].shape
    extra_width = extra.shape[0]
    q_stack, kv_stack = 128 // q_cols, 128 // kv_cols
    packed = rows // q_stack + rows // kv_stack
    copies = 1 + 3 * (sp_size + 1) + 2 * sp_size

    def body(*refs):
        mine_refs, refs = refs[:sp_size], refs[sp_size:]
        their_refs, refs = refs[:sp_size], refs[sp_size:]
        block_ref, refs = refs[0], refs[1:]
        peer_refs, refs = refs[:9], refs[9:]
        extra_ref, fine_ref, pack_ref, ext_ref, lat_ref, weight_ref, token_ref, sems = refs
        place, fs_at = lax.axis_index("sp"), lax.axis_index("fs")
        tp_at, grp_at = lax.axis_index("tp"), lax.axis_index("grp")
        step = piece // 2

        def rows_at(same_grp, same_fs, source, first, number):
            grp_from = grp_at if same_grp else 1 - grp_at
            block_from = (grp_from * 2 + (fs_at if same_fs else 1 - fs_at)) * sp_size + source
            return weight_ref.at[pl.ds(pl.multiple_of(block_from * piece + first, step), number)]

        moves = [(block_ref, rows_at(True, True, 0, 0, sp_size * piece))]
        half_rows = (sp_size - 1) * step
        for k, flips in enumerate(((True, False), (False, True), (False, False))):
            own_ref, low_ref, high_ref = peer_refs[3 * k : 3 * k + 3]
            moves.append((own_ref, rows_at(*flips, place, 0, piece)))
            for o in range(1, sp_size):
                source = lax.rem(place + o, sp_size)
                begin, end = (o - 1) * piece, o * piece
                cut = min(max(begin, half_rows), end)
                if cut > begin:
                    from_ref = low_ref.at[begin:cut]
                    moves.append((from_ref, rows_at(*flips, source, 0, cut - begin)))
                if end > cut:
                    from_ref = high_ref.at[cut - half_rows : end - half_rows]
                    moves.append((from_ref, rows_at(*flips, source, cut - begin, end - cut)))
        for o in range(sp_size):
            of = pl.ds(o * chunk, chunk)
            at = pl.ds(pl.multiple_of(tp_at * part, part), part)
            moves.append((mine_refs[o], token_ref.at[of, at]))
            at = pl.ds(pl.multiple_of((1 - tp_at) * part, part), part)
            moves.append((their_refs[o], token_ref.at[of, at]))
        assert len(moves) <= copies
        moves = started(moves, sems)
        for copy in moves[: -2 * sp_size]:
            copy.wait()
        for o in range(sp_size):
            for copy in moves[len(moves) - 2 * (sp_size - o) :][:2]:
                copy.wait()
            lhs = token_ref[o * chunk : (o + 1) * chunk, :]
            value = dot32(lhs, weight_ref[...]).astype(jnp.bfloat16)
            outer = dot_t(lhs, extra_ref[...])
            source = lax.bitwise_xor(place, o)
            for n in range(seq_count):
                of = slice(n * token_count, (n + 1) * token_count)
                at = pl.ds(pl.multiple_of(source * token_count, token_count), token_count)
                fine_ref[n, at, :] = value[of, :fine]
                ext_ref[n, at, :] = outer[of]
                at = pl.ds(
                    pl.multiple_of(n * span + source * token_count, token_count), token_count
                )
                lat_ref[at, :] = value[of, fine : fine + 128]
        for start, first, width, count in (
            (0, 0, q_cols, q_stack),
            (rows // q_stack, q_cols, kv_cols, kv_stack),
        ):
            group = rows // count
            joined = jnp.concatenate(
                [
                    lat_ref[k * group : (k + 1) * group, first : first + width]
                    for k in range(count)
                ],
                axis=1,
            )
            for j in range(sp_size):
                pack_ref[j, start : start + group, :] = joined

    space = pl.BlockSpec(memory_space=pltpu.VMEM)
    moved = tuple(
        pltpu.with_memory_space_constraint(array, pltpu.HBM)
        for array in (*mine, *theirs, block, *peers)
    )
    return pl.pallas_call(
        body,
        out_shape=(
            pltpu.VMEM((seq_count, span, fine), jnp.bfloat16),
            pltpu.VMEM((sp_size, packed, 128), jnp.bfloat16),
            pltpu.VMEM((seq_count, span, extra_width), jnp.float32),
        ),
        in_specs=[pl.BlockSpec(memory_space=pl.ANY)] * len(moved) + [space],
        out_specs=(space,) * 3,
        scratch_shapes=(
            pltpu.VMEM((rows, 128), jnp.bfloat16),
            pltpu.VMEM((2 * part, columns), jnp.bfloat16),
            pltpu.VMEM((rows, 2 * part), jnp.bfloat16),
            pltpu.SemaphoreType.DMA((copies,)),
        ),
        name="project",
        compiler_params=pltpu.CompilerParams(vmem_limit_bytes=16 * 1024 * 1024),
    )(*moved, pltpu.with_memory_space_constraint(extra, pltpu.VMEM))


def send_by_pair(out_refs, pieces, sp_size):
    place = lax.axis_index("sp")
    for step, out_ref in enumerate(out_refs):
        second = lax.rem(place + step, sp_size) >= sp_size // 2
        for n, (low, high) in enumerate(pieces):
            rows = low.shape[0]
            out_ref[n * rows : (n + 1) * rows, :] = jnp.where(second, high, low)


def lower_inverses(lowers, base):
    size = lowers[0].shape[0]
    row = lax.broadcasted_iota(jnp.int32, (size, size), 0)
    col = lax.broadcasted_iota(jnp.int32, (size, size), 1)
    unit = jnp.where(row == col, 1.0, 0.0)
    powers = [jnp.where(row // base == col // base, low, 0.0) for low in lowers]
    inverses = [unit - p for p in powers]
    reach = 2
    while reach < base:
        powers = [fine_dot(p, p) for p in powers]
        inverses = [i + fine_dot(i, p) for i, p in zip(inverses, powers)]
        reach *= 2
    block = base
    while block < size:
        joint = (row // (2 * block) == col // (2 * block)) & (row // block != col // block)
        moved = [fine_dot(i, jnp.where(joint, low, 0.0)) for i, low in zip(inverses, lowers)]
        inverses = [i - fine_dot(m, i) for i, m in zip(inverses, moved)]
        block *= 2
    return inverses


def delta_mix(fine, ext, gains, gain_at, gates, gate_at, heads, sp_size):
    seq_count, span, _ = fine.shape
    tile = math.gcd(span, 128)
    tiles = span // tile

    def terms(raw_query, raw_key, raw_value, beta_pre, decay_pre, rate):
        query = unit_rows(jax.nn.silu(raw_query)) * HEAD ** (-0.5)
        key = unit_rows(jax.nn.silu(raw_key))
        value = jax.nn.silu(raw_value)
        beta = jax.nn.sigmoid(beta_pre)
        log_decay = -rate * jax.nn.softplus(decay_pre)
        row = lax.broadcasted_iota(jnp.int32, (span, span), 0)
        col = lax.broadcasted_iota(jnp.int32, (span, span), 1)
        as_row = jnp.sum(jnp.where(row == col, log_decay, 0.0), axis=0, keepdims=True)
        gate = jnp.sum(jnp.where(row >= col, as_row, 0.0), axis=1, keepdims=True)
        gate_row = jnp.sum(jnp.where(row == col, gate, 0.0), axis=0, keepdims=True)
        decay = jnp.where(row >= col, jnp.exp(jnp.where(row >= col, gate - gate_row, 0.0)), 0.0)
        lower = fine_dot(key * beta, key, dot_t) * jnp.where(row > col, decay, 0.0)
        scores = fine_dot(query, key, dot_t) * decay
        return lower, scores, value * beta

    def body(fine_ref, ext_ref, gain_ref, *out_refs):
        gain_row = gain_ref[:, gain_at : gain_at + HEAD]
        rate_row = gain_ref[:, gain_at + HEAD : gain_at + 2 * HEAD]
        first_head = (lax.axis_index("tp") * sp_size + lax.axis_index("sp")) * heads
        lane = lax.broadcasted_iota(jnp.int32, (span, ext.shape[2]), 1)
        rate_lane = lax.broadcasted_iota(jnp.int32, (1, HEAD), 1)
        chains = []
        for n in range(seq_count):
            for h in range(heads):
                raw = [
                    fine_ref[n, :, (k * heads + h) * HEAD : (k * heads + h + 1) * HEAD].astype(
                        jnp.float32
                    )
                    for k in range(3)
                ]
                head = first_head + h
                outer = ext_ref[n]
                beta_pre, decay_pre = (
                    jnp.sum(
                        jnp.where(lane == gate_at + k * gates + head, outer, 0.0),
                        axis=1,
                        keepdims=True,
                    )
                    for k in range(2)
                )
                rate = jnp.sum(
                    jnp.where(rate_lane == head, rate_row, 0.0), axis=1, keepdims=True
                )
                chains.append(terms(*raw, beta_pre, decay_pre, rate))
        cuts = [slice(j * tile, (j + 1) * tile) for j in range(tiles)]
        inverses = lower_inverses([c[0][cut, cut] for c in chains for cut in cuts], 8)
        solved = [[] for _ in chains]
        for j, cut in enumerate(cuts):
            for i, (lower, _, wanted) in enumerate(chains):
                rest = wanted[cut]
                if j:
                    rest = rest - fine_dot(
                        lower[cut, : j * tile], jnp.concatenate(solved[i], axis=0)
                    )
                solved[i].append(fine_dot(inverses[i * tiles + j], rest))
        pieces = []
        for i, (_, scores, _) in enumerate(chains):
            out = fine_dot(scores, jnp.concatenate(solved[i], axis=0))
            out = (out * rms_scale(out) * gain_row).astype(jnp.bfloat16)
            pieces.append((out[: span // 2], out[span // 2 :]))
        for h in range(heads):
            columns = slice(h * HEAD, (h + 1) * HEAD)
            views = [ref.at[:, columns] for ref in out_refs] if heads > 1 else out_refs
            send_by_pair(views, pieces[h::heads], sp_size)

    shape = jax.ShapeDtypeStruct((seq_count * span // 2, heads * HEAD), jnp.bfloat16)
    return kernel_call(body, (shape,) * sp_size, (fine, ext, gains), inside=(True, False))


def latent_mix(mine, theirs, ext, tables, gains, ups, q_cols, kv_cols, heads):
    sp_size = mine.shape[0]
    seq_count, span, _ = ext.shape
    rows = seq_count * span
    q_rank, kv_rank = ups[0].shape[0], ups[1].shape[0]
    scale = (NOPE + ROPE) ** (-0.5)

    def unpack(value, n, base, width):
        group = rows * width // 128
        pieces = []
        for k in range(128 // width):
            if n * span < (k + 1) * group and k * group < (n + 1) * span:
                low = max(n * span - k * group, 0)
                high = min((n + 1) * span - k * group, group)
                pieces.append(
                    value[base + low : base + high, k * width : (k + 1) * width]
                )
        return jnp.concatenate(pieces, axis=0) if len(pieces) > 1 else pieces[0]

    def body(mine_ref, their_ref, ext_ref, cos_ref, sin_ref, *refs):
        gain_ref, qup_ref, kup_ref, *out_refs = refs
        q_gain = gain_ref[:, :q_rank]
        kv_gain = gain_ref[:, q_rank : q_rank + kv_rank]
        first = lax.axis_index("tp") == 0
        row = lax.broadcasted_iota(jnp.int32, (span, span), 0) // BLOCK
        col = lax.broadcasted_iota(jnp.int32, (span, span), 1) // BLOCK
        allowed = col <= row
        cosine, sine = cos_ref[...], sin_ref[...]
        pairs = []
        for s in range(sp_size):
            own, other = mine_ref[s], their_ref[s]
            pairs += [jnp.where(first, own, other), jnp.where(first, other, own)]
        joins = []
        for n in range(seq_count):
            q_parts = [unpack(p, n, 0, q_cols) for p in pairs]
            kv_parts = [unpack(p, n, rows * q_cols // 128, kv_cols) for p in pairs]
            q_lat = jnp.concatenate(q_parts, axis=1).astype(jnp.float32)
            kv_lat = jnp.concatenate(kv_parts, axis=1).astype(jnp.float32)
            q_norm = (q_lat * rms_scale(q_lat) * q_gain).astype(jnp.bfloat16)
            kv_norm = (kv_lat * rms_scale(kv_lat) * kv_gain).astype(jnp.bfloat16)
            q_all = dot32(q_norm, qup_ref[...]).astype(jnp.bfloat16)
            kv_all = dot32(kv_norm, kup_ref[...]).astype(jnp.bfloat16)
            plain_width, turn_width = heads * NOPE, heads * ROPE
            plain = q_all[:, :plain_width]
            turn = q_all[:, plain_width : plain_width + turn_width].astype(jnp.float32)
            swapped = q_all[:, plain_width + turn_width :].astype(jnp.float32)
            turned = (turn * cosine + swapped * sine).astype(jnp.bfloat16)
            raw = ext_ref[n, :, :ROPE].astype(jnp.bfloat16).astype(jnp.float32)
            back = jnp.concatenate([raw[:, ROPE // 2 :], raw[:, : ROPE // 2]], axis=1)
            key_turn = (raw * cosine[:, :ROPE] + back * sine[:, :ROPE]).astype(jnp.bfloat16)
            results = []
            for h in range(heads):
                key_plain = kv_all[:, h * (NOPE + VDIM) : h * (NOPE + VDIM) + NOPE]
                values = kv_all[:, h * (NOPE + VDIM) + NOPE : (h + 1) * (NOPE + VDIM)]
                logits = (
                    dot_t(plain[:, h * NOPE : (h + 1) * NOPE], key_plain)
                    + dot_t(turned[:, h * ROPE : (h + 1) * ROPE], key_turn)
                ) * scale
                logits = jnp.where(allowed, logits, -jnp.inf)
                peak = jnp.max(logits, axis=-1, keepdims=True)
                weights = jnp.exp(logits - peak)
                total = jnp.sum(weights, axis=-1, keepdims=True)
                results.append(dot32(weights.astype(jnp.bfloat16), values) / total)
            joined = jnp.concatenate(results, axis=1).astype(jnp.bfloat16)
            joins.append((joined[: span // 2], joined[span // 2 :]))
        send_by_pair(out_refs, joins, sp_size)

    shape = jax.ShapeDtypeStruct((rows // 2, heads * VDIM), jnp.bfloat16)
    return kernel_call(
        body, (shape,) * sp_size, (mine, theirs, ext, *tables, gains, *ups), outside=1
    )


def output_partial(delta_all, latent_all, near, near_fs, far, gain, sizes):
    seq_count, token_count = sizes
    sp_size = len(delta_all)
    rows, d_width = delta_all[0].shape
    l_width = latent_all[0].shape[1]
    total, columns = near.shape
    half = total // 2
    per_half = sp_size // 2

    def body(*refs):
        d_refs, refs = refs[:sp_size], refs[sp_size:]
        l_refs, refs = refs[:sp_size], refs[sp_size:]
        near_ref, near_fs_ref, *far_refs, gain_ref, keep_ref, pass_ref, kept_ref, lhs_ref = refs
        kept_ref[...] = gain_ref[...]
        place, fs_at = lax.axis_index("sp"), lax.axis_index("fs")
        grp_at = lax.axis_index("grp")
        for o in range(sp_size):
            source = lax.rem(place + o, sp_size)
            base = (source // per_half) * half
            within = lax.rem(source, per_half)
            at = pl.multiple_of(base + within * d_width, 128)
            lhs_ref[:, pl.ds(at, d_width)] = d_refs[o][...]
            at = pl.multiple_of(base + per_half * d_width + within * l_width, 128)
            lhs_ref[:, pl.ds(at, l_width)] = l_refs[o][...]
        lhs = lhs_ref[...]
        own = lhs_ref[:, pl.ds(pl.multiple_of(grp_at * half, half), half)]
        other = lhs_ref[:, pl.ds(pl.multiple_of((1 - grp_at) * half, half), half)]
        close = (
            dot32(lhs, near_ref[...]).astype(jnp.bfloat16),
            dot32(lhs, near_fs_ref[...]).astype(jnp.bfloat16),
        )
        away = tuple(
            (dot32(own, far_refs[k][...]) + dot32(other, far_refs[k + 1][...])).astype(jnp.bfloat16)
            for k in (0, 2)
        )
        straight = place // per_half == lax.axis_index("tp")
        for k in range(2):
            begin = (1 - fs_at) if k else fs_at
            at = pl.ds(pl.multiple_of(begin * columns, columns), columns)
            keep = jnp.where(straight, close[k], away[k])
            onward = jnp.where(straight, away[k], close[k])
            pair_rows = 2 * token_count
            for n in range(seq_count):
                for p in range(2):
                    of = slice(n * pair_rows + p * token_count, n * pair_rows + (p + 1) * token_count)
                    to = slice(n * token_count, (n + 1) * token_count)
                    keep_ref[p, to, at] = keep[of]
                    pass_ref[p, to, at] = onward[of]

    shape = jax.ShapeDtypeStruct((2, rows // 2, 2 * columns), jnp.bfloat16)
    return kernel_call(
        body,
        (shape, shape, jax.ShapeDtypeStruct(gain.shape, gain.dtype)),
        (*delta_all, *latent_all, near, near_fs, *far, gain),
        scratch=(pltpu.VMEM((rows, total), jnp.bfloat16),),
    )


def whole_tables(length, repeats):
    frequency = ROPE_THETA ** (-np.arange(0, ROPE, 2, dtype=np.float32) / np.float32(ROPE))
    angles = np.arange(length, dtype=np.float32)[:, None] * frequency[None, :].astype(np.float32)
    cosine, sine = np.cos(angles), np.sin(angles)
    return tuple(
        jnp.asarray(np.tile(np.concatenate(pair, axis=1), (1, repeats)), jnp.float32)
        for pair in ((cosine, cosine), (-sine, sine))
    )


def whole_sequences(
    tokens,
    pre_gain,
    query_weight,
    key_weight,
    value_weight,
    beta_weight,
    decay_weight,
    decay_rate,
    delta_gain,
    query_down,
    latent_down,
    rope_weight,
    query_gain,
    latent_gain,
    query_up,
    latent_up,
    delta_out,
    latent_out,
    post_gain,
):
    f32, bf16 = jnp.float32, jnp.bfloat16
    sp_size, tp_size = lax.axis_size("sp"), lax.axis_size("tp")
    place, grp_at = lax.axis_index("sp"), lax.axis_index("grp")
    seq_count, token_count, width = tokens.shape
    rows = seq_count * token_count
    heads = query_weight.shape[1] // HEAD // sp_size
    shares = sp_size * tp_size
    q_cols, kv_cols = query_down.shape[1] // shares, latent_down.shape[1] // shares

    def exchange(values, axis):
        return lax.all_to_all(values, axis, 0, 0, tiled=True)

    def swap(values, axis):
        return lax.ppermute(values, axis, [(0, 1), (1, 0)])

    def along(values, step):
        return lax.ppermute(values, "sp", [(i, (i + step) % sp_size) for i in range(sp_size)])

    def from_sp(sends):
        return [sends[0]] + [along(sends[step], step) for step in range(sp_size - 1, 0, -1)]

    outgoing, own_piece = outgoing_weights(
        (query_weight, key_weight, value_weight), (query_down, latent_down), sp_size
    )
    block = exchange(outgoing, "sp")
    token_rows, outgoing = lax.optimization_barrier((tokens.reshape(rows, width), outgoing))

    own_half, other_half = outgoing_tokens(token_rows, pre_gain[None, :], sp_size)

    def beside(values):
        return lax.ppermute(values, "sp", [(i, i ^ 1) for i in range(sp_size)])

    far_half = along(own_half, sp_size // 2)
    mine = [own_half, beside(own_half), far_half, beside(far_half)]
    theirs = [other_half] + [swap(piece, "tp") for piece in mine[1:]]

    quarter = delta_out.shape[0] // 2
    near = jnp.concatenate(
        [w[k * quarter : (k + 1) * quarter] for k in range(2) for w in (delta_out, latent_out)]
    )
    near_fs = swap(near, "fs")

    own_grp, own_fs = swap(own_piece, "grp"), swap(own_piece, "fs")
    own_corner = swap(own_grp, "fs")
    rest = lax.dynamic_slice_in_dim(jnp.concatenate([block, block]), place + 1, sp_size - 1, 0)
    rest = rest.reshape(-1, rest.shape[2])
    block = block.reshape(-1, block.shape[2])
    middle = rest.shape[0] // 2
    low, high = rest[:middle], rest[middle:]
    low_grp, high_fs = swap(low, "grp"), swap(high, "fs")
    high_grp, low_fs = swap(high, "grp"), swap(low, "fs")
    corner = swap(low_grp, "fs"), swap(high_fs, "grp")
    peers = (own_fs, low_fs, high_fs, own_grp, low_grp, high_grp, own_corner, *corner)

    far_own = lax.dynamic_slice_in_dim(near, grp_at * 2 * quarter, 2 * quarter, 0)
    far_own = along(far_own, sp_size // 2)
    far_other = swap(far_own, "grp")
    far = (far_own, far_other, swap(far_own, "fs"))
    far = (*far, swap(far_other, "fs"))

    gate_at = rope_weight.shape[1]
    latent_heads = query_up.shape[1] // (NOPE + ROPE) // sp_size
    extra, q_up, kv_up = prepare(
        (rope_weight.T, beta_weight.T, decay_weight.T), query_up, latent_up, sp_size
    )
    tables = whole_tables(sp_size * token_count, latent_heads)
    rates = jnp.pad(decay_rate, (0, HEAD - decay_rate.shape[0]))
    latent_gains = jnp.concatenate([query_gain, latent_gain])[None, :]
    gains = jnp.concatenate([delta_gain, rates])[None, :]
    mine[1], gains, latent_gains = lax.optimization_barrier((mine[1], gains, latent_gains))

    fine, lat, ext = project(
        mine,
        theirs,
        block,
        peers,
        extra,
        (seq_count, token_count, 3 * heads * HEAD, q_cols, kv_cols),
    )
    lat_mine = exchange(lat, "sp")
    delta_sends = delta_mix(
        fine, ext, gains, 0, decay_rate.shape[0], gate_at, heads, sp_size
    )
    lat_mine, _ = lax.optimization_barrier((lat_mine, delta_sends))
    lat_theirs = swap(lat_mine, "tp")
    delta_all = from_sp(delta_sends)
    latent_sends = latent_mix(
        lat_mine,
        lat_theirs,
        ext,
        tables,
        latent_gains,
        (q_up, kv_up),
        q_cols,
        kv_cols,
        latent_heads,
    )
    latent_all = from_sp(latent_sends)

    keep, onward, post_row = output_partial(
        delta_all, latent_all, near, near_fs, far, post_gain[None, :], (seq_count, token_count)
    )
    mixed = (keep.astype(f32) + swap(onward, "tp").astype(f32)).astype(bf16)
    side = lax.rem(place, 2)

    def across(values):
        return lax.ppermute(pick(values, 1 - side), "sp", [(i, i ^ 1) for i in range(sp_size)])

    there = across(mixed)
    squares = jnp.sum(mixed.astype(f32) * mixed.astype(f32), axis=2)
    squares = squares + swap(squares, "tp")
    squares = (pick(squares, side) + across(squares))[:, None]
    here, there = pick(mixed, side).astype(f32), there.astype(f32)
    final = jnp.concatenate(
        [jnp.where(side == 0, here, there), jnp.where(side == 0, there, here)], axis=1
    )
    result = final * lax.rsqrt(squares / D + NORM_EPS) * post_row
    return result.astype(bf16).reshape(seq_count, token_count, final.shape[1])


def fits_whole(mesh):
    shape = mesh.shape
    return all(shape[name] == 2 for name in ("grp", "fs", "tp")) and shape["sp"] == 4


def solution(mesh):
    def chosen(*args):
        head_count = args[2].shape[1] // HEAD
        latent_count = args[14].shape[1] // (NOPE + ROPE)
        sp_size = mesh.shape["sp"]
        whole = fits_whole(mesh) and head_count % sp_size == 0 and latent_count % sp_size == 0
        return (whole_sequences if whole else local)(*args)

    return jax.shard_map(
        chosen,
        mesh=mesh,
        in_specs=(
            P(("grp", "fs"), "sp", None),
            P(),
            P(("sp", "fs"), "tp"),
            P(("sp", "fs"), "tp"),
            P(("sp", "fs"), "tp"),
            P(),
            P(),
            P(),
            P(),
            P(("sp", "fs"), None),
            P(("sp", "fs"), None),
            P(),
            P(),
            P(),
            P(None, "tp"),
            P(None, "tp"),
            P("tp", ("sp", "fs")),
            P("tp", ("sp", "fs")),
            P("tp"),
        ),
        out_specs=P(("grp", "fs"), "sp", "tp"),
        check_vma=False,
    )
```

```python
import math

import jax
import jax.numpy as jnp
import numpy as np
from jax import lax
from jax.experimental import pallas as pl
from jax.experimental.pallas import tpu as pltpu
from jax.sharding import PartitionSpec as P


D = 2048
HEAD = 128
NOPE = 64
ROPE = 32
VDIM = 64
BLOCK = 64


NORM_EPS = 1e-06
ROPE_THETA = 10000.0
HIGHEST = lax.Precision.HIGHEST


def prefix(array, axis, join, neutral):
    place = lax.axis_index(axis)
    gathered = jax.tree.map(
        lambda a, kind: lax.all_gather(a.astype(kind), axis), array, (jnp.bfloat16, jnp.bfloat16)
    )
    state = jax.tree.map(lambda a, e: jnp.zeros_like(a) + jnp.asarray(e, a.dtype), array, neutral)

    def one(step, state):
        return join(
            state,
            jax.tree.map(
                lambda a, own: lax.dynamic_index_in_dim(a, step, 0, False).astype(own.dtype),
                gathered,
                array,
            ),
        )

    return lax.fori_loop(0, place, one, state)


def stored(values):
    return lax.optimization_barrier(values.astype(jnp.bfloat16))


def rms_scale(values):
    return lax.rsqrt(jnp.mean(values * values, axis=-1, keepdims=True) + NORM_EPS)


def unit_rows(values):
    return values * lax.rsqrt(jnp.sum(values * values, axis=-1, keepdims=True) + NORM_EPS)


def rope_tables(positions, rope_width):
    frequency = ROPE_THETA ** (-jnp.arange(0, rope_width, 2, dtype=jnp.float32) / rope_width)
    angles = positions.astype(jnp.float32)[:, None] * frequency[None, :]
    return (jnp.cos(angles), jnp.sin(angles))


def rotate(values, cosine_table, sine_table):
    lower_half, upper_half = jnp.split(values, 2, axis=-1)
    return jnp.concatenate(
        [
            lower_half * cosine_table - upper_half * sine_table,
            upper_half * cosine_table + lower_half * sine_table,
        ],
        axis=-1,
    )


def delta_terms(query_vectors, key_vectors, value_vectors, beta_gate, log_decay):
    length, head_count, _ = query_vectors.shape
    nblocks = length // BLOCK

    def split_blocks(tensor):
        return jnp.moveaxis(tensor.reshape((nblocks, BLOCK, head_count) + tensor.shape[2:]), 2, 0)

    query_vectors = split_blocks(query_vectors)
    key_vectors = split_blocks(key_vectors)
    value_vectors = split_blocks(value_vectors)
    beta_gate = split_blocks(beta_gate)
    gate_sum = jnp.cumsum(split_blocks(log_decay), axis=-1)
    position = jnp.arange(BLOCK)
    strict = position[:, None] > position[None, :]
    causal = position[:, None] >= position[None, :]
    gate_gap = gate_sum[..., :, None] - gate_sum[..., None, :]
    strict_decay = jnp.where(strict, jnp.exp(jnp.where(strict, gate_gap, 0.0)), 0.0)
    causal_decay = jnp.where(causal, jnp.exp(jnp.where(causal, gate_gap, 0.0)), 0.0)
    keys_scaled = key_vectors * beta_gate[..., None]
    lower_mat = (
        jnp.einsum("hnid,hnjd->hnij", keys_scaled, key_vectors, precision=HIGHEST) * strict_decay
    )
    identity = jnp.eye(BLOCK, dtype=jnp.float32)
    inverse = jax.scipy.linalg.solve_triangular(
        identity + lower_mat, jnp.broadcast_to(identity, lower_mat.shape), lower=True
    )
    new_values = jnp.einsum(
        "hnij,hnjd->hnid", inverse, value_vectors * beta_gate[..., None], precision=HIGHEST
    )
    key_weights = jnp.einsum(
        "hnij,hnjd->hnid", inverse, keys_scaled * jnp.exp(gate_sum)[..., None], precision=HIGHEST
    )
    scores = (
        jnp.einsum("hnid,hnjd->hnij", query_vectors, key_vectors, precision=HIGHEST) * causal_decay
    )
    last_gate = gate_sum[..., -1]
    query_decay = query_vectors * jnp.exp(gate_sum)[..., None]
    key_decay = key_vectors * jnp.exp(last_gate[..., None] - gate_sum)[..., None]
    return (query_decay, key_decay, new_values, key_weights, scores, last_gate)


def compose(earlier, following):
    return (
        jnp.einsum("hij,hjk->hik", following[0], earlier[0], precision=HIGHEST),
        jnp.einsum("hij,hjk->hik", following[0], earlier[1], precision=HIGHEST) + following[1],
    )


def keep_same(current):
    return current


def local(
    tokens,
    pre_gain,
    query_weight,
    key_weight,
    value_weight,
    beta_weight,
    decay_weight,
    decay_rate,
    delta_gain,
    query_down,
    latent_down,
    rope_weight,
    query_gain,
    latent_gain,
    query_up,
    latent_up,
    delta_out,
    latent_out,
    post_gain,
):
    f32 = jnp.float32
    seq_count, token_count = (tokens.shape[0], tokens.shape[1])
    row_total = seq_count * token_count
    sequence = tokens.reshape(row_total, tokens.shape[2]).astype(f32)
    query_start = lax.axis_index("sp") * token_count
    positions = query_start + jnp.arange(token_count)
    normed = (sequence * rms_scale(sequence) * pre_gain).astype(jnp.bfloat16)
    head_group = lax.axis_index("tp")
    q_width = query_down.shape[1] // lax.axis_size("tp")
    kv_width = latent_down.shape[1] // lax.axis_size("tp")
    q_own = lax.dynamic_slice_in_dim(query_down, head_group * q_width, q_width, 1)
    kv_own = lax.dynamic_slice_in_dim(latent_down, head_group * kv_width, kv_width, 1)
    portion = (
        lax.all_gather(query_weight, ("sp", "fs"), axis=0, tiled=True),
        lax.all_gather(key_weight, ("sp", "fs"), axis=0, tiled=True),
        lax.all_gather(value_weight, ("sp", "fs"), axis=0, tiled=True),
        lax.all_gather(q_own, ("sp", "fs"), axis=0, tiled=True),
        lax.all_gather(kv_own, ("sp", "fs"), axis=0, tiled=True),
    )
    row_count = portion[0].shape[0]
    projected = tuple((jnp.dot(normed, weight, preferred_element_type=f32) for weight in portion))
    raw_query, raw_key, raw_value, q_half, kv_half = tuple((stored(member) for member in projected))
    q_latent, kv_latent = (
        lax.all_gather(q_half, "tp", axis=1, tiled=True),
        lax.all_gather(kv_half, "tp", axis=1, tiled=True),
    )
    head_count = query_weight.shape[1] // HEAD
    lane_count = seq_count * head_count
    beta_full = jax.nn.sigmoid(jnp.dot(normed, beta_weight, preferred_element_type=f32))
    beta_gate = lax.dynamic_slice_in_dim(beta_full, head_group * head_count, head_count, 1)
    decay_full = jnp.dot(normed, decay_weight, preferred_element_type=f32)
    decay_pre = lax.dynamic_slice_in_dim(decay_full, head_group * head_count, head_count, 1)
    decay_local = lax.dynamic_slice_in_dim(decay_rate, head_group * head_count, head_count, 0)
    log_decay = -decay_local[None, :] * jax.nn.softplus(decay_pre)

    def by_position(values):
        shaped = values.reshape((seq_count, token_count) + values.shape[1:])
        shaped = jnp.moveaxis(shaped, 0, 1)
        return shaped.reshape((token_count, seq_count * values.shape[1]) + values.shape[2:])

    query_vectors = by_position(
        unit_rows(jax.nn.silu(raw_query.astype(f32)).reshape(row_total, head_count, HEAD))
        * HEAD ** (-0.5)
    )
    key_vectors = by_position(
        unit_rows(jax.nn.silu(raw_key.astype(f32)).reshape(row_total, head_count, HEAD))
    )
    value_vectors = by_position(
        jax.nn.silu(raw_value.astype(f32)).reshape(row_total, head_count, HEAD)
    )
    block_terms = delta_terms(
        query_vectors, key_vectors, value_vectors, by_position(beta_gate), by_position(log_decay)
    )
    inputs = tuple((jnp.moveaxis(tensor, 1, 0) for tensor in block_terms))

    def advance(totals, block_in):
        carried, transfer = totals
        query_decay, key_decay, new_values, key_weights, scores, last_gate = block_in
        corrected = new_values - jnp.einsum("hcd,hde->hce", key_weights, carried, precision=HIGHEST)
        output = jnp.einsum("hcd,hde->hce", query_decay, carried, precision=HIGHEST) + jnp.einsum(
            "hij,hje->hie", scores, corrected, precision=HIGHEST
        )
        reader_rows = query_decay - jnp.einsum(
            "hij,hjd->hid", scores, key_weights, precision=HIGHEST
        )
        reader = jnp.einsum("hcd,hde->hce", reader_rows, transfer, precision=HIGHEST)
        factor = jnp.exp(last_gate)[:, None, None]
        carried = carried * factor + jnp.einsum(
            "hcd,hce->hde", key_decay, corrected, precision=HIGHEST
        )
        moved = jnp.einsum("hcd,hde->hce", key_weights, transfer, precision=HIGHEST)
        transfer = transfer * factor - jnp.einsum(
            "hcd,hce->hde", key_decay, moved, precision=HIGHEST
        )
        return ((carried, transfer), (output, reader))

    eye_stack = jnp.broadcast_to(jnp.eye(HEAD, dtype=f32), (lane_count, HEAD, HEAD))
    zero_state = jnp.zeros((lane_count, HEAD, HEAD), f32)
    (state_end, transfer_end), (outputs, readers) = lax.scan(
        advance, (zero_state, eye_stack), inputs
    )
    _, incoming = prefix((transfer_end, state_end), "sp", compose, (eye_stack, zero_state))
    outputs = outputs + jnp.einsum("nhcd,hde->nhce", readers, incoming, precision=HIGHEST)
    delta_raw = jnp.transpose(outputs, (0, 2, 1, 3)).reshape(
        token_count, seq_count, head_count, HEAD
    )
    delta_raw = jnp.moveaxis(delta_raw, 1, 0).reshape(row_total, head_count, HEAD)
    delta_heads = (
        (delta_raw * rms_scale(delta_raw) * delta_gain)
        .astype(jnp.bfloat16)
        .reshape(row_total, head_count * HEAD)
    )
    q_lat32 = q_latent.astype(f32)
    kv_lat32 = kv_latent.astype(f32)
    q_normed = (q_lat32 * rms_scale(q_lat32) * query_gain).astype(jnp.bfloat16)
    kv_normed = (kv_lat32 * rms_scale(kv_lat32) * latent_gain).astype(jnp.bfloat16)
    rope_raw = stored(jnp.dot(normed, rope_weight, preferred_element_type=f32))
    cosine_table, sine_table = rope_tables(positions, rope_raw.shape[1])
    rope_keys = rotate(
        rope_raw.astype(f32).reshape(seq_count, token_count, rope_raw.shape[1]),
        cosine_table,
        sine_table,
    ).astype(jnp.bfloat16)
    latent_count = query_up.shape[1] // (NOPE + ROPE)
    query_all = stored(jnp.dot(q_normed, query_up, preferred_element_type=f32)).reshape(
        seq_count, token_count, latent_count, NOPE + ROPE
    )
    query_plain = query_all[..., :NOPE]
    query_turned = rotate(
        query_all[..., NOPE:].astype(f32), cosine_table[:, None, :], sine_table[:, None, :]
    ).astype(jnp.bfloat16)
    score_scale = (NOPE + ROPE) ** (-0.5)
    query_block = positions // BLOCK
    kv_seq = kv_normed.reshape(seq_count, token_count, kv_normed.shape[1])

    def attend_block(totals, key_plain, value_rows, rope_rows, key_start):
        row_max, row_sum, weighted = totals
        key_block = (key_start + jnp.arange(key_plain.shape[1])) // BLOCK
        allowed = key_block[None, :] <= query_block[:, None]
        logits = (
            jnp.einsum("sqhd,skhd->shqk", query_plain, key_plain, preferred_element_type=f32)
            + jnp.einsum("sqhd,skd->shqk", query_turned, rope_rows, preferred_element_type=f32)
        ) * score_scale
        logits = jnp.where(allowed[None, None], logits, -jnp.inf)
        new_max = jnp.maximum(row_max, jnp.max(logits, axis=-1))
        shift = jnp.where(jnp.isfinite(new_max), new_max, 0.0)
        weights = jnp.where(allowed[None, None], jnp.exp(logits - shift[..., None]), 0.0)
        rescale = jnp.exp(row_max - shift)
        row_sum = row_sum * rescale + jnp.sum(weights, axis=-1)
        weighted = weighted * rescale[..., None] + jnp.einsum(
            "shqk,skhd->shqd", weights.astype(jnp.bfloat16), value_rows, preferred_element_type=f32
        )
        return (new_max, row_sum, weighted)

    start_stats = (
        jnp.full((seq_count, latent_count, token_count), -jnp.inf, f32),
        jnp.zeros((seq_count, latent_count, token_count), f32),
        jnp.zeros((seq_count, latent_count, token_count, VDIM), f32),
    )

    def expand_latent(portion, row_start, span_rows):
        latent_rows = lax.dynamic_slice_in_dim(portion[0], row_start, span_rows, 1)
        expanded = jnp.dot(
            latent_rows.reshape(seq_count * span_rows, latent_rows.shape[2]),
            latent_up,
            preferred_element_type=f32,
        ).astype(jnp.bfloat16)
        expanded = expanded.reshape(seq_count, span_rows, latent_count, NOPE + VDIM)
        return (
            expanded[..., :NOPE],
            expanded[..., NOPE:],
            lax.dynamic_slice_in_dim(portion[1], row_start, span_rows, 1),
        )

    portion = (
        lax.all_gather(kv_seq, "sp", axis=1, tiled=True),
        lax.all_gather(rope_keys, "sp", axis=1, tiled=True),
    )
    row_count = portion[0].shape[1]
    span_rows = math.gcd(row_count, token_count * max(1, 512 // token_count))

    def visit_rows(current):

        def visit_block(block_index, stats):
            row_start = block_index * span_rows
            key_plain, value_rows, rope_rows = expand_latent(portion, row_start, span_rows)
            return attend_block(stats, key_plain, value_rows, rope_rows, row_start)

        return lax.fori_loop(0, row_count // span_rows, visit_block, current)

    _, row_sum, weighted = lax.cond(
        jnp.int32(0) < query_start + token_count, visit_rows, keep_same, start_stats
    )
    latent_heads = (
        jnp.transpose(weighted / row_sum[..., None], (0, 2, 1, 3))
        .reshape(row_total, latent_count * VDIM)
        .astype(jnp.bfloat16)
    )
    heads_joined = jnp.concatenate([delta_heads, latent_heads], axis=1)
    out_rows = jnp.concatenate([delta_out, latent_out], axis=0)
    partial_value = jnp.dot(
        heads_joined,
        lax.all_gather(out_rows, ("sp", "fs"), axis=1, tiled=True),
        preferred_element_type=f32,
    )
    mixed_half = lax.psum_scatter(
        partial_value.astype(jnp.bfloat16), "tp", scatter_dimension=1, tiled=True
    ).astype(jnp.float32)
    squares = lax.psum(jnp.sum(mixed_half * mixed_half, axis=1), "tp")
    row_scale = lax.rsqrt(squares / D + NORM_EPS)
    result = mixed_half * row_scale[:, None] * post_gain
    return result.astype(jnp.bfloat16).reshape(seq_count, token_count, result.shape[1])


def pick(array, index):
    return lax.dynamic_index_in_dim(array, index, 0, False)


def dot32(left, right):
    return jnp.dot(left, right, preferred_element_type=jnp.float32)


def dot_t(left, right):
    return lax.dot_general(
        left, right, (((1,), (1,)), ((), ())), preferred_element_type=jnp.float32
    )


def two_parts(values):
    high = values.astype(jnp.bfloat16)
    return high, (values - high.astype(jnp.float32)).astype(jnp.bfloat16)


def fine_dot(left, right, product=dot32):
    left_high, left_low = two_parts(left)
    right_high, right_low = two_parts(right)
    return product(left_high, right_high) + (
        product(left_high, right_low) + product(left_low, right_high)
    )


def kernel_call(body, out_shapes, args, scratch=(), inside=(True, True), outside=0):
    space = pl.BlockSpec(memory_space=pltpu.VMEM)
    operand_space, result_space = (pltpu.VMEM if here else pltpu.HBM for here in inside)
    return pl.pallas_call(
        body,
        out_shape=jax.tree.map(lambda leaf: result_space(leaf.shape, leaf.dtype), out_shapes),
        in_specs=[space] * len(args),
        out_specs=jax.tree.map(lambda _: space, out_shapes),
        scratch_shapes=scratch,
        compiler_params=pltpu.CompilerParams(vmem_limit_bytes=16 * 1024 * 1024),
    )(
        *(
            pltpu.with_memory_space_constraint(arg, pltpu.HBM if i < outside else operand_space)
            for i, arg in enumerate(args)
        )
    )


def started(pairs, sems):
    copies = [pltpu.make_async_copy(*pair, sems.at[i]) for i, pair in enumerate(pairs)]
    for copy in copies:
        copy.start()
    return copies


def outgoing_weights(mixers, lats, sp_size):
    count = len(mixers)
    half = mixers[0].shape[0] // 2
    per_mixer = mixers[0].shape[1] // sp_size
    per_lat = [w.shape[1] // sp_size // 2 for w in lats]
    first_lat = count * per_mixer
    padded = first_lat + 128

    def body(*refs):
        out_ref, own_ref, *held_refs, sems = refs[count + 2 :]
        rows = pl.ds(pl.multiple_of(lax.axis_index("grp") * half, half), half)
        held = started([(ref.at[rows], to) for ref, to in zip(refs, held_refs)], sems)
        first = lax.axis_index("tp") == 0
        for copy in held:
            copy.wait()
        for s in range(sp_size):
            for k in range(count):
                out_ref[s, :, k * per_mixer : (k + 1) * per_mixer] = held_refs[k][
                    :, s * per_mixer : (s + 1) * per_mixer
                ]
            pieces = []
            for ref, per in zip(held_refs[count:], per_lat):
                pair = ref[:, 2 * s * per : 2 * (s + 1) * per]
                pieces.append(jnp.where(first, pair[:, :per], pair[:, per:]))
            pieces.append(jnp.zeros((half, 128 - sum(per_lat)), jnp.bfloat16))
            out_ref[s, :, first_lat:] = jnp.concatenate(pieces, axis=1)
        own_ref[...] = out_ref[lax.axis_index("sp")]

    space = pl.BlockSpec(memory_space=pltpu.VMEM)
    return pl.pallas_call(
        body,
        out_shape=(
            pltpu.HBM((sp_size, half, padded), jnp.bfloat16),
            pltpu.HBM((half, padded), jnp.bfloat16),
        ),
        in_specs=[pl.BlockSpec(memory_space=pl.ANY)] * (count + 2),
        out_specs=(space, space),
        scratch_shapes=(
            *(pltpu.VMEM((half, w.shape[1]), jnp.bfloat16) for w in (*mixers, *lats)),
            pltpu.SemaphoreType.DMA((count + 2,)),
        ),
        name="outgoing_weights",
        compiler_params=pltpu.CompilerParams(vmem_limit_bytes=16 * 1024 * 1024),
    )(*(pltpu.with_memory_space_constraint(w, pltpu.HBM) for w in (*mixers, *lats)))


def outgoing_tokens(tokens, gain, sp_size):
    rows, width = tokens.shape
    block = width // (sp_size * 4)

    def body(token_ref, gain_ref, mine_ref, their_ref):
        values = token_ref[...].astype(jnp.float32)
        normed = (values * rms_scale(values) * gain_ref[...]).astype(jnp.bfloat16)
        first = lax.axis_index("tp") == 0
        for f in range(2):
            for s in range(sp_size):
                begin = (s * 2 + f) * 2 * block
                low = normed[:, begin : begin + block]
                high = normed[:, begin + block : begin + 2 * block]
                at = (f * sp_size + s) * block
                mine_ref[:, at : at + block] = jnp.where(first, low, high)
                their_ref[:, at : at + block] = jnp.where(first, high, low)

    shape = jax.ShapeDtypeStruct((rows, width // 2), jnp.bfloat16)
    return kernel_call(body, (shape, shape), (tokens, gain))


def prepare(narrow, query_up, latent_up, sp_size):
    width = narrow[0].shape[1]
    block = width // (sp_size * 4)
    rank, query_width = query_up.shape
    per_query = query_width // sp_size
    heads = per_query // (NOPE + ROPE)
    per_latent = latent_up.shape[1] // sp_size

    def body(rope_ref, beta_ref, decay_ref, query_ref, latent_ref, narrow_ref, q_ref, kv_ref):
        place = lax.axis_index("sp")
        rows = jnp.concatenate([rope_ref[...], beta_ref[...], decay_ref[...]], axis=0)
        for s in range(sp_size):
            for f in range(2):
                for g in range(2):
                    begin = ((s * 2 + f) * 2 + g) * block
                    at = ((g * 2 + f) * sp_size + s) * block
                    narrow_ref[:, at : at + block] = rows[:, begin : begin + block]
        own = query_ref[:, :per_query]
        for s in range(1, sp_size):
            own = jnp.where(place == s, query_ref[:, s * per_query : (s + 1) * per_query], own)
        pairs = [
            (own[:, h * (NOPE + ROPE) :][:, :NOPE], own[:, h * (NOPE + ROPE) :][:, NOPE : NOPE + ROPE])
            for h in range(heads)
        ]
        parts = [plain for plain, _ in pairs] + [turn for _, turn in pairs]
        for _, turn in pairs:
            parts += [turn[:, ROPE // 2 :], turn[:, : ROPE // 2]]
        q_ref[...] = jnp.concatenate(parts, axis=1)
        kv_ref[...] = latent_ref[:, pl.ds(pl.multiple_of(place * per_latent, 128), per_latent)]

    bf16 = jnp.bfloat16
    return kernel_call(
        body,
        (
            jax.ShapeDtypeStruct((sum(n.shape[0] for n in narrow), width), bf16),
            jax.ShapeDtypeStruct((rank, heads * (NOPE + 2 * ROPE)), bf16),
            jax.ShapeDtypeStruct((latent_up.shape[0], per_latent), bf16),
        ),
        (*narrow, query_up, latent_up),
        inside=(False, True),
    )


def project(mine, theirs, block, peers, extra, sizes):
    seq_count, token_count, fine, q_cols, kv_cols = sizes
    sp_size = len(mine)
    chunk, part = mine[0].shape
    span = sp_size * token_count
    rows = seq_count * span
    piece, columns = peers[0].shape
    extra_width = extra.shape[0]
    q_stack, kv_stack = 128 // q_cols, 128 // kv_cols
    packed = rows // q_stack + rows // kv_stack
    copies = 1 + 3 * (sp_size + 1) + 2 * sp_size

    def body(*refs):
        mine_refs, refs = refs[:sp_size], refs[sp_size:]
        their_refs, refs = refs[:sp_size], refs[sp_size:]
        block_ref, refs = refs[0], refs[1:]
        peer_refs, refs = refs[:9], refs[9:]
        extra_ref, fine_ref, pack_ref, ext_ref, lat_ref, weight_ref, token_ref, sems = refs
        place, fs_at = lax.axis_index("sp"), lax.axis_index("fs")
        tp_at, grp_at = lax.axis_index("tp"), lax.axis_index("grp")
        step = piece // 2

        def rows_at(same_grp, same_fs, source, first, number):
            grp_from = grp_at if same_grp else 1 - grp_at
            block_from = (grp_from * 2 + (fs_at if same_fs else 1 - fs_at)) * sp_size + source
            return weight_ref.at[pl.ds(pl.multiple_of(block_from * piece + first, step), number)]

        moves = [(block_ref, rows_at(True, True, 0, 0, sp_size * piece))]
        half_rows = (sp_size - 1) * step
        for k, flips in enumerate(((True, False), (False, True), (False, False))):
            own_ref, low_ref, high_ref = peer_refs[3 * k : 3 * k + 3]
            moves.append((own_ref, rows_at(*flips, place, 0, piece)))
            for o in range(1, sp_size):
                source = lax.rem(place + o, sp_size)
                begin, end = (o - 1) * piece, o * piece
                cut = min(max(begin, half_rows), end)
                if cut > begin:
                    from_ref = low_ref.at[begin:cut]
                    moves.append((from_ref, rows_at(*flips, source, 0, cut - begin)))
                if end > cut:
                    from_ref = high_ref.at[cut - half_rows : end - half_rows]
                    moves.append((from_ref, rows_at(*flips, source, cut - begin, end - cut)))
        for o in range(sp_size):
            of = pl.ds(o * chunk, chunk)
            at = pl.ds(pl.multiple_of(tp_at * part, part), part)
            moves.append((mine_refs[o], token_ref.at[of, at]))
            at = pl.ds(pl.multiple_of((1 - tp_at) * part, part), part)
            moves.append((their_refs[o], token_ref.at[of, at]))
        assert len(moves) <= copies
        moves = started(moves, sems)
        for copy in moves[: -2 * sp_size]:
            copy.wait()
        for o in range(sp_size):
            for copy in moves[len(moves) - 2 * (sp_size - o) :][:2]:
                copy.wait()
            lhs = token_ref[o * chunk : (o + 1) * chunk, :]
            value = dot32(lhs, weight_ref[...]).astype(jnp.bfloat16)
            outer = dot_t(lhs, extra_ref[...])
            source = lax.bitwise_xor(place, o)
            for n in range(seq_count):
                of = slice(n * token_count, (n + 1) * token_count)
                at = pl.ds(pl.multiple_of(source * token_count, token_count), token_count)
                fine_ref[n, at, :] = value[of, :fine]
                ext_ref[n, at, :] = outer[of]
                at = pl.ds(
                    pl.multiple_of(n * span + source * token_count, token_count), token_count
                )
                lat_ref[at, :] = value[of, fine : fine + 128]
        for start, first, width, count in (
            (0, 0, q_cols, q_stack),
            (rows // q_stack, q_cols, kv_cols, kv_stack),
        ):
            group = rows // count
            joined = jnp.concatenate(
                [
                    lat_ref[k * group : (k + 1) * group, first : first + width]
                    for k in range(count)
                ],
                axis=1,
            )
            for j in range(sp_size):
                pack_ref[j, start : start + group, :] = joined

    space = pl.BlockSpec(memory_space=pltpu.VMEM)
    moved = tuple(
        pltpu.with_memory_space_constraint(array, pltpu.HBM)
        for array in (*mine, *theirs, block, *peers)
    )
    return pl.pallas_call(
        body,
        out_shape=(
            pltpu.VMEM((seq_count, span, fine), jnp.bfloat16),
            pltpu.VMEM((sp_size, packed, 128), jnp.bfloat16),
            pltpu.VMEM((seq_count, span, extra_width), jnp.float32),
        ),
        in_specs=[pl.BlockSpec(memory_space=pl.ANY)] * len(moved) + [space],
        out_specs=(space,) * 3,
        scratch_shapes=(
            pltpu.VMEM((rows, 128), jnp.bfloat16),
            pltpu.VMEM((2 * part, columns), jnp.bfloat16),
            pltpu.VMEM((rows, 2 * part), jnp.bfloat16),
            pltpu.SemaphoreType.DMA((copies,)),
        ),
        name="project",
        compiler_params=pltpu.CompilerParams(vmem_limit_bytes=16 * 1024 * 1024),
    )(*moved, pltpu.with_memory_space_constraint(extra, pltpu.VMEM))


def send_by_pair(out_refs, pieces, sp_size):
    place = lax.axis_index("sp")
    for step, out_ref in enumerate(out_refs):
        second = lax.rem(place + step, sp_size) >= sp_size // 2
        for n, (low, high) in enumerate(pieces):
            rows = low.shape[0]
            out_ref[n * rows : (n + 1) * rows, :] = jnp.where(second, high, low)


def lower_inverses(lowers, base):
    size = lowers[0].shape[0]
    row = lax.broadcasted_iota(jnp.int32, (size, size), 0)
    col = lax.broadcasted_iota(jnp.int32, (size, size), 1)
    unit = jnp.where(row == col, 1.0, 0.0)
    powers = [jnp.where(row // base == col // base, low, 0.0) for low in lowers]
    inverses = [unit - p for p in powers]
    reach = 2
    while reach < base:
        powers = [fine_dot(p, p) for p in powers]
        inverses = [i + fine_dot(i, p) for i, p in zip(inverses, powers)]
        reach *= 2
    block = base
    while block < size:
        joint = (row // (2 * block) == col // (2 * block)) & (row // block != col // block)
        moved = [fine_dot(i, jnp.where(joint, low, 0.0)) for i, low in zip(inverses, lowers)]
        inverses = [i - fine_dot(m, i) for i, m in zip(inverses, moved)]
        block *= 2
    return inverses


def delta_mix(fine, ext, gains, gain_at, gates, gate_at, heads, sp_size):
    seq_count, span, _ = fine.shape
    tile = math.gcd(span, 128)
    tiles = span // tile

    def terms(raw_query, raw_key, raw_value, beta_pre, decay_pre, rate):
        query = unit_rows(jax.nn.silu(raw_query)) * HEAD ** (-0.5)
        key = unit_rows(jax.nn.silu(raw_key))
        value = jax.nn.silu(raw_value)
        beta = jax.nn.sigmoid(beta_pre)
        log_decay = -rate * jax.nn.softplus(decay_pre)
        row = lax.broadcasted_iota(jnp.int32, (span, span), 0)
        col = lax.broadcasted_iota(jnp.int32, (span, span), 1)
        as_row = jnp.sum(jnp.where(row == col, log_decay, 0.0), axis=0, keepdims=True)
        gate = jnp.sum(jnp.where(row >= col, as_row, 0.0), axis=1, keepdims=True)
        gate_row = jnp.sum(jnp.where(row == col, gate, 0.0), axis=0, keepdims=True)
        decay = jnp.where(row >= col, jnp.exp(jnp.where(row >= col, gate - gate_row, 0.0)), 0.0)
        lower = fine_dot(key * beta, key, dot_t) * jnp.where(row > col, decay, 0.0)
        scores = fine_dot(query, key, dot_t) * decay
        return lower, scores, value * beta

    def body(fine_ref, ext_ref, gain_ref, *out_refs):
        gain_row = gain_ref[:, gain_at : gain_at + HEAD]
        rate_row = gain_ref[:, gain_at + HEAD : gain_at + 2 * HEAD]
        first_head = (lax.axis_index("tp") * sp_size + lax.axis_index("sp")) * heads
        lane = lax.broadcasted_iota(jnp.int32, (span, ext.shape[2]), 1)
        rate_lane = lax.broadcasted_iota(jnp.int32, (1, HEAD), 1)
        chains = []
        for n in range(seq_count):
            for h in range(heads):
                raw = [
                    fine_ref[n, :, (k * heads + h) * HEAD : (k * heads + h + 1) * HEAD].astype(
                        jnp.float32
                    )
                    for k in range(3)
                ]
                head = first_head + h
                outer = ext_ref[n]
                beta_pre, decay_pre = (
                    jnp.sum(
                        jnp.where(lane == gate_at + k * gates + head, outer, 0.0),
                        axis=1,
                        keepdims=True,
                    )
                    for k in range(2)
                )
                rate = jnp.sum(
                    jnp.where(rate_lane == head, rate_row, 0.0), axis=1, keepdims=True
                )
                chains.append(terms(*raw, beta_pre, decay_pre, rate))
        cuts = [slice(j * tile, (j + 1) * tile) for j in range(tiles)]
        inverses = lower_inverses([c[0][cut, cut] for c in chains for cut in cuts], 8)
        solved = [[] for _ in chains]
        for j, cut in enumerate(cuts):
            for i, (lower, _, wanted) in enumerate(chains):
                rest = wanted[cut]
                if j:
                    rest = rest - fine_dot(
                        lower[cut, : j * tile], jnp.concatenate(solved[i], axis=0)
                    )
                solved[i].append(fine_dot(inverses[i * tiles + j], rest))
        pieces = []
        for i, (_, scores, _) in enumerate(chains):
            out = fine_dot(scores, jnp.concatenate(solved[i], axis=0))
            out = (out * rms_scale(out) * gain_row).astype(jnp.bfloat16)
            pieces.append((out[: span // 2], out[span // 2 :]))
        for h in range(heads):
            columns = slice(h * HEAD, (h + 1) * HEAD)
            views = [ref.at[:, columns] for ref in out_refs] if heads > 1 else out_refs
            send_by_pair(views, pieces[h::heads], sp_size)

    shape = jax.ShapeDtypeStruct((seq_count * span // 2, heads * HEAD), jnp.bfloat16)
    return kernel_call(body, (shape,) * sp_size, (fine, ext, gains), inside=(True, False))


def latent_mix(mine, theirs, ext, tables, gains, ups, q_cols, kv_cols, heads):
    sp_size = mine.shape[0]
    seq_count, span, _ = ext.shape
    rows = seq_count * span
    q_rank, kv_rank = ups[0].shape[0], ups[1].shape[0]
    scale = (NOPE + ROPE) ** (-0.5)

    def unpack(value, n, base, width):
        group = rows * width // 128
        pieces = []
        for k in range(128 // width):
            if n * span < (k + 1) * group and k * group < (n + 1) * span:
                low = max(n * span - k * group, 0)
                high = min((n + 1) * span - k * group, group)
                pieces.append(
                    value[base + low : base + high, k * width : (k + 1) * width]
                )
        return jnp.concatenate(pieces, axis=0) if len(pieces) > 1 else pieces[0]

    def body(mine_ref, their_ref, ext_ref, cos_ref, sin_ref, *refs):
        gain_ref, qup_ref, kup_ref, *out_refs = refs
        q_gain = gain_ref[:, :q_rank]
        kv_gain = gain_ref[:, q_rank : q_rank + kv_rank]
        first = lax.axis_index("tp") == 0
        row = lax.broadcasted_iota(jnp.int32, (span, span), 0) // BLOCK
        col = lax.broadcasted_iota(jnp.int32, (span, span), 1) // BLOCK
        allowed = col <= row
        cosine, sine = cos_ref[...], sin_ref[...]
        pairs = []
        for s in range(sp_size):
            own, other = mine_ref[s], their_ref[s]
            pairs += [jnp.where(first, own, other), jnp.where(first, other, own)]
        joins, held = [], []
        for n in range(seq_count):
            q_parts = [unpack(p, n, 0, q_cols) for p in pairs]
            kv_parts = [unpack(p, n, rows * q_cols // 128, kv_cols) for p in pairs]
            q_lat = jnp.concatenate(q_parts, axis=1).astype(jnp.float32)
            kv_lat = jnp.concatenate(kv_parts, axis=1).astype(jnp.float32)
            q_norm = (q_lat * rms_scale(q_lat) * q_gain).astype(jnp.bfloat16)
            kv_norm = (kv_lat * rms_scale(kv_lat) * kv_gain).astype(jnp.bfloat16)
            q_all = dot32(q_norm, qup_ref[...]).astype(jnp.bfloat16)
            kv_all = dot32(kv_norm, kup_ref[...]).astype(jnp.bfloat16)
            plain_width, turn_width = heads * NOPE, heads * ROPE
            plain = q_all[:, :plain_width]
            turn = q_all[:, plain_width : plain_width + turn_width].astype(jnp.float32)
            swapped = q_all[:, plain_width + turn_width :].astype(jnp.float32)
            turned = (turn * cosine + swapped * sine).astype(jnp.bfloat16)
            raw = ext_ref[n, :, :ROPE].astype(jnp.bfloat16).astype(jnp.float32)
            back = jnp.concatenate([raw[:, ROPE // 2 :], raw[:, : ROPE // 2]], axis=1)
            key_turn = (raw * cosine[:, :ROPE] + back * sine[:, :ROPE]).astype(jnp.bfloat16)
            for h in range(heads):
                key_plain = kv_all[:, h * (NOPE + VDIM) : h * (NOPE + VDIM) + NOPE]
                values = kv_all[:, h * (NOPE + VDIM) + NOPE : (h + 1) * (NOPE + VDIM)]
                logits = (
                    dot_t(plain[:, h * NOPE : (h + 1) * NOPE], key_plain)
                    + dot_t(turned[:, h * ROPE : (h + 1) * ROPE], key_turn)
                ) * scale
                held.append((jnp.where(allowed, logits, -jnp.inf), values))
        peaks = [jnp.max(logits, axis=-1, keepdims=True) for logits, _ in held]
        weights = [jnp.exp(logits - peak) for (logits, _), peak in zip(held, peaks)]
        totals = [jnp.sum(w, axis=-1, keepdims=True) for w in weights]
        mixed = [dot32(w.astype(jnp.bfloat16), v) for w, (_, v) in zip(weights, held)]
        results = [m / t for m, t in zip(mixed, totals)]
        for n in range(seq_count):
            joined = jnp.concatenate(results[n * heads : (n + 1) * heads], axis=1).astype(
                jnp.bfloat16
            )
            joins.append((joined[: span // 2], joined[span // 2 :]))
        send_by_pair(out_refs, joins, sp_size)

    shape = jax.ShapeDtypeStruct((rows // 2, heads * VDIM), jnp.bfloat16)
    return kernel_call(
        body, (shape,) * sp_size, (mine, theirs, ext, *tables, gains, *ups), outside=1
    )


def output_partial(delta_all, latent_all, near, near_fs, far, gain, sizes):
    seq_count, token_count = sizes
    sp_size = len(delta_all)
    rows, d_width = delta_all[0].shape
    l_width = latent_all[0].shape[1]
    total, columns = near.shape
    half = total // 2
    per_half = sp_size // 2

    def body(*refs):
        d_refs, refs = refs[:sp_size], refs[sp_size:]
        l_refs, refs = refs[:sp_size], refs[sp_size:]
        near_ref, near_fs_ref, *far_refs, gain_ref, keep_ref, pass_ref, kept_ref, lhs_ref = refs
        kept_ref[...] = gain_ref[...]
        place, fs_at = lax.axis_index("sp"), lax.axis_index("fs")
        grp_at = lax.axis_index("grp")
        for o in range(sp_size):
            source = lax.rem(place + o, sp_size)
            base = (source // per_half) * half
            within = lax.rem(source, per_half)
            at = pl.multiple_of(base + within * d_width, 128)
            lhs_ref[:, pl.ds(at, d_width)] = d_refs[o][...]
            at = pl.multiple_of(base + per_half * d_width + within * l_width, 128)
            lhs_ref[:, pl.ds(at, l_width)] = l_refs[o][...]
        lhs = lhs_ref[...]
        own = lhs_ref[:, pl.ds(pl.multiple_of(grp_at * half, half), half)]
        other = lhs_ref[:, pl.ds(pl.multiple_of((1 - grp_at) * half, half), half)]
        close = (
            dot32(lhs, near_ref[...]).astype(jnp.bfloat16),
            dot32(lhs, near_fs_ref[...]).astype(jnp.bfloat16),
        )
        away = tuple(
            (dot32(own, far_refs[k][...]) + dot32(other, far_refs[k + 1][...])).astype(jnp.bfloat16)
            for k in (0, 2)
        )
        straight = place // per_half == lax.axis_index("tp")
        for k in range(2):
            begin = (1 - fs_at) if k else fs_at
            at = pl.ds(pl.multiple_of(begin * columns, columns), columns)
            keep = jnp.where(straight, close[k], away[k])
            onward = jnp.where(straight, away[k], close[k])
            pair_rows = 2 * token_count
            for n in range(seq_count):
                for p in range(2):
                    of = slice(n * pair_rows + p * token_count, n * pair_rows + (p + 1) * token_count)
                    to = slice(n * token_count, (n + 1) * token_count)
                    keep_ref[p, to, at] = keep[of]
                    pass_ref[p, to, at] = onward[of]

    shape = jax.ShapeDtypeStruct((2, rows // 2, 2 * columns), jnp.bfloat16)
    return kernel_call(
        body,
        (shape, shape, jax.ShapeDtypeStruct(gain.shape, gain.dtype)),
        (*delta_all, *latent_all, near, near_fs, *far, gain),
        scratch=(pltpu.VMEM((rows, total), jnp.bfloat16),),
    )


def whole_tables(length, repeats):
    frequency = ROPE_THETA ** (-np.arange(0, ROPE, 2, dtype=np.float32) / np.float32(ROPE))
    angles = np.arange(length, dtype=np.float32)[:, None] * frequency[None, :].astype(np.float32)
    cosine, sine = np.cos(angles), np.sin(angles)
    return tuple(
        jnp.asarray(np.tile(np.concatenate(pair, axis=1), (1, repeats)), jnp.float32)
        for pair in ((cosine, cosine), (-sine, sine))
    )


def whole_sequences(
    tokens,
    pre_gain,
    query_weight,
    key_weight,
    value_weight,
    beta_weight,
    decay_weight,
    decay_rate,
    delta_gain,
    query_down,
    latent_down,
    rope_weight,
    query_gain,
    latent_gain,
    query_up,
    latent_up,
    delta_out,
    latent_out,
    post_gain,
):
    f32, bf16 = jnp.float32, jnp.bfloat16
    sp_size, tp_size = lax.axis_size("sp"), lax.axis_size("tp")
    place, grp_at = lax.axis_index("sp"), lax.axis_index("grp")
    seq_count, token_count, width = tokens.shape
    rows = seq_count * token_count
    heads = query_weight.shape[1] // HEAD // sp_size
    shares = sp_size * tp_size
    q_cols, kv_cols = query_down.shape[1] // shares, latent_down.shape[1] // shares

    def exchange(values, axis):
        return lax.all_to_all(values, axis, 0, 0, tiled=True)

    def swap(values, axis):
        return lax.ppermute(values, axis, [(0, 1), (1, 0)])

    def along(values, step):
        return lax.ppermute(values, "sp", [(i, (i + step) % sp_size) for i in range(sp_size)])

    def from_sp(sends):
        return [sends[0]] + [along(sends[step], step) for step in range(sp_size - 1, 0, -1)]

    outgoing, own_piece = outgoing_weights(
        (query_weight, key_weight, value_weight), (query_down, latent_down), sp_size
    )
    block = exchange(outgoing, "sp")
    token_rows, outgoing = lax.optimization_barrier((tokens.reshape(rows, width), outgoing))

    own_half, other_half = outgoing_tokens(token_rows, pre_gain[None, :], sp_size)

    def beside(values):
        return lax.ppermute(values, "sp", [(i, i ^ 1) for i in range(sp_size)])

    far_half = along(own_half, sp_size // 2)
    mine = [own_half, beside(own_half), far_half, beside(far_half)]
    theirs = [other_half] + [swap(piece, "tp") for piece in mine[1:]]

    quarter = delta_out.shape[0] // 2
    near = jnp.concatenate(
        [w[k * quarter : (k + 1) * quarter] for k in range(2) for w in (delta_out, latent_out)]
    )
    near_fs = swap(near, "fs")

    own_grp, own_fs = swap(own_piece, "grp"), swap(own_piece, "fs")
    own_corner = swap(own_grp, "fs")
    rest = lax.dynamic_slice_in_dim(jnp.concatenate([block, block]), place + 1, sp_size - 1, 0)
    rest = rest.reshape(-1, rest.shape[2])
    block = block.reshape(-1, block.shape[2])
    middle = rest.shape[0] // 2
    low, high = rest[:middle], rest[middle:]
    low_grp, high_fs = swap(low, "grp"), swap(high, "fs")
    high_grp, low_fs = swap(high, "grp"), swap(low, "fs")
    corner = swap(low_grp, "fs"), swap(high_fs, "grp")
    peers = (own_fs, low_fs, high_fs, own_grp, low_grp, high_grp, own_corner, *corner)

    far_own = lax.dynamic_slice_in_dim(near, grp_at * 2 * quarter, 2 * quarter, 0)
    far_own = along(far_own, sp_size // 2)
    far_other = swap(far_own, "grp")
    far = (far_own, far_other, swap(far_own, "fs"))
    far = (*far, swap(far_other, "fs"))

    gate_at = rope_weight.shape[1]
    latent_heads = query_up.shape[1] // (NOPE + ROPE) // sp_size
    extra, q_up, kv_up = prepare(
        (rope_weight.T, beta_weight.T, decay_weight.T), query_up, latent_up, sp_size
    )
    tables = whole_tables(sp_size * token_count, latent_heads)
    rates = jnp.pad(decay_rate, (0, HEAD - decay_rate.shape[0]))
    latent_gains = jnp.concatenate([query_gain, latent_gain])[None, :]
    gains = jnp.concatenate([delta_gain, rates])[None, :]
    mine[1], gains, latent_gains = lax.optimization_barrier((mine[1], gains, latent_gains))

    fine, lat, ext = project(
        mine,
        theirs,
        block,
        peers,
        extra,
        (seq_count, token_count, 3 * heads * HEAD, q_cols, kv_cols),
    )
    lat_mine = exchange(lat, "sp")
    delta_sends = delta_mix(
        fine, ext, gains, 0, decay_rate.shape[0], gate_at, heads, sp_size
    )
    lat_mine, _ = lax.optimization_barrier((lat_mine, delta_sends))
    lat_theirs = swap(lat_mine, "tp")
    delta_all = from_sp(delta_sends)
    latent_sends = latent_mix(
        lat_mine,
        lat_theirs,
        ext,
        tables,
        latent_gains,
        (q_up, kv_up),
        q_cols,
        kv_cols,
        latent_heads,
    )
    latent_all = from_sp(latent_sends)

    keep, onward, post_row = output_partial(
        delta_all, latent_all, near, near_fs, far, post_gain[None, :], (seq_count, token_count)
    )
    mixed = (keep.astype(f32) + swap(onward, "tp").astype(f32)).astype(bf16)
    side = lax.rem(place, 2)

    def across(values):
        return lax.ppermute(pick(values, 1 - side), "sp", [(i, i ^ 1) for i in range(sp_size)])

    there = across(mixed)
    squares = jnp.sum(mixed.astype(f32) * mixed.astype(f32), axis=2)
    squares = squares + swap(squares, "tp")
    squares = (pick(squares, side) + across(squares))[:, None]
    here, there = pick(mixed, side).astype(f32), there.astype(f32)
    final = jnp.concatenate(
        [jnp.where(side == 0, here, there), jnp.where(side == 0, there, here)], axis=1
    )
    result = final * lax.rsqrt(squares / D + NORM_EPS) * post_row
    return result.astype(bf16).reshape(seq_count, token_count, final.shape[1])


def fits_whole(mesh):
    shape = mesh.shape
    return all(shape[name] == 2 for name in ("grp", "fs", "tp")) and shape["sp"] == 4


def solution(mesh):
    def chosen(*args):
        head_count = args[2].shape[1] // HEAD
        latent_count = args[14].shape[1] // (NOPE + ROPE)
        sp_size = mesh.shape["sp"]
        whole = fits_whole(mesh) and head_count % sp_size == 0 and latent_count % sp_size == 0
        return (whole_sequences if whole else local)(*args)

    return jax.shard_map(
        chosen,
        mesh=mesh,
        in_specs=(
            P(("grp", "fs"), "sp", None),
            P(),
            P(("sp", "fs"), "tp"),
            P(("sp", "fs"), "tp"),
            P(("sp", "fs"), "tp"),
            P(),
            P(),
            P(),
            P(),
            P(("sp", "fs"), None),
            P(("sp", "fs"), None),
            P(),
            P(),
            P(),
            P(None, "tp"),
            P(None, "tp"),
            P("tp", ("sp", "fs")),
            P("tp", ("sp", "fs")),
            P("tp"),
        ),
        out_specs=P(("grp", "fs"), "sp", "tp"),
        check_vma=False,
    )
```

```python
import math

import jax
import jax.numpy as jnp
import numpy as np
from jax import lax
from jax.experimental import pallas as pl
from jax.experimental.pallas import tpu as pltpu
from jax.sharding import PartitionSpec as P


D = 2048
HEAD = 128
NOPE = 64
ROPE = 32
VDIM = 64
BLOCK = 64


NORM_EPS = 1e-06
ROPE_THETA = 10000.0
HIGHEST = lax.Precision.HIGHEST


def prefix(array, axis, join, neutral):
    place = lax.axis_index(axis)
    gathered = jax.tree.map(
        lambda a, kind: lax.all_gather(a.astype(kind), axis), array, (jnp.bfloat16, jnp.bfloat16)
    )
    state = jax.tree.map(lambda a, e: jnp.zeros_like(a) + jnp.asarray(e, a.dtype), array, neutral)

    def one(step, state):
        return join(
            state,
            jax.tree.map(
                lambda a, own: lax.dynamic_index_in_dim(a, step, 0, False).astype(own.dtype),
                gathered,
                array,
            ),
        )

    return lax.fori_loop(0, place, one, state)


def stored(values):
    return lax.optimization_barrier(values.astype(jnp.bfloat16))


def rms_scale(values):
    return lax.rsqrt(jnp.mean(values * values, axis=-1, keepdims=True) + NORM_EPS)


def unit_rows(values):
    return values * lax.rsqrt(jnp.sum(values * values, axis=-1, keepdims=True) + NORM_EPS)


def rope_tables(positions, rope_width):
    frequency = ROPE_THETA ** (-jnp.arange(0, rope_width, 2, dtype=jnp.float32) / rope_width)
    angles = positions.astype(jnp.float32)[:, None] * frequency[None, :]
    return (jnp.cos(angles), jnp.sin(angles))


def rotate(values, cosine_table, sine_table):
    lower_half, upper_half = jnp.split(values, 2, axis=-1)
    return jnp.concatenate(
        [
            lower_half * cosine_table - upper_half * sine_table,
            upper_half * cosine_table + lower_half * sine_table,
        ],
        axis=-1,
    )


def delta_terms(query_vectors, key_vectors, value_vectors, beta_gate, log_decay):
    length, head_count, _ = query_vectors.shape
    nblocks = length // BLOCK

    def split_blocks(tensor):
        return jnp.moveaxis(tensor.reshape((nblocks, BLOCK, head_count) + tensor.shape[2:]), 2, 0)

    query_vectors = split_blocks(query_vectors)
    key_vectors = split_blocks(key_vectors)
    value_vectors = split_blocks(value_vectors)
    beta_gate = split_blocks(beta_gate)
    gate_sum = jnp.cumsum(split_blocks(log_decay), axis=-1)
    position = jnp.arange(BLOCK)
    strict = position[:, None] > position[None, :]
    causal = position[:, None] >= position[None, :]
    gate_gap = gate_sum[..., :, None] - gate_sum[..., None, :]
    strict_decay = jnp.where(strict, jnp.exp(jnp.where(strict, gate_gap, 0.0)), 0.0)
    causal_decay = jnp.where(causal, jnp.exp(jnp.where(causal, gate_gap, 0.0)), 0.0)
    keys_scaled = key_vectors * beta_gate[..., None]
    lower_mat = (
        jnp.einsum("hnid,hnjd->hnij", keys_scaled, key_vectors, precision=HIGHEST) * strict_decay
    )
    identity = jnp.eye(BLOCK, dtype=jnp.float32)
    inverse = jax.scipy.linalg.solve_triangular(
        identity + lower_mat, jnp.broadcast_to(identity, lower_mat.shape), lower=True
    )
    new_values = jnp.einsum(
        "hnij,hnjd->hnid", inverse, value_vectors * beta_gate[..., None], precision=HIGHEST
    )
    key_weights = jnp.einsum(
        "hnij,hnjd->hnid", inverse, keys_scaled * jnp.exp(gate_sum)[..., None], precision=HIGHEST
    )
    scores = (
        jnp.einsum("hnid,hnjd->hnij", query_vectors, key_vectors, precision=HIGHEST) * causal_decay
    )
    last_gate = gate_sum[..., -1]
    query_decay = query_vectors * jnp.exp(gate_sum)[..., None]
    key_decay = key_vectors * jnp.exp(last_gate[..., None] - gate_sum)[..., None]
    return (query_decay, key_decay, new_values, key_weights, scores, last_gate)


def compose(earlier, following):
    return (
        jnp.einsum("hij,hjk->hik", following[0], earlier[0], precision=HIGHEST),
        jnp.einsum("hij,hjk->hik", following[0], earlier[1], precision=HIGHEST) + following[1],
    )


def keep_same(current):
    return current


def local(
    tokens,
    pre_gain,
    query_weight,
    key_weight,
    value_weight,
    beta_weight,
    decay_weight,
    decay_rate,
    delta_gain,
    query_down,
    latent_down,
    rope_weight,
    query_gain,
    latent_gain,
    query_up,
    latent_up,
    delta_out,
    latent_out,
    post_gain,
):
    f32 = jnp.float32
    seq_count, token_count = (tokens.shape[0], tokens.shape[1])
    row_total = seq_count * token_count
    sequence = tokens.reshape(row_total, tokens.shape[2]).astype(f32)
    query_start = lax.axis_index("sp") * token_count
    positions = query_start + jnp.arange(token_count)
    normed = (sequence * rms_scale(sequence) * pre_gain).astype(jnp.bfloat16)
    head_group = lax.axis_index("tp")
    q_width = query_down.shape[1] // lax.axis_size("tp")
    kv_width = latent_down.shape[1] // lax.axis_size("tp")
    q_own = lax.dynamic_slice_in_dim(query_down, head_group * q_width, q_width, 1)
    kv_own = lax.dynamic_slice_in_dim(latent_down, head_group * kv_width, kv_width, 1)
    portion = (
        lax.all_gather(query_weight, ("sp", "fs"), axis=0, tiled=True),
        lax.all_gather(key_weight, ("sp", "fs"), axis=0, tiled=True),
        lax.all_gather(value_weight, ("sp", "fs"), axis=0, tiled=True),
        lax.all_gather(q_own, ("sp", "fs"), axis=0, tiled=True),
        lax.all_gather(kv_own, ("sp", "fs"), axis=0, tiled=True),
    )
    row_count = portion[0].shape[0]
    projected = tuple((jnp.dot(normed, weight, preferred_element_type=f32) for weight in portion))
    raw_query, raw_key, raw_value, q_half, kv_half = tuple((stored(member) for member in projected))
    q_latent, kv_latent = (
        lax.all_gather(q_half, "tp", axis=1, tiled=True),
        lax.all_gather(kv_half, "tp", axis=1, tiled=True),
    )
    head_count = query_weight.shape[1] // HEAD
    lane_count = seq_count * head_count
    beta_full = jax.nn.sigmoid(jnp.dot(normed, beta_weight, preferred_element_type=f32))
    beta_gate = lax.dynamic_slice_in_dim(beta_full, head_group * head_count, head_count, 1)
    decay_full = jnp.dot(normed, decay_weight, preferred_element_type=f32)
    decay_pre = lax.dynamic_slice_in_dim(decay_full, head_group * head_count, head_count, 1)
    decay_local = lax.dynamic_slice_in_dim(decay_rate, head_group * head_count, head_count, 0)
    log_decay = -decay_local[None, :] * jax.nn.softplus(decay_pre)

    def by_position(values):
        shaped = values.reshape((seq_count, token_count) + values.shape[1:])
        shaped = jnp.moveaxis(shaped, 0, 1)
        return shaped.reshape((token_count, seq_count * values.shape[1]) + values.shape[2:])

    query_vectors = by_position(
        unit_rows(jax.nn.silu(raw_query.astype(f32)).reshape(row_total, head_count, HEAD))
        * HEAD ** (-0.5)
    )
    key_vectors = by_position(
        unit_rows(jax.nn.silu(raw_key.astype(f32)).reshape(row_total, head_count, HEAD))
    )
    value_vectors = by_position(
        jax.nn.silu(raw_value.astype(f32)).reshape(row_total, head_count, HEAD)
    )
    block_terms = delta_terms(
        query_vectors, key_vectors, value_vectors, by_position(beta_gate), by_position(log_decay)
    )
    inputs = tuple((jnp.moveaxis(tensor, 1, 0) for tensor in block_terms))

    def advance(totals, block_in):
        carried, transfer = totals
        query_decay, key_decay, new_values, key_weights, scores, last_gate = block_in
        corrected = new_values - jnp.einsum("hcd,hde->hce", key_weights, carried, precision=HIGHEST)
        output = jnp.einsum("hcd,hde->hce", query_decay, carried, precision=HIGHEST) + jnp.einsum(
            "hij,hje->hie", scores, corrected, precision=HIGHEST
        )
        reader_rows = query_decay - jnp.einsum(
            "hij,hjd->hid", scores, key_weights, precision=HIGHEST
        )
        reader = jnp.einsum("hcd,hde->hce", reader_rows, transfer, precision=HIGHEST)
        factor = jnp.exp(last_gate)[:, None, None]
        carried = carried * factor + jnp.einsum(
            "hcd,hce->hde", key_decay, corrected, precision=HIGHEST
        )
        moved = jnp.einsum("hcd,hde->hce", key_weights, transfer, precision=HIGHEST)
        transfer = transfer * factor - jnp.einsum(
            "hcd,hce->hde", key_decay, moved, precision=HIGHEST
        )
        return ((carried, transfer), (output, reader))

    eye_stack = jnp.broadcast_to(jnp.eye(HEAD, dtype=f32), (lane_count, HEAD, HEAD))
    zero_state = jnp.zeros((lane_count, HEAD, HEAD), f32)
    (state_end, transfer_end), (outputs, readers) = lax.scan(
        advance, (zero_state, eye_stack), inputs
    )
    _, incoming = prefix((transfer_end, state_end), "sp", compose, (eye_stack, zero_state))
    outputs = outputs + jnp.einsum("nhcd,hde->nhce", readers, incoming, precision=HIGHEST)
    delta_raw = jnp.transpose(outputs, (0, 2, 1, 3)).reshape(
        token_count, seq_count, head_count, HEAD
    )
    delta_raw = jnp.moveaxis(delta_raw, 1, 0).reshape(row_total, head_count, HEAD)
    delta_heads = (
        (delta_raw * rms_scale(delta_raw) * delta_gain)
        .astype(jnp.bfloat16)
        .reshape(row_total, head_count * HEAD)
    )
    q_lat32 = q_latent.astype(f32)
    kv_lat32 = kv_latent.astype(f32)
    q_normed = (q_lat32 * rms_scale(q_lat32) * query_gain).astype(jnp.bfloat16)
    kv_normed = (kv_lat32 * rms_scale(kv_lat32) * latent_gain).astype(jnp.bfloat16)
    rope_raw = stored(jnp.dot(normed, rope_weight, preferred_element_type=f32))
    cosine_table, sine_table = rope_tables(positions, rope_raw.shape[1])
    rope_keys = rotate(
        rope_raw.astype(f32).reshape(seq_count, token_count, rope_raw.shape[1]),
        cosine_table,
        sine_table,
    ).astype(jnp.bfloat16)
    latent_count = query_up.shape[1] // (NOPE + ROPE)
    query_all = stored(jnp.dot(q_normed, query_up, preferred_element_type=f32)).reshape(
        seq_count, token_count, latent_count, NOPE + ROPE
    )
    query_plain = query_all[..., :NOPE]
    query_turned = rotate(
        query_all[..., NOPE:].astype(f32), cosine_table[:, None, :], sine_table[:, None, :]
    ).astype(jnp.bfloat16)
    score_scale = (NOPE + ROPE) ** (-0.5)
    query_block = positions // BLOCK
    kv_seq = kv_normed.reshape(seq_count, token_count, kv_normed.shape[1])

    def attend_block(totals, key_plain, value_rows, rope_rows, key_start):
        row_max, row_sum, weighted = totals
        key_block = (key_start + jnp.arange(key_plain.shape[1])) // BLOCK
        allowed = key_block[None, :] <= query_block[:, None]
        logits = (
            jnp.einsum("sqhd,skhd->shqk", query_plain, key_plain, preferred_element_type=f32)
            + jnp.einsum("sqhd,skd->shqk", query_turned, rope_rows, preferred_element_type=f32)
        ) * score_scale
        logits = jnp.where(allowed[None, None], logits, -jnp.inf)
        new_max = jnp.maximum(row_max, jnp.max(logits, axis=-1))
        shift = jnp.where(jnp.isfinite(new_max), new_max, 0.0)
        weights = jnp.where(allowed[None, None], jnp.exp(logits - shift[..., None]), 0.0)
        rescale = jnp.exp(row_max - shift)
        row_sum = row_sum * rescale + jnp.sum(weights, axis=-1)
        weighted = weighted * rescale[..., None] + jnp.einsum(
            "shqk,skhd->shqd", weights.astype(jnp.bfloat16), value_rows, preferred_element_type=f32
        )
        return (new_max, row_sum, weighted)

    start_stats = (
        jnp.full((seq_count, latent_count, token_count), -jnp.inf, f32),
        jnp.zeros((seq_count, latent_count, token_count), f32),
        jnp.zeros((seq_count, latent_count, token_count, VDIM), f32),
    )

    def expand_latent(portion, row_start, span_rows):
        latent_rows = lax.dynamic_slice_in_dim(portion[0], row_start, span_rows, 1)
        expanded = jnp.dot(
            latent_rows.reshape(seq_count * span_rows, latent_rows.shape[2]),
            latent_up,
            preferred_element_type=f32,
        ).astype(jnp.bfloat16)
        expanded = expanded.reshape(seq_count, span_rows, latent_count, NOPE + VDIM)
        return (
            expanded[..., :NOPE],
            expanded[..., NOPE:],
            lax.dynamic_slice_in_dim(portion[1], row_start, span_rows, 1),
        )

    portion = (
        lax.all_gather(kv_seq, "sp", axis=1, tiled=True),
        lax.all_gather(rope_keys, "sp", axis=1, tiled=True),
    )
    row_count = portion[0].shape[1]
    span_rows = math.gcd(row_count, token_count * max(1, 512 // token_count))

    def visit_rows(current):

        def visit_block(block_index, stats):
            row_start = block_index * span_rows
            key_plain, value_rows, rope_rows = expand_latent(portion, row_start, span_rows)
            return attend_block(stats, key_plain, value_rows, rope_rows, row_start)

        return lax.fori_loop(0, row_count // span_rows, visit_block, current)

    _, row_sum, weighted = lax.cond(
        jnp.int32(0) < query_start + token_count, visit_rows, keep_same, start_stats
    )
    latent_heads = (
        jnp.transpose(weighted / row_sum[..., None], (0, 2, 1, 3))
        .reshape(row_total, latent_count * VDIM)
        .astype(jnp.bfloat16)
    )
    heads_joined = jnp.concatenate([delta_heads, latent_heads], axis=1)
    out_rows = jnp.concatenate([delta_out, latent_out], axis=0)
    partial_value = jnp.dot(
        heads_joined,
        lax.all_gather(out_rows, ("sp", "fs"), axis=1, tiled=True),
        preferred_element_type=f32,
    )
    mixed_half = lax.psum_scatter(
        partial_value.astype(jnp.bfloat16), "tp", scatter_dimension=1, tiled=True
    ).astype(jnp.float32)
    squares = lax.psum(jnp.sum(mixed_half * mixed_half, axis=1), "tp")
    row_scale = lax.rsqrt(squares / D + NORM_EPS)
    result = mixed_half * row_scale[:, None] * post_gain
    return result.astype(jnp.bfloat16).reshape(seq_count, token_count, result.shape[1])


def pick(array, index):
    return lax.dynamic_index_in_dim(array, index, 0, False)


def dot32(left, right):
    return jnp.dot(left, right, preferred_element_type=jnp.float32)


def dot_t(left, right):
    return lax.dot_general(
        left, right, (((1,), (1,)), ((), ())), preferred_element_type=jnp.float32
    )


def two_parts(values):
    high = values.astype(jnp.bfloat16)
    return high, (values - high.astype(jnp.float32)).astype(jnp.bfloat16)


def fine_dot(left, right, product=dot32):
    left_high, left_low = two_parts(left)
    right_high, right_low = two_parts(right)
    return product(left_high, right_high) + (
        product(left_high, right_low) + product(left_low, right_high)
    )


def kernel_call(body, out_shapes, args, scratch=(), inside=(True, True), outside=0):
    space = pl.BlockSpec(memory_space=pltpu.VMEM)
    operand_space, result_space = (pltpu.VMEM if here else pltpu.HBM for here in inside)
    return pl.pallas_call(
        body,
        out_shape=jax.tree.map(lambda leaf: result_space(leaf.shape, leaf.dtype), out_shapes),
        in_specs=[space] * len(args),
        out_specs=jax.tree.map(lambda _: space, out_shapes),
        scratch_shapes=scratch,
        compiler_params=pltpu.CompilerParams(vmem_limit_bytes=16 * 1024 * 1024),
    )(
        *(
            pltpu.with_memory_space_constraint(arg, pltpu.HBM if i < outside else operand_space)
            for i, arg in enumerate(args)
        )
    )


def started(pairs, sems):
    copies = [pltpu.make_async_copy(*pair, sems.at[i]) for i, pair in enumerate(pairs)]
    for copy in copies:
        copy.start()
    return copies


def outgoing_weights(mixers, lats, sp_size):
    count = len(mixers)
    half = mixers[0].shape[0] // 2
    per_mixer = mixers[0].shape[1] // sp_size
    per_lat = [w.shape[1] // sp_size // 2 for w in lats]
    first_lat = count * per_mixer
    padded = first_lat + 128

    def body(*refs):
        out_ref, own_ref, *held_refs, sems = refs[count + 2 :]
        rows = pl.ds(pl.multiple_of(lax.axis_index("grp") * half, half), half)
        held = started([(ref.at[rows], to) for ref, to in zip(refs, held_refs)], sems)
        first = lax.axis_index("tp") == 0
        for copy in held:
            copy.wait()
        for s in range(sp_size):
            for k in range(count):
                out_ref[s, :, k * per_mixer : (k + 1) * per_mixer] = held_refs[k][
                    :, s * per_mixer : (s + 1) * per_mixer
                ]
            pieces = []
            for ref, per in zip(held_refs[count:], per_lat):
                pair = ref[:, 2 * s * per : 2 * (s + 1) * per]
                pieces.append(jnp.where(first, pair[:, :per], pair[:, per:]))
            pieces.append(jnp.zeros((half, 128 - sum(per_lat)), jnp.bfloat16))
            out_ref[s, :, first_lat:] = jnp.concatenate(pieces, axis=1)
        own_ref[...] = out_ref[lax.axis_index("sp")]

    space = pl.BlockSpec(memory_space=pltpu.VMEM)
    return pl.pallas_call(
        body,
        out_shape=(
            pltpu.HBM((sp_size, half, padded), jnp.bfloat16),
            pltpu.HBM((half, padded), jnp.bfloat16),
        ),
        in_specs=[pl.BlockSpec(memory_space=pl.ANY)] * (count + 2),
        out_specs=(space, space),
        scratch_shapes=(
            *(pltpu.VMEM((half, w.shape[1]), jnp.bfloat16) for w in (*mixers, *lats)),
            pltpu.SemaphoreType.DMA((count + 2,)),
        ),
        name="outgoing_weights",
        compiler_params=pltpu.CompilerParams(vmem_limit_bytes=16 * 1024 * 1024),
    )(*(pltpu.with_memory_space_constraint(w, pltpu.HBM) for w in (*mixers, *lats)))


def outgoing_tokens(tokens, gain, sp_size):
    rows, width = tokens.shape
    block = width // (sp_size * 4)

    def body(token_ref, gain_ref, mine_ref, their_ref):
        values = token_ref[...].astype(jnp.float32)
        normed = (values * rms_scale(values) * gain_ref[...]).astype(jnp.bfloat16)
        first = lax.axis_index("tp") == 0
        for f in range(2):
            for s in range(sp_size):
                begin = (s * 2 + f) * 2 * block
                low = normed[:, begin : begin + block]
                high = normed[:, begin + block : begin + 2 * block]
                at = (f * sp_size + s) * block
                mine_ref[:, at : at + block] = jnp.where(first, low, high)
                their_ref[:, at : at + block] = jnp.where(first, high, low)

    shape = jax.ShapeDtypeStruct((rows, width // 2), jnp.bfloat16)
    return kernel_call(body, (shape, shape), (tokens, gain))


def prepare(narrow, query_up, latent_up, sp_size):
    width = narrow[0].shape[1]
    block = width // (sp_size * 4)
    rank, query_width = query_up.shape
    per_query = query_width // sp_size
    heads = per_query // (NOPE + ROPE)
    per_latent = latent_up.shape[1] // sp_size

    def body(rope_ref, beta_ref, decay_ref, query_ref, latent_ref, narrow_ref, q_ref, kv_ref):
        place = lax.axis_index("sp")
        rows = jnp.concatenate([rope_ref[...], beta_ref[...], decay_ref[...]], axis=0)
        for s in range(sp_size):
            for f in range(2):
                for g in range(2):
                    begin = ((s * 2 + f) * 2 + g) * block
                    at = ((g * 2 + f) * sp_size + s) * block
                    narrow_ref[:, at : at + block] = rows[:, begin : begin + block]
        own = query_ref[:, :per_query]
        for s in range(1, sp_size):
            own = jnp.where(place == s, query_ref[:, s * per_query : (s + 1) * per_query], own)
        pairs = [
            (own[:, h * (NOPE + ROPE) :][:, :NOPE], own[:, h * (NOPE + ROPE) :][:, NOPE : NOPE + ROPE])
            for h in range(heads)
        ]
        parts = [plain for plain, _ in pairs] + [turn for _, turn in pairs]
        for _, turn in pairs:
            parts += [turn[:, ROPE // 2 :], turn[:, : ROPE // 2]]
        q_ref[...] = jnp.concatenate(parts, axis=1)
        kv_ref[...] = latent_ref[:, pl.ds(pl.multiple_of(place * per_latent, 128), per_latent)]

    bf16 = jnp.bfloat16
    return kernel_call(
        body,
        (
            jax.ShapeDtypeStruct((sum(n.shape[0] for n in narrow), width), bf16),
            jax.ShapeDtypeStruct((rank, heads * (NOPE + 2 * ROPE)), bf16),
            jax.ShapeDtypeStruct((latent_up.shape[0], per_latent), bf16),
        ),
        (*narrow, query_up, latent_up),
        inside=(False, True),
    )


def project(mine, theirs, block, peers, extra, sizes):
    seq_count, token_count, fine, q_cols, kv_cols = sizes
    sp_size = len(mine)
    chunk, part = mine[0].shape
    span = sp_size * token_count
    rows = seq_count * span
    piece, columns = peers[0].shape
    extra_width = extra.shape[0]
    q_stack, kv_stack = 128 // q_cols, 128 // kv_cols
    packed = rows // q_stack + rows // kv_stack
    copies = 1 + 3 * (sp_size + 1) + 2 * sp_size

    def body(*refs):
        mine_refs, refs = refs[:sp_size], refs[sp_size:]
        their_refs, refs = refs[:sp_size], refs[sp_size:]
        block_ref, refs = refs[0], refs[1:]
        peer_refs, refs = refs[:9], refs[9:]
        extra_ref, fine_ref, pack_ref, ext_ref, lat_ref, weight_ref, token_ref, sems = refs
        place, fs_at = lax.axis_index("sp"), lax.axis_index("fs")
        tp_at, grp_at = lax.axis_index("tp"), lax.axis_index("grp")
        step = piece // 2

        def rows_at(same_grp, same_fs, source, first, number):
            grp_from = grp_at if same_grp else 1 - grp_at
            block_from = (grp_from * 2 + (fs_at if same_fs else 1 - fs_at)) * sp_size + source
            return weight_ref.at[pl.ds(pl.multiple_of(block_from * piece + first, step), number)]

        moves = [(block_ref, rows_at(True, True, 0, 0, sp_size * piece))]
        half_rows = (sp_size - 1) * step
        for k, flips in enumerate(((True, False), (False, True), (False, False))):
            own_ref, low_ref, high_ref = peer_refs[3 * k : 3 * k + 3]
            moves.append((own_ref, rows_at(*flips, place, 0, piece)))
            for o in range(1, sp_size):
                source = lax.rem(place + o, sp_size)
                begin, end = (o - 1) * piece, o * piece
                cut = min(max(begin, half_rows), end)
                if cut > begin:
                    from_ref = low_ref.at[begin:cut]
                    moves.append((from_ref, rows_at(*flips, source, 0, cut - begin)))
                if end > cut:
                    from_ref = high_ref.at[cut - half_rows : end - half_rows]
                    moves.append((from_ref, rows_at(*flips, source, cut - begin, end - cut)))
        for o in range(sp_size):
            of = pl.ds(o * chunk, chunk)
            at = pl.ds(pl.multiple_of(tp_at * part, part), part)
            moves.append((mine_refs[o], token_ref.at[of, at]))
            at = pl.ds(pl.multiple_of((1 - tp_at) * part, part), part)
            moves.append((their_refs[o], token_ref.at[of, at]))
        assert len(moves) <= copies
        moves = started(moves, sems)
        for copy in moves[: -2 * sp_size]:
            copy.wait()
        for o in range(sp_size):
            for copy in moves[len(moves) - 2 * (sp_size - o) :][:2]:
                copy.wait()
            lhs = token_ref[o * chunk : (o + 1) * chunk, :]
            value = dot32(lhs, weight_ref[...]).astype(jnp.bfloat16)
            source = lax.bitwise_xor(place, o)
            for n in range(seq_count):
                of = slice(n * token_count, (n + 1) * token_count)
                at = pl.ds(pl.multiple_of(source * token_count, token_count), token_count)
                fine_ref[n, at, :] = value[of, :fine]
                at = pl.ds(
                    pl.multiple_of(n * span + source * token_count, token_count), token_count
                )
                lat_ref[at, :] = value[of, fine : fine + 128]
        outer = dot_t(token_ref[...], extra_ref[...])
        for o in range(sp_size):
            source = lax.bitwise_xor(place, o)
            for n in range(seq_count):
                of = slice(o * chunk + n * token_count, o * chunk + (n + 1) * token_count)
                at = pl.ds(pl.multiple_of(source * token_count, token_count), token_count)
                ext_ref[n, at, :] = outer[of]
        for start, first, width, count in (
            (0, 0, q_cols, q_stack),
            (rows // q_stack, q_cols, kv_cols, kv_stack),
        ):
            group = rows // count
            joined = jnp.concatenate(
                [
                    lat_ref[k * group : (k + 1) * group, first : first + width]
                    for k in range(count)
                ],
                axis=1,
            )
            for j in range(sp_size):
                pack_ref[j, start : start + group, :] = joined

    space = pl.BlockSpec(memory_space=pltpu.VMEM)
    moved = tuple(
        pltpu.with_memory_space_constraint(array, pltpu.HBM)
        for array in (*mine, *theirs, block, *peers)
    )
    return pl.pallas_call(
        body,
        out_shape=(
            pltpu.VMEM((seq_count, span, fine), jnp.bfloat16),
            pltpu.VMEM((sp_size, packed, 128), jnp.bfloat16),
            pltpu.VMEM((seq_count, span, extra_width), jnp.float32),
        ),
        in_specs=[pl.BlockSpec(memory_space=pl.ANY)] * len(moved) + [space],
        out_specs=(space,) * 3,
        scratch_shapes=(
            pltpu.VMEM((rows, 128), jnp.bfloat16),
            pltpu.VMEM((2 * part, columns), jnp.bfloat16),
            pltpu.VMEM((rows, 2 * part), jnp.bfloat16),
            pltpu.SemaphoreType.DMA((copies,)),
        ),
        name="project",
        compiler_params=pltpu.CompilerParams(vmem_limit_bytes=16 * 1024 * 1024),
    )(*moved, pltpu.with_memory_space_constraint(extra, pltpu.VMEM))


def send_by_pair(out_refs, pieces, sp_size):
    place = lax.axis_index("sp")
    for step, out_ref in enumerate(out_refs):
        second = lax.rem(place + step, sp_size) >= sp_size // 2
        for n, (low, high) in enumerate(pieces):
            rows = low.shape[0]
            out_ref[n * rows : (n + 1) * rows, :] = jnp.where(second, high, low)


def lower_inverses(lowers, base):
    size = lowers[0].shape[0]
    row = lax.broadcasted_iota(jnp.int32, (size, size), 0)
    col = lax.broadcasted_iota(jnp.int32, (size, size), 1)
    unit = jnp.where(row == col, 1.0, 0.0)
    powers = [jnp.where(row // base == col // base, low, 0.0) for low in lowers]
    inverses = [unit - p for p in powers]
    reach = 2
    while reach < base:
        powers = [fine_dot(p, p) for p in powers]
        inverses = [i + fine_dot(i, p) for i, p in zip(inverses, powers)]
        reach *= 2
    block = base
    while block < size:
        joint = (row // (2 * block) == col // (2 * block)) & (row // block != col // block)
        moved = [fine_dot(i, jnp.where(joint, low, 0.0)) for i, low in zip(inverses, lowers)]
        inverses = [i - fine_dot(m, i) for i, m in zip(inverses, moved)]
        block *= 2
    return inverses


def delta_mix(fine, ext, gains, gain_at, gates, gate_at, heads, sp_size):
    seq_count, span, _ = fine.shape
    tile = math.gcd(span, 128)
    tiles = span // tile

    def terms(raw_query, raw_key, raw_value, beta_pre, decay_pre, rate):
        query = unit_rows(jax.nn.silu(raw_query)) * HEAD ** (-0.5)
        key = unit_rows(jax.nn.silu(raw_key))
        value = jax.nn.silu(raw_value)
        beta = jax.nn.sigmoid(beta_pre)
        log_decay = -rate * jax.nn.softplus(decay_pre)
        row = lax.broadcasted_iota(jnp.int32, (span, span), 0)
        col = lax.broadcasted_iota(jnp.int32, (span, span), 1)
        as_row = jnp.sum(jnp.where(row == col, log_decay, 0.0), axis=0, keepdims=True)
        gate = jnp.sum(jnp.where(row >= col, as_row, 0.0), axis=1, keepdims=True)
        gate_row = jnp.sum(jnp.where(row == col, gate, 0.0), axis=0, keepdims=True)
        decay = jnp.where(row >= col, jnp.exp(jnp.where(row >= col, gate - gate_row, 0.0)), 0.0)
        lower = fine_dot(key * beta, key, dot_t) * jnp.where(row > col, decay, 0.0)
        scores = fine_dot(query, key, dot_t) * decay
        return lower, scores, value * beta

    def body(fine_ref, ext_ref, gain_ref, *out_refs):
        gain_row = gain_ref[:, gain_at : gain_at + HEAD]
        rate_row = gain_ref[:, gain_at + HEAD : gain_at + 2 * HEAD]
        first_head = (lax.axis_index("tp") * sp_size + lax.axis_index("sp")) * heads
        lane = lax.broadcasted_iota(jnp.int32, (span, ext.shape[2]), 1)
        rate_lane = lax.broadcasted_iota(jnp.int32, (1, HEAD), 1)
        chains = []
        for n in range(seq_count):
            for h in range(heads):
                raw = [
                    fine_ref[n, :, (k * heads + h) * HEAD : (k * heads + h + 1) * HEAD].astype(
                        jnp.float32
                    )
                    for k in range(3)
                ]
                head = first_head + h
                outer = ext_ref[n]
                beta_pre, decay_pre = (
                    jnp.sum(
                        jnp.where(lane == gate_at + k * gates + head, outer, 0.0),
                        axis=1,
                        keepdims=True,
                    )
                    for k in range(2)
                )
                rate = jnp.sum(
                    jnp.where(rate_lane == head, rate_row, 0.0), axis=1, keepdims=True
                )
                chains.append(terms(*raw, beta_pre, decay_pre, rate))
        cuts = [slice(j * tile, (j + 1) * tile) for j in range(tiles)]
        inverses = lower_inverses([c[0][cut, cut] for c in chains for cut in cuts], 8)
        solved = [[] for _ in chains]
        for j, cut in enumerate(cuts):
            for i, (lower, _, wanted) in enumerate(chains):
                rest = wanted[cut]
                if j:
                    rest = rest - fine_dot(
                        lower[cut, : j * tile], jnp.concatenate(solved[i], axis=0)
                    )
                solved[i].append(fine_dot(inverses[i * tiles + j], rest))
        pieces = []
        for i, (_, scores, _) in enumerate(chains):
            out = fine_dot(scores, jnp.concatenate(solved[i], axis=0))
            out = (out * rms_scale(out) * gain_row).astype(jnp.bfloat16)
            pieces.append((out[: span // 2], out[span // 2 :]))
        for h in range(heads):
            columns = slice(h * HEAD, (h + 1) * HEAD)
            views = [ref.at[:, columns] for ref in out_refs] if heads > 1 else out_refs
            send_by_pair(views, pieces[h::heads], sp_size)

    shape = jax.ShapeDtypeStruct((seq_count * span // 2, heads * HEAD), jnp.bfloat16)
    return kernel_call(body, (shape,) * sp_size, (fine, ext, gains), inside=(True, False))


def latent_mix(mine, theirs, ext, tables, gains, ups, q_cols, kv_cols, heads):
    sp_size = mine.shape[0]
    seq_count, span, _ = ext.shape
    rows = seq_count * span
    q_rank, kv_rank = ups[0].shape[0], ups[1].shape[0]
    scale = (NOPE + ROPE) ** (-0.5)

    def unpack(value, n, base, width):
        group = rows * width // 128
        pieces = []
        for k in range(128 // width):
            if n * span < (k + 1) * group and k * group < (n + 1) * span:
                low = max(n * span - k * group, 0)
                high = min((n + 1) * span - k * group, group)
                pieces.append(
                    value[base + low : base + high, k * width : (k + 1) * width]
                )
        return jnp.concatenate(pieces, axis=0) if len(pieces) > 1 else pieces[0]

    def body(mine_ref, their_ref, ext_ref, cos_ref, sin_ref, *refs):
        gain_ref, qup_ref, kup_ref, *out_refs = refs
        q_gain = gain_ref[:, :q_rank]
        kv_gain = gain_ref[:, q_rank : q_rank + kv_rank]
        first = lax.axis_index("tp") == 0
        row = lax.broadcasted_iota(jnp.int32, (span, span), 0) // BLOCK
        col = lax.broadcasted_iota(jnp.int32, (span, span), 1) // BLOCK
        allowed = col <= row
        cosine, sine = cos_ref[...], sin_ref[...]
        pairs = []
        for s in range(sp_size):
            own, other = mine_ref[s], their_ref[s]
            pairs += [jnp.where(first, own, other), jnp.where(first, other, own)]
        joins, held = [], []
        for n in range(seq_count):
            q_parts = [unpack(p, n, 0, q_cols) for p in pairs]
            kv_parts = [unpack(p, n, rows * q_cols // 128, kv_cols) for p in pairs]
            q_lat = jnp.concatenate(q_parts, axis=1).astype(jnp.float32)
            kv_lat = jnp.concatenate(kv_parts, axis=1).astype(jnp.float32)
            q_norm = (q_lat * rms_scale(q_lat) * q_gain).astype(jnp.bfloat16)
            kv_norm = (kv_lat * rms_scale(kv_lat) * kv_gain).astype(jnp.bfloat16)
            q_all = dot32(q_norm, qup_ref[...]).astype(jnp.bfloat16)
            kv_all = dot32(kv_norm, kup_ref[...]).astype(jnp.bfloat16)
            plain_width, turn_width = heads * NOPE, heads * ROPE
            plain = q_all[:, :plain_width]
            turn = q_all[:, plain_width : plain_width + turn_width].astype(jnp.float32)
            swapped = q_all[:, plain_width + turn_width :].astype(jnp.float32)
            turned = (turn * cosine + swapped * sine).astype(jnp.bfloat16)
            raw = ext_ref[n, :, :ROPE].astype(jnp.bfloat16).astype(jnp.float32)
            back = jnp.concatenate([raw[:, ROPE // 2 :], raw[:, : ROPE // 2]], axis=1)
            key_turn = (raw * cosine[:, :ROPE] + back * sine[:, :ROPE]).astype(jnp.bfloat16)
            for h in range(heads):
                key_plain = kv_all[:, h * (NOPE + VDIM) : h * (NOPE + VDIM) + NOPE]
                values = kv_all[:, h * (NOPE + VDIM) + NOPE : (h + 1) * (NOPE + VDIM)]
                logits = (
                    dot_t(plain[:, h * NOPE : (h + 1) * NOPE], key_plain)
                    + dot_t(turned[:, h * ROPE : (h + 1) * ROPE], key_turn)
                ) * scale
                held.append((jnp.where(allowed, logits, -jnp.inf), values))
        peaks = [jnp.max(logits, axis=-1, keepdims=True) for logits, _ in held]
        weights = [jnp.exp(logits - peak) for (logits, _), peak in zip(held, peaks)]
        totals = [jnp.sum(w, axis=-1, keepdims=True) for w in weights]
        mixed = [dot32(w.astype(jnp.bfloat16), v) for w, (_, v) in zip(weights, held)]
        results = [m / t for m, t in zip(mixed, totals)]
        for n in range(seq_count):
            joined = jnp.concatenate(results[n * heads : (n + 1) * heads], axis=1).astype(
                jnp.bfloat16
            )
            joins.append((joined[: span // 2], joined[span // 2 :]))
        send_by_pair(out_refs, joins, sp_size)

    shape = jax.ShapeDtypeStruct((rows // 2, heads * VDIM), jnp.bfloat16)
    return kernel_call(
        body, (shape,) * sp_size, (mine, theirs, ext, *tables, gains, *ups), outside=1
    )


def output_partial(delta_all, latent_all, near, near_fs, far, gain, sizes):
    seq_count, token_count = sizes
    sp_size = len(delta_all)
    rows, d_width = delta_all[0].shape
    l_width = latent_all[0].shape[1]
    total, columns = near.shape
    half = total // 2
    per_half = sp_size // 2

    def body(*refs):
        d_refs, refs = refs[:sp_size], refs[sp_size:]
        l_refs, refs = refs[:sp_size], refs[sp_size:]
        near_ref, near_fs_ref, *far_refs, gain_ref, keep_ref, pass_ref, kept_ref, lhs_ref = refs
        kept_ref[...] = gain_ref[...]
        place, fs_at = lax.axis_index("sp"), lax.axis_index("fs")
        grp_at = lax.axis_index("grp")
        for o in range(sp_size):
            source = lax.rem(place + o, sp_size)
            base = (source // per_half) * half
            within = lax.rem(source, per_half)
            at = pl.multiple_of(base + within * d_width, 128)
            lhs_ref[:, pl.ds(at, d_width)] = d_refs[o][...]
            at = pl.multiple_of(base + per_half * d_width + within * l_width, 128)
            lhs_ref[:, pl.ds(at, l_width)] = l_refs[o][...]
        lhs = lhs_ref[...]
        own = lhs_ref[:, pl.ds(pl.multiple_of(grp_at * half, half), half)]
        other = lhs_ref[:, pl.ds(pl.multiple_of((1 - grp_at) * half, half), half)]
        close = (
            dot32(lhs, near_ref[...]).astype(jnp.bfloat16),
            dot32(lhs, near_fs_ref[...]).astype(jnp.bfloat16),
        )
        away = tuple(
            (dot32(own, far_refs[k][...]) + dot32(other, far_refs[k + 1][...])).astype(jnp.bfloat16)
            for k in (0, 2)
        )
        straight = place // per_half == lax.axis_index("tp")
        for k in range(2):
            begin = (1 - fs_at) if k else fs_at
            at = pl.ds(pl.multiple_of(begin * columns, columns), columns)
            keep = jnp.where(straight, close[k], away[k])
            onward = jnp.where(straight, away[k], close[k])
            pair_rows = 2 * token_count
            for n in range(seq_count):
                for p in range(2):
                    of = slice(n * pair_rows + p * token_count, n * pair_rows + (p + 1) * token_count)
                    to = slice(n * token_count, (n + 1) * token_count)
                    keep_ref[p, to, at] = keep[of]
                    pass_ref[p, to, at] = onward[of]

    shape = jax.ShapeDtypeStruct((2, rows // 2, 2 * columns), jnp.bfloat16)
    return kernel_call(
        body,
        (shape, shape, jax.ShapeDtypeStruct(gain.shape, gain.dtype)),
        (*delta_all, *latent_all, near, near_fs, *far, gain),
        scratch=(pltpu.VMEM((rows, total), jnp.bfloat16),),
    )


def whole_tables(length, repeats):
    frequency = ROPE_THETA ** (-np.arange(0, ROPE, 2, dtype=np.float32) / np.float32(ROPE))
    angles = np.arange(length, dtype=np.float32)[:, None] * frequency[None, :].astype(np.float32)
    cosine, sine = np.cos(angles), np.sin(angles)
    return tuple(
        jnp.asarray(np.tile(np.concatenate(pair, axis=1), (1, repeats)), jnp.float32)
        for pair in ((cosine, cosine), (-sine, sine))
    )


def whole_sequences(
    tokens,
    pre_gain,
    query_weight,
    key_weight,
    value_weight,
    beta_weight,
    decay_weight,
    decay_rate,
    delta_gain,
    query_down,
    latent_down,
    rope_weight,
    query_gain,
    latent_gain,
    query_up,
    latent_up,
    delta_out,
    latent_out,
    post_gain,
):
    f32, bf16 = jnp.float32, jnp.bfloat16
    sp_size, tp_size = lax.axis_size("sp"), lax.axis_size("tp")
    place, grp_at = lax.axis_index("sp"), lax.axis_index("grp")
    seq_count, token_count, width = tokens.shape
    rows = seq_count * token_count
    heads = query_weight.shape[1] // HEAD // sp_size
    shares = sp_size * tp_size
    q_cols, kv_cols = query_down.shape[1] // shares, latent_down.shape[1] // shares

    def exchange(values, axis):
        return lax.all_to_all(values, axis, 0, 0, tiled=True)

    def swap(values, axis):
        return lax.ppermute(values, axis, [(0, 1), (1, 0)])

    def along(values, step):
        return lax.ppermute(values, "sp", [(i, (i + step) % sp_size) for i in range(sp_size)])

    def from_sp(sends):
        return [sends[0]] + [along(sends[step], step) for step in range(sp_size - 1, 0, -1)]

    outgoing, own_piece = outgoing_weights(
        (query_weight, key_weight, value_weight), (query_down, latent_down), sp_size
    )
    block = exchange(outgoing, "sp")
    token_rows, outgoing = lax.optimization_barrier((tokens.reshape(rows, width), outgoing))

    own_half, other_half = outgoing_tokens(token_rows, pre_gain[None, :], sp_size)

    def beside(values):
        return lax.ppermute(values, "sp", [(i, i ^ 1) for i in range(sp_size)])

    far_half = along(own_half, sp_size // 2)
    mine = [own_half, beside(own_half), far_half, beside(far_half)]
    theirs = [other_half] + [swap(piece, "tp") for piece in mine[1:]]

    quarter = delta_out.shape[0] // 2
    near = jnp.concatenate(
        [w[k * quarter : (k + 1) * quarter] for k in range(2) for w in (delta_out, latent_out)]
    )
    near_fs = swap(near, "fs")

    own_grp, own_fs = swap(own_piece, "grp"), swap(own_piece, "fs")
    own_corner = swap(own_grp, "fs")
    rest = lax.dynamic_slice_in_dim(jnp.concatenate([block, block]), place + 1, sp_size - 1, 0)
    rest = rest.reshape(-1, rest.shape[2])
    block = block.reshape(-1, block.shape[2])
    middle = rest.shape[0] // 2
    low, high = rest[:middle], rest[middle:]
    low_grp, high_fs = swap(low, "grp"), swap(high, "fs")
    high_grp, low_fs = swap(high, "grp"), swap(low, "fs")
    corner = swap(low_grp, "fs"), swap(high_fs, "grp")
    peers = (own_fs, low_fs, high_fs, own_grp, low_grp, high_grp, own_corner, *corner)

    far_own = lax.dynamic_slice_in_dim(near, grp_at * 2 * quarter, 2 * quarter, 0)
    far_own = along(far_own, sp_size // 2)
    far_other = swap(far_own, "grp")
    far = (far_own, far_other, swap(far_own, "fs"))
    far = (*far, swap(far_other, "fs"))

    gate_at = rope_weight.shape[1]
    latent_heads = query_up.shape[1] // (NOPE + ROPE) // sp_size
    extra, q_up, kv_up = prepare(
        (rope_weight.T, beta_weight.T, decay_weight.T), query_up, latent_up, sp_size
    )
    tables = whole_tables(sp_size * token_count, latent_heads)
    rates = jnp.pad(decay_rate, (0, HEAD - decay_rate.shape[0]))
    latent_gains = jnp.concatenate([query_gain, latent_gain])[None, :]
    gains = jnp.concatenate([delta_gain, rates])[None, :]
    mine[1], gains, latent_gains = lax.optimization_barrier((mine[1], gains, latent_gains))

    fine, lat, ext = project(
        mine,
        theirs,
        block,
        peers,
        extra,
        (seq_count, token_count, 3 * heads * HEAD, q_cols, kv_cols),
    )
    lat_mine = exchange(lat, "sp")
    delta_sends = delta_mix(
        fine, ext, gains, 0, decay_rate.shape[0], gate_at, heads, sp_size
    )
    lat_mine, _ = lax.optimization_barrier((lat_mine, delta_sends))
    lat_theirs = swap(lat_mine, "tp")
    delta_all = from_sp(delta_sends)
    latent_sends = latent_mix(
        lat_mine,
        lat_theirs,
        ext,
        tables,
        latent_gains,
        (q_up, kv_up),
        q_cols,
        kv_cols,
        latent_heads,
    )
    latent_all = from_sp(latent_sends)

    keep, onward, post_row = output_partial(
        delta_all, latent_all, near, near_fs, far, post_gain[None, :], (seq_count, token_count)
    )
    mixed = (keep.astype(f32) + swap(onward, "tp").astype(f32)).astype(bf16)
    side = lax.rem(place, 2)

    def across(values):
        return lax.ppermute(pick(values, 1 - side), "sp", [(i, i ^ 1) for i in range(sp_size)])

    there = across(mixed)
    squares = jnp.sum(mixed.astype(f32) * mixed.astype(f32), axis=2)
    squares = squares + swap(squares, "tp")
    squares = (pick(squares, side) + across(squares))[:, None]
    here, there = pick(mixed, side).astype(f32), there.astype(f32)
    final = jnp.concatenate(
        [jnp.where(side == 0, here, there), jnp.where(side == 0, there, here)], axis=1
    )
    result = final * lax.rsqrt(squares / D + NORM_EPS) * post_row
    return result.astype(bf16).reshape(seq_count, token_count, final.shape[1])


def fits_whole(mesh):
    shape = mesh.shape
    return all(shape[name] == 2 for name in ("grp", "fs", "tp")) and shape["sp"] == 4


def solution(mesh):
    def chosen(*args):
        head_count = args[2].shape[1] // HEAD
        latent_count = args[14].shape[1] // (NOPE + ROPE)
        sp_size = mesh.shape["sp"]
        whole = fits_whole(mesh) and head_count % sp_size == 0 and latent_count % sp_size == 0
        return (whole_sequences if whole else local)(*args)

    return jax.shard_map(
        chosen,
        mesh=mesh,
        in_specs=(
            P(("grp", "fs"), "sp", None),
            P(),
            P(("sp", "fs"), "tp"),
            P(("sp", "fs"), "tp"),
            P(("sp", "fs"), "tp"),
            P(),
            P(),
            P(),
            P(),
            P(("sp", "fs"), None),
            P(("sp", "fs"), None),
            P(),
            P(),
            P(),
            P(None, "tp"),
            P(None, "tp"),
            P("tp", ("sp", "fs")),
            P("tp", ("sp", "fs")),
            P("tp"),
        ),
        out_specs=P(("grp", "fs"), "sp", "tp"),
        check_vma=False,
    )
```
